32 devices in a mesh: sp: 16 (over z, y, x), tp: 2 (over core).
Axes of the slice: x: 2, y: 2, z: 4, core: 2. Of those that a mesh axis runs over, the one named last changes fastest.
Arguments:
- tokens: bfloat16 [8192, 3072], P('sp'), may hold values from -72 to 72
- w_query: bfloat16 [3072, 1024], P('sp', 'tp'), may hold values from -0.109375 to 0.109375
- w_key: bfloat16 [3072, 1024], P('sp', 'tp'), may hold values from -0.109375 to 0.109375
- w_value: bfloat16 [3072, 1024], P('sp', 'tp'), may hold values from -0.4375 to 0.4375
- w_out: bfloat16 [1024, 3072], P('tp', 'sp'), may hold values from -0.1875 to 0.1875
Outputs:
- mixed: bfloat16 [8192, 3072], P(('sp', 'tp'))
- row_lse: float32 [16, 8192], P('tp', 'sp')
The draws below stay inside these ranges and needn't reach their ends.
All inputs are finite; a program needn't handle non-finite values.
Results may differ from the reference program's by a relative error of at most 0.014.
Values may be sent and summed in bfloat16 or wider, within the bound.
A program may use at most 64 MiB of HBM per device.

```python
import jax
import jax.numpy as jnp
from jax import lax

D = 3072
HEADS = 16
HEAD_SIZE = 64
KEYS_BEHIND = 128
D_ATT = 1024
SEQUENCE_TOKENS = 8192
N_TP = 2


def draw_tokens(key, part):
    base_offset = jax.random.truncated_normal(key, -6.0, 6.0, (SEQUENCE_TOKENS, D), jnp.float32)
    return base_offset.astype(jnp.bfloat16)


def block_levels(own_key, extent, pieces, least, high):
    factor_of = 1.0
    for dim, blocks in pieces:
        steps = jax.random.uniform(jax.random.fold_in(jax.random.fold_in(own_key, 6), dim), (blocks,), jnp.float32, least / len(pieces), high / len(pieces))
        factor_of = factor_of * jnp.repeat(jnp.exp(steps), extent[dim] // blocks).reshape((-1,) + (1,) * (len(extent) - 1 - dim))
    return factor_of


def centred(key, extent, spread, bound, pieces=(), held_as=jnp.bfloat16):
    result = jax.random.normal(key, extent, jnp.float32) * spread
    if len(pieces) > 0:
        result = block_levels(key, extent, pieces, -0.22, 0.18) * result
    return jnp.clip(result, min=-bound, max=bound).astype(held_as)


def setup_inputs(seed: int = 0) -> dict:
    arg_keys = jax.random.split(jax.random.key(seed), 6)
    tokens = draw_tokens(jax.random.fold_in(arg_keys[5], 71), 0)
    w_query = centred(arg_keys[1], (D, D_ATT), D ** -0.5, 0.109375, ((0, 16), (1, 2)))
    w_key = centred(arg_keys[2], (D, D_ATT), D ** -0.5, 0.109375, ((0, 16), (1, 2)))
    w_value = centred(arg_keys[3], (D, D_ATT), (D // 16) ** -0.5, 0.4375, ((0, 16), (1, 2)))
    w_out = centred(arg_keys[4], (D_ATT, D), D_ATT ** -0.5, 0.1875, ((0, 2), (1, 16)))
    return {"tokens": tokens, "w_query": w_query, "w_key": w_key, "w_value": w_value, "w_out": w_out}


dilation_rates = (1, 4, 16)
neg_big = -1e30


def band(query_class_rows, key_class_rows, value_class_rows, key_first_index):
    sequence_length = query_class_rows.shape[0]
    if sequence_length <= KEYS_BEHIND:
        blocks = 1
        step = sequence_length
        q_blk = query_class_rows[None]
        k_blk = key_class_rows[None]
        v_blk = value_class_rows[None]
    else:
        blocks = sequence_length // KEYS_BEHIND
        step = KEYS_BEHIND
        q_blk = query_class_rows.reshape(blocks, KEYS_BEHIND, HEAD_SIZE)
        k_rows = key_class_rows.reshape(blocks + 1, KEYS_BEHIND, HEAD_SIZE)
        v_rows = value_class_rows.reshape(blocks + 1, KEYS_BEHIND, HEAD_SIZE)
        k_blk = jnp.concatenate([k_rows[:-1], k_rows[1:]], axis=1)
        v_blk = jnp.concatenate([v_rows[:-1], v_rows[1:]], axis=1)
    score = jnp.einsum('nqd,nkd->nqk', q_blk.astype(jnp.float32), k_blk.astype(jnp.float32)) * (HEAD_SIZE ** -0.5)
    row_at = jnp.arange(step, dtype=jnp.int32)[:, None]
    col_at = jnp.arange(k_blk.shape[1], dtype=jnp.int32)[None, :]
    dist = KEYS_BEHIND + row_at - col_at
    key_pos = key_first_index + jnp.arange(blocks, dtype=jnp.int32)[:, None, None] * step + col_at[None]
    mask = (dist >= 0) & (dist <= KEYS_BEHIND) & (key_pos >= 0)
    score = jnp.where(mask, score, neg_big)
    top = jnp.max(score, axis=-1, keepdims=True)
    weight = jnp.exp(score - top)
    denom = jnp.sum(weight, axis=-1)
    weight_bf = weight.astype(jnp.bfloat16)
    out = jnp.einsum('nqk,nkd->nqd', weight_bf.astype(jnp.float32), v_blk.astype(jnp.float32)) / denom[..., None]
    lse = top[..., 0] + jnp.log(denom)
    return out.reshape(sequence_length, HEAD_SIZE), lse.reshape(sequence_length)


def one_head(parts):
    query_head_rows, key_head_rows, value_head_rows = parts
    outs = []
    lses = []
    for dilation_rate in dilation_rates:
        sequence_length = SEQUENCE_TOKENS // dilation_rate
        query_class_rows = query_head_rows.reshape(sequence_length, dilation_rate, HEAD_SIZE).transpose(1, 0, 2)
        padding_rows = jnp.zeros((KEYS_BEHIND * dilation_rate, HEAD_SIZE), jnp.bfloat16)
        key_class_rows = jnp.concatenate([padding_rows, key_head_rows], 0).reshape(KEYS_BEHIND + sequence_length, dilation_rate, HEAD_SIZE).transpose(1, 0, 2)
        value_class_rows = jnp.concatenate([padding_rows, value_head_rows], 0).reshape(KEYS_BEHIND + sequence_length, dilation_rate, HEAD_SIZE).transpose(1, 0, 2)
        out, lse = jax.vmap(lambda a, b, c: band(a, b, c, -KEYS_BEHIND))(query_class_rows, key_class_rows, value_class_rows)
        outs.append(out.transpose(1, 0, 2).reshape(SEQUENCE_TOKENS, HEAD_SIZE))
        lses.append(lse.T.reshape(SEQUENCE_TOKENS))
    lse_all = jnp.stack(lses, 0)
    peak = jnp.max(lse_all, axis=0)
    expo = jnp.exp(lse_all - peak)
    total = jnp.sum(expo, axis=0)
    mix = expo / total
    attended = jnp.sum(mix[..., None] * jnp.stack(outs, 0), axis=0)
    return attended, peak + jnp.log(total)


def reference(tokens, w_query, w_key, w_value, w_out):
    query_input = jnp.dot(tokens, w_query, preferred_element_type=jnp.float32).astype(jnp.bfloat16)
    keys = jnp.dot(tokens, w_key, preferred_element_type=jnp.float32).astype(jnp.bfloat16)
    values = jnp.dot(tokens, w_value, preferred_element_type=jnp.float32).astype(jnp.bfloat16)

    def heads_first(a):
        return a.reshape(SEQUENCE_TOKENS, HEADS, HEAD_SIZE).transpose(1, 0, 2)

    attended, row_lse = lax.map(one_head, (heads_first(query_input), heads_first(keys), heads_first(values)))
    attended = attended.transpose(1, 0, 2).reshape(SEQUENCE_TOKENS, D_ATT).astype(jnp.bfloat16)
    cols = D_ATT // N_TP
    total = jnp.zeros((SEQUENCE_TOKENS, D), jnp.float32)
    for group in range(N_TP):
        part = jnp.dot(attended[:, group * cols:(group + 1) * cols], w_out[group * cols:(group + 1) * cols],
                       preferred_element_type=jnp.float32).astype(jnp.bfloat16)
        total = total + part.astype(jnp.float32)
    return total.astype(jnp.bfloat16), row_lse
```

```python
import functools

import jax
import jax.numpy as jnp
from jax import lax
from jax.experimental import pallas as pl
from jax.experimental.pallas import tpu as pltpu
from jax.sharding import PartitionSpec as P

HEAD_SIZE = 64
KEYS_BEHIND = 128
LANES = 128

dilation_rates = (1, 4, 16)
neg_big = -1e30

MESH = pl.DeviceIdType.MESH
VMEM = pltpu.VMEM


def at(sp, tp):
    return {"sp": sp, "tp": tp}


def layer_kernel(
    n, n_tp, group, far, heads, wq_ref, wk_ref, wv_ref, tok_ref, o_ref, mixed_ref, lse_out_ref,
    tok_all, w_all, w_ref, kv_ref, halo_ref, o_all, qs, ks, vs, bias, top_s, den_s, acc_s, att, lse_ref, lse_all,
    att_all, sums, sums_in,
    pack_sem, own_sem, w1_send, w1_recv, up_send, up_recv, down_send, down_recv, t_send, t_recv, d_send, d_recv,
    f_send, f_recv, h_send, h_recv, ou_send, ou_recv, od_send, od_recv, b_send, b_recv, c_send, c_recv,
    a_send, a_recv, l_send, l_recv, s_send, s_recv,
):
    sp, tp = lax.axis_index("sp"), lax.axis_index("tp")
    planes = n // group
    g, plane = lax.rem(sp, group), sp // group
    rows = tok_ref.shape[0]
    own = group * rows
    base = plane * own
    half = rows // 2
    unit_rows = half // n_tp
    part = mixed_ref.shape[0]
    cut, width = o_ref.shape
    half_cut = cut // 2
    behind = far * own

    above = lax.rem(sp + group, n)
    below = lax.rem(sp + n - group, n)

    def mate(i):
        return plane * group + (g ^ i)

    near = [i for i in (1, 2) if i < group]

    barrier = pltpu.get_barrier_semaphore()
    greeted = 0

    def greet(sp_to, tp_to):
        pl.semaphore_signal(barrier, inc=1, device_id=at(sp_to, tp_to), device_id_type=MESH)
        return 1

    for i in range(1, group):
        greeted += greet(mate(i), tp)
    if planes > 1:
        for h in range(1, max(far, 1) + 1):
            greeted += greet(lax.rem(sp + h * group, n), tp)
            greeted += greet(lax.rem(sp + n - h * group, n), tp)
    for j in range(1, n_tp):
        greeted += greet(sp, lax.rem(tp + j, n_tp))

    own_t = pltpu.make_async_copy(tok_ref, tok_all.at[g], own_sem.at[0])

    def strip(q, i, part_of=None):
        origin = q * group + (g ^ i)
        if part_of is None:
            return o_all.at[pl.ds(pl.multiple_of(origin * cut, cut), cut)]
        return o_all.at[pl.ds(pl.multiple_of(origin * cut + part_of * half_cut, half_cut), half_cut)]

    own_o = pltpu.make_async_copy(o_ref, strip(plane, 0), own_sem.at[3])

    def pack(t, i):
        source = (wq_ref, wk_ref, wv_ref)[t].at[:, pl.ds(pl.multiple_of((g ^ i) * LANES, LANES), LANES)]
        lanes = pl.ds(t * LANES, LANES)
        to = w_all.at[sp, :, lanes] if i == 0 else w_ref.at[i, :, lanes]
        return pltpu.make_async_copy(source, to, pack_sem.at[t, i])

    for i in list(range(1, group)) + [0]:
        for t in range(3):
            pack(t, i).start()
    own_o.start()
    own_t.start()
    pl.semaphore_wait(barrier, greeted)

    def w_in_plane(i):
        return pltpu.make_async_remote_copy(
            src_ref=w_ref.at[i], dst_ref=w_all.at[sp], send_sem=w1_send.at[i], recv_sem=w1_recv.at[i],
            device_id=at(mate(i), tp), device_id_type=MESH)

    def w_in_plane_arrives(i):
        return pltpu.make_async_remote_copy(
            src_ref=w_ref.at[i], dst_ref=w_all.at[mate(i)], send_sem=w1_send.at[i], recv_sem=w1_recv.at[i],
            device_id=at(mate(i), tp), device_id_type=MESH)

    def slab(p, i):
        return w_all.at[lax.rem(p + 2 * planes, planes) * group + (g ^ i)]

    def up(i, k, p):
        return pltpu.make_async_remote_copy(
            src_ref=slab(p, i), dst_ref=slab(p, i), send_sem=up_send.at[i, k], recv_sem=up_recv.at[i, k],
            device_id=at(above, tp), device_id_type=MESH)

    def down(i, k, p):
        return pltpu.make_async_remote_copy(
            src_ref=slab(p, i), dst_ref=slab(p, i), send_sem=down_send.at[i, k], recv_sem=down_recv.at[i, k],
            device_id=at(below, tp), device_id_type=MESH)

    def o_up(k, p):
        ref = strip(lax.rem(p + 2 * planes, planes), 0)
        return pltpu.make_async_remote_copy(
            src_ref=ref, dst_ref=ref, send_sem=ou_send.at[k], recv_sem=ou_recv.at[k],
            device_id=at(above, tp), device_id_type=MESH)

    def o_down(k, p):
        ref = strip(lax.rem(p + 2 * planes, planes), 0)
        return pltpu.make_async_remote_copy(
            src_ref=ref, dst_ref=ref, send_sem=od_send.at[k], recv_sem=od_recv.at[k],
            device_id=at(below, tp), device_id_type=MESH)

    def when(condition, action):
        @pl.when(condition)
        def _():
            action()

    first, last = plane == 0, plane == planes - 1

    def relay(k, i):
        when(~last & (plane - k + 1 >= 0), lambda: up(i, k, plane - k + 1).start())
        when(~first & (plane + k - 1 < planes), lambda: down(i, k, plane + k - 1).start())

    def relayed(k, i):
        when(plane - k >= 0, lambda: up(i, k, plane - k).wait_recv())
        when(plane + k < planes, lambda: down(i, k, plane + k).wait_recv())

    def relay_left(k, i):
        when(~last & (plane - k + 1 >= 0), lambda: up(i, k, plane - k + 1).wait_send())
        when(~first & (plane + k - 1 < planes), lambda: down(i, k, plane + k - 1).wait_send())

    def o_relay(k):
        when(~last & (plane - k + 1 >= 0), lambda: o_up(k, plane - k + 1).start())
        when(~first & (plane + k - 1 < planes), lambda: o_down(k, plane + k - 1).start())

    def o_relay_left(k):
        when(~last & (plane - k + 1 >= 0), lambda: o_up(k, plane - k + 1).wait_send())
        when(~first & (plane + k - 1 < planes), lambda: o_down(k, plane + k - 1).wait_send())

    def hops(body):
        def one(k, _):
            for i in range(group):
                body(k, i)
            return _

        return one

    def back(q):
        return lax.rem(plane - q + planes, planes)

    def side_out(q, i):
        k = back(q)
        return pltpu.make_async_remote_copy(
            src_ref=strip(q, 0), dst_ref=strip(q, 0), send_sem=b_send.at[k, i], recv_sem=b_recv.at[k, i],
            device_id=at(mate(i), tp), device_id_type=MESH)

    def side_in(q, i):
        k = back(q)
        return pltpu.make_async_remote_copy(
            src_ref=strip(q, i), dst_ref=strip(q, i), send_sem=b_send.at[k, i], recv_sem=b_recv.at[k, i],
            device_id=at(mate(i), tp), device_id_type=MESH)

    def edge_out(q, i):
        k = back(q)
        return pltpu.make_async_remote_copy(
            src_ref=strip(q, i, i - 1), dst_ref=strip(q, i, i - 1), send_sem=c_send.at[k, i], recv_sem=c_recv.at[k, i],
            device_id=at(mate(3 - i), tp), device_id_type=MESH)

    def edge_in(q, i):
        k = back(q)
        return pltpu.make_async_remote_copy(
            src_ref=strip(q, 3, i - 1), dst_ref=strip(q, 3, i - 1), send_sem=c_send.at[k, i], recv_sem=c_recv.at[k, i],
            device_id=at(mate(3 - i), tp), device_id_type=MESH)

    def sides(q):
        for i in near:
            side_out(q, i).start()

    def edges(q):
        for i in near:
            side_in(q, i).wait_recv()
            if group == 4:
                edge_out(q, i).start()

    def o_relayed(k):
        def from_below():
            o_up(k, plane - k).wait_recv()

        def from_above():
            o_down(k, plane + k).wait_recv()

        when(plane - k >= 0, from_below)
        when(plane + k < planes, from_above)

    def o_sides(k):
        if near:
            when(plane - k >= 0, lambda: sides(plane - k))
            when(plane + k < planes, lambda: sides(plane + k))

    def unit(k, t):
        return pl.ds(pl.multiple_of(k * half + t * unit_rows, unit_rows), unit_rows)

    def tokens_out(i, k):
        return pltpu.make_async_remote_copy(
            src_ref=tok_ref.at[unit(k, tp)], dst_ref=tok_all.at[g, unit(k, tp)],
            send_sem=t_send.at[i, k], recv_sem=t_recv.at[i, k], device_id=at(mate(i), tp), device_id_type=MESH)

    def tokens_in(i, k):
        return pltpu.make_async_remote_copy(
            src_ref=tok_ref.at[unit(k, tp)], dst_ref=tok_all.at[g ^ i, unit(k, tp)],
            send_sem=t_send.at[i, k], recv_sem=t_recv.at[i, k], device_id=at(mate(i), tp), device_id_type=MESH)

    def corner_out(i):
        ref = tok_all.at[g ^ i, unit(i - 1, tp)]
        return pltpu.make_async_remote_copy(
            src_ref=ref, dst_ref=ref, send_sem=d_send.at[i], recv_sem=d_recv.at[i],
            device_id=at(mate(3 - i), tp), device_id_type=MESH)

    def corner_in(i):
        ref = tok_all.at[g ^ 3, unit(i - 1, tp)]
        return pltpu.make_async_remote_copy(
            src_ref=ref, dst_ref=ref, send_sem=d_send.at[i], recv_sem=d_recv.at[i],
            device_id=at(mate(3 - i), tp), device_id_type=MESH)

    def across(i, k, j):
        ref = tok_all.at[g ^ i, unit(k, tp)]
        return pltpu.make_async_remote_copy(
            src_ref=ref, dst_ref=ref, send_sem=f_send.at[i, k, j], recv_sem=f_recv.at[i, k, j],
            device_id=at(sp, lax.rem(tp + j, n_tp)), device_id_type=MESH)

    def across_in(i, k, j):
        ref = tok_all.at[g ^ i, unit(k, lax.rem(tp + n_tp - j, n_tp))]
        return pltpu.make_async_remote_copy(
            src_ref=ref, dst_ref=ref, send_sem=f_send.at[i, k, j], recv_sem=f_recv.at[i, k, j],
            device_id=at(sp, lax.rem(tp + j, n_tp)), device_id_type=MESH)

    def to_other_cores(i, k):
        for j in range(1, n_tp):
            across(i, k, j).start()

    def piece(i, s):
        return s if i == 1 else 1 - s

    for i in range(1, group):
        for t in range(3):
            pack(t, i).wait()
        w_in_plane(i).start()
    for t in range(3):
        pack(t, 0).wait()
    if planes > 1:
        relay(1, 0)
    for s in range(2):
        for i in near:
            tokens_out(i, piece(i, s)).start()
    for i in range(1, group):
        w_in_plane_arrives(i).wait_recv()
        if planes > 1:
            relay(1, i)

    def pass_on(k, i):
        relayed(k, i)
        relay(k + 1, i)

    row = lax.broadcasted_iota(jnp.int32, (KEYS_BEHIND, 2 * KEYS_BEHIND), 0)
    col = lax.broadcasted_iota(jnp.int32, (KEYS_BEHIND, 2 * KEYS_BEHIND), 1)
    dist = KEYS_BEHIND + row - col
    band = (dist >= 0) & (dist <= KEYS_BEHIND)
    bias[0] = jnp.where(band, 0.0, neg_big)
    for number, d in enumerate(dilation_rates):
        bias[1 + number] = jnp.where(band & (base // d - KEYS_BEHIND + col >= 0), 0.0, neg_big)
    for h in range(1, far + 1):
        @pl.when(plane - h < 0)
        def _():
            ks[(far - h) * own : (far - h + 1) * own] = jnp.zeros((own, LANES), jnp.float32)
            vs[(far - h) * own : (far - h + 1) * own] = jnp.zeros((own, LANES), jnp.float32)

    if planes > 1:
        lax.fori_loop(1, planes - 1, hops(pass_on), 0)
    own_o.wait()
    if planes > 1:
        o_relay(1)
    for i in near:
        tokens_in(i, piece(i, 0)).wait_recv()
        if group == 4:
            corner_out(i).start()
        to_other_cores(i, piece(i, 0))
    if planes > 1:
        for i in range(group):
            relayed(planes - 1, i)
    for i in near:
        tokens_in(i, piece(i, 1)).wait_recv()
        to_other_cores(i, piece(i, 1))
    if near:
        sides(plane)
    own_t.wait()

    def halo_out(h, i, k):
        view = pl.ds(pl.multiple_of((g ^ i) * rows + k * half, half), half)
        return pltpu.make_async_remote_copy(
            src_ref=kv_ref.at[view], dst_ref=halo_ref.at[far - h, view],
            send_sem=h_send.at[h, i, k], recv_sem=h_recv.at[h, i, k],
            device_id=at(lax.rem(sp + h * group, n), tp), device_id_type=MESH)

    def tile(i, k):
        block = g ^ i
        x = tok_all[block, pl.ds(pl.multiple_of(k * half, half), half), :]
        w = w_all[...].reshape(-1, 3 * LANES)
        y = jnp.dot(x, w, preferred_element_type=jnp.float32).astype(jnp.bfloat16)
        start = block * rows + k * half
        to = pl.ds(pl.multiple_of(start, half), half)
        past = pl.ds(pl.multiple_of(behind + start, half), half)
        kv_ref[to, :] = y[:, LANES:]
        qs[to, :] = y[:, :LANES].astype(jnp.float32) * HEAD_SIZE ** (-0.5)
        ks[past, :] = y[:, LANES : 2 * LANES].astype(jnp.float32)
        vs[past, :] = y[:, 2 * LANES :].astype(jnp.float32)
        for h in range(1, far + 1):
            @pl.when(plane + h < planes)
            def _():
                halo_out(h, i, k).start()

    def tiles(picks, ready):
        def one(s, _):
            i, k = picks(s)
            ready(i, k)
            tile(i, k)
            return _

        lax.fori_loop(0, 2, one, 0)

    def crossed(i, k):
        for j in range(1, n_tp):
            across_in(i, k, j).wait_recv()

    def o_step(k):
        if k < planes:
            o_relayed(k)
            o_sides(k)
            if k + 1 < planes:
                o_relay(k + 1)

    tiles(lambda s: (0, s), lambda i, k: None)
    if group > 1:
        o_step(1)
    if group == 2:
        tiles(lambda s: (1, s), crossed)
    if group == 4:
        tiles(lambda s: (1 + s, s), crossed)
        o_step(2)
        tiles(lambda s: (1 + s, 1 - s), crossed)
        o_step(3)
        for k in (1, 2):
            corner_in(k).wait_recv()
            to_other_cores(3, k - 1)
        tiles(lambda s: (3, s), crossed)
    done = {1: 1, 2: 2, 4: 4}[group]

    def o_rest(k, _):
        o_relayed(k)
        o_sides(k)
        if True:
            when(k + 1 < planes, lambda: o_relay(k + 1))
        return _

    if done < planes:
        lax.fori_loop(done, planes, o_rest, 0)

    def nearest(m):
        left, right = plane, planes - 1 - plane
        short = jnp.minimum(left, right)
        zigzag = plane + (m // 2 if m % 2 == 0 else -((m + 1) // 2))
        return jnp.where(m <= 2 * short, zigzag, jnp.where(left < right, m, planes - 1 - m))

    by_plane = group > 1
    passed = 0

    def edges_next():
        nonlocal passed
        if by_plane and passed < planes:
            edges(nearest(passed))
            passed += 1

    low_of = {}

    def attention(number, begin, end, unroll):
        d = dilation_rates[number]
        step = min(KEYS_BEHIND, own // d)
        span = step + KEYS_BEHIND
        mask_at = 1 + number if begin == 0 else 0

        def block(index, _):
            cls, b = lax.rem(index, d), index // d
            start = b * (step * d) + cls
            q_at = pl.ds(start, step, stride=d) if d > 1 else pl.ds(pl.multiple_of(start, step), step)
            k_start = behind - KEYS_BEHIND * d + start
            k_at = pl.ds(k_start, span, stride=d) if d > 1 else pl.ds(pl.multiple_of(k_start, step), span)
            q = qs[q_at, :]
            k = ks[k_at, :].astype(jnp.bfloat16)
            v = vs[k_at, :].astype(jnp.bfloat16)
            v = jnp.concatenate([v, jnp.ones((span, LANES), jnp.bfloat16)], axis=1)
            low = lax.broadcasted_iota(jnp.int32, (step, LANES), 1) < HEAD_SIZE
            q2 = jnp.concatenate([jnp.where(low, q, 0.0), jnp.where(low, 0.0, q)], axis=0).astype(jnp.bfloat16)
            s = lax.dot_general(q2, k, (((1,), (1,)), ((), ())), preferred_element_type=jnp.float32)
            seen = bias[mask_at, :step, :span]
            s = s + jnp.concatenate([seen, seen], axis=0)
            top = jnp.max(s, axis=1, keepdims=True)
            p = jnp.exp(s - top)
            o = jnp.dot(p.astype(jnp.bfloat16), v, preferred_element_type=jnp.float32)
            top = jnp.where(low, top[:step], top[step:])
            den = jnp.where(low, o[:step, LANES:], o[step:, LANES:])
            o = jnp.where(low, o[:step, :LANES], o[step:, :LANES])
            if number == 0:
                top_s[q_at, :] = top
                den_s[q_at, :] = den
                acc_s[q_at, :] = o
            else:
                was = top_s[q_at, :]
                new = jnp.maximum(was, top)
                old_scale, scale = jnp.exp(was - new), jnp.exp(top - new)
                top_s[q_at, :] = new
                den_s[q_at, :] = den_s[q_at, :] * old_scale + den * scale
                acc_s[q_at, :] = acc_s[q_at, :] * old_scale + o * scale
            return _

        lax.fori_loop(begin * d, end * d, block, 0, unroll=unroll)

    counts = [own // d // min(KEYS_BEHIND, own // d) for d in dilation_rates]

    def unroll_of(trips):
        return next(u for u in (2, 3, 1) if trips % u == 0)

    for number, d in enumerate(dilation_rates):
        if counts[number] > 1:
            attention(number, 1, counts[number], unroll_of((counts[number] - 1) * d))
            edges_next()

    for h in range(1, far + 1):
        @pl.when(plane - h >= 0)
        def _():
            for i in range(group):
                for k in range(2):
                    halo_out(h, i, k).wait_recv()
            to = slice((far - h) * own, (far - h + 1) * own)
            ks[to] = halo_ref[far - h, :, :LANES].astype(jnp.float32)
            vs[to] = halo_ref[far - h, :, LANES:].astype(jnp.float32)

    for number, d in enumerate(dilation_rates):
        attention(number, 0, 1, unroll_of(d))
        edges_next()

    att[...] = (acc_s[...] / den_s[...]).astype(jnp.bfloat16)

    def att_out(i):
        mine = pl.ds(pl.multiple_of((g ^ i) * rows, rows), rows)
        return pltpu.make_async_remote_copy(
            src_ref=att.at[mine], dst_ref=att_all.at[g], send_sem=a_send.at[i], recv_sem=a_recv.at[i],
            device_id=at(mate(i), tp), device_id_type=MESH)

    def att_in(i):
        return pltpu.make_async_remote_copy(
            src_ref=att.at[pl.ds(0, rows)], dst_ref=att_all.at[g ^ i], send_sem=a_send.at[i], recv_sem=a_recv.at[i],
            device_id=at(mate(i), tp), device_id_type=MESH)

    def lse_out(i):
        return pltpu.make_async_remote_copy(
            src_ref=lse_ref.at[g ^ i], dst_ref=lse_all.at[g], send_sem=l_send.at[i], recv_sem=l_recv.at[i],
            device_id=at(mate(i), tp), device_id_type=MESH)

    def lse_in(i):
        return pltpu.make_async_remote_copy(
            src_ref=lse_ref.at[g ^ i], dst_ref=lse_all.at[g ^ i], send_sem=l_send.at[i], recv_sem=l_recv.at[i],
            device_id=at(mate(i), tp), device_id_type=MESH)

    for i in range(1, group):
        att_out(i).start()
    own_a = pltpu.make_async_copy(att.at[pl.ds(pl.multiple_of(g * rows, rows), rows)], att_all.at[g], own_sem.at[1])
    own_a.start()

    for t in range(own // LANES):
        at_rows = pl.ds(t * LANES, LANES)
        lse = (top_s[at_rows, :] + jnp.log(den_s[at_rows, :])).T
        b, off = (t * LANES) // rows, (t * LANES) % rows
        for h in range(heads):
            lse_ref[b, h : h + 1, off : off + LANES] = lse[h * HEAD_SIZE : h * HEAD_SIZE + 1, :]
    for i in range(1, group):
        lse_out(i).start()
    own_l = pltpu.make_async_copy(lse_ref.at[g], lse_all.at[g], own_sem.at[2])
    own_l.start()

    while by_plane and passed < planes:
        edges_next()
    own_a.wait()
    for i in range(1, group):
        att_in(i).wait_recv()

    chunks, chunk = sums.shape[1], sums.shape[3]

    def columns_of(m):
        if by_plane:
            return pl.ds(pl.multiple_of(nearest(m) * chunk, chunk), chunk)
        return pl.ds(m * chunk, chunk)

    def product(c, j):
        wanted = lax.rem(tp + j, n_tp)
        here = pl.ds(pl.multiple_of(wanted * part, part), part)
        a = jnp.concatenate([att_all[b, here, :] for b in range(group)], axis=1)
        w = o_all[columns_of(c), :]
        return lax.dot_general(a, w, (((1,), (1,)), ((), ())), preferred_element_type=jnp.float32)

    def sum_out(c, j):
        return pltpu.make_async_remote_copy(
            src_ref=sums.at[j, c], dst_ref=sums_in.at[j, c], send_sem=s_send.at[j, c], recv_sem=s_recv.at[j, c],
            device_id=at(sp, lax.rem(tp + j, n_tp)), device_id_type=MESH)

    def for_others(c):
        for j in range(1, n_tp):
            sums[j, c] = product(c, j).astype(jnp.bfloat16)
            sum_out(c, j).start()

    def for_self(c):
        total = product(c, 0).astype(jnp.bfloat16).astype(jnp.float32)
        for j in range(1, n_tp):
            sum_out(c, j).wait_recv()
            total += sums_in[j, c].astype(jnp.float32)
        mixed_ref[:, columns_of(c)] = total.astype(jnp.bfloat16)

    for c in range(chunks):
        if group == 4:
            for i in near:
                edge_in(nearest(c), i).wait_recv()
        for_others(c)
        if 0 < c < chunks - 1:
            for_self(c - 1)
    if chunks > 1:
        for_self(chunks - 2)
    for_self(chunks - 1)

    own_l.wait()
    for i in range(1, group):
        lse_in(i).wait_recv()
    for b in range(group):
        lse_out_ref[b * heads : (b + 1) * heads, :] = lse_all[b]

    for i in range(1, group):
        w_in_plane(i).wait_send()
        for k in range(2):
            for j in range(1, n_tp):
                across(i, k, j).wait_send()
    for i in near:
        for k in range(2):
            tokens_out(i, k).wait_send()
        if group == 4:
            corner_out(i).wait_send()
    if planes > 1:
        lax.fori_loop(1, planes, hops(relay_left), 0)
        lax.fori_loop(1, planes, lambda k, _: (o_relay_left(k), _)[1], 0)
    for h in range(1, far + 1):
        @pl.when(plane + h < planes)
        def _():
            for i in range(group):
                for k in range(2):
                    halo_out(h, i, k).wait_send()
    for j in range(1, n_tp):
        for c in range(chunks):
            sum_out(c, j).wait_send()
    for i in range(1, group):
        att_out(i).wait_send()
        lse_out(i).wait_send()
    if by_plane:
        for m in range(planes):
            for i in near:
                side_out(nearest(m), i).wait_send()
                if group == 4:
                    edge_out(nearest(m), i).wait_send()


def shards(n, n_tp, tokens, w_query, w_key, w_value, w_out):
    rows, model = tokens.shape
    depth, width = w_query.shape
    slabs = width // LANES
    reach = KEYS_BEHIND * dilation_rates[-1]
    group = 1
    while group < 4 and group * rows < reach and slabs % (2 * group) == 0 and n % (2 * group) == 0:
        group *= 2
    assert slabs == group
    far = (reach + group * rows - 1) // (group * rows)
    planes = n // group
    own = group * rows
    part = rows // n_tp
    heads = LANES // HEAD_SIZE

    turned = w_out.T
    cut = w_out.shape[1]
    behind = far * own
    chunks = planes if group > 1 else (4 if (n * cut) % (4 * LANES) == 0 else 1)
    chunk = n * cut // chunks

    f32, bf16 = jnp.float32, jnp.bfloat16
    dma = pltpu.SemaphoreType.DMA
    vmem = pl.BlockSpec(memory_space=VMEM)
    mixed, lse = pl.pallas_call(
        functools.partial(layer_kernel, n, n_tp, group, far, heads),
        out_shape=(
            jax.ShapeDtypeStruct((part, n * cut), bf16),
            jax.ShapeDtypeStruct((group * heads, rows), f32),
        ),
        in_specs=[pl.BlockSpec(memory_space=pltpu.HBM)] * 5,
        out_specs=(vmem, vmem),
        scratch_shapes=[
            VMEM((group, rows, model), bf16),
            VMEM((n, depth, 3 * LANES), bf16),
            VMEM((group, depth, 3 * LANES), bf16),
            VMEM((own, 2 * LANES), bf16), VMEM((far, own, 2 * LANES), bf16),
            VMEM((n * cut, width), bf16),
            VMEM((own, LANES), f32), VMEM((behind + own, LANES), f32), VMEM((behind + own, LANES), f32),
            VMEM((1 + len(dilation_rates), KEYS_BEHIND, 2 * KEYS_BEHIND), f32),
            VMEM((own, LANES), f32), VMEM((own, LANES), f32), VMEM((own, LANES), f32),
            VMEM((own, LANES), bf16), VMEM((group, heads, rows), f32), VMEM((group, heads, rows), f32),
            VMEM((group, rows, LANES), bf16),
            VMEM((n_tp, chunks, part, chunk), bf16), VMEM((n_tp, chunks, part, chunk), bf16),
            dma((3, group)), dma((4,)),
            dma((group,)), dma((group,)),
            dma((group, planes)), dma((group, planes)),
            dma((group, planes)), dma((group, planes)),
            dma((group, 2)), dma((group, 2)),
            dma((group,)), dma((group,)),
            dma((group, 2, n_tp)), dma((group, 2, n_tp)),
            dma((far + 1, group, 2)), dma((far + 1, group, 2)),
            dma((planes,)), dma((planes,)), dma((planes,)), dma((planes,)),
            dma((planes, group)), dma((planes, group)),
            dma((planes, group)), dma((planes, group)),
            dma((group,)), dma((group,)), dma((group,)), dma((group,)),
            dma((n_tp, chunks)), dma((n_tp, chunks)),
        ],
        compiler_params=pltpu.CompilerParams(collective_id=0, has_side_effects=True, vmem_limit_bytes=56 << 20),
        cost_estimate=pl.CostEstimate(
            flops=2 * own * model * 3 * LANES, bytes_accessed=1 << 24, transcendentals=1 << 22),
        name="layer",
    )(w_query, w_key, w_value, tokens, turned)
    return mixed, lse


def solution(mesh):
    placed = (P("sp", None), P("sp", "tp"), P("sp", "tp"), P("sp", "tp"), P("tp", "sp"))
    return jax.shard_map(
        functools.partial(shards, mesh.shape["sp"], mesh.shape["tp"]),
        mesh=mesh,
        in_specs=placed,
        out_specs=(P(("sp", "tp"), None), P("tp", "sp")),
        check_vma=False,
    )
```

```python
import functools

import jax
import jax.numpy as jnp
from jax import lax
from jax.experimental import pallas as pl
from jax.experimental.pallas import tpu as pltpu
from jax.sharding import PartitionSpec as P

HEAD_SIZE = 64
KEYS_BEHIND = 128
LANES = 128

dilation_rates = (1, 4, 16)
neg_big = -1e30

MESH = pl.DeviceIdType.MESH
VMEM = pltpu.VMEM


def at(sp, tp):
    return {"sp": sp, "tp": tp}


def layer_kernel(
    n, n_tp, group, far, heads, wq_ref, wk_ref, wv_ref, tok_ref, o_ref, mixed_ref, lse_out_ref,
    tok_all, w_all, w_ref, kv_ref, halo_ref, o_all, qs, ks, vs, bias, top_s, den_s, acc_s, att, lse_ref, lse_all,
    att_all, sums, sums_in,
    pack_sem, own_sem, w1_send, w1_recv, up_send, up_recv, down_send, down_recv, t_send, t_recv, d_send, d_recv,
    f_send, f_recv, h_send, h_recv, ou_send, ou_recv, od_send, od_recv, b_send, b_recv, c_send, c_recv,
    zu_send, zu_recv, zd_send, zd_recv, a_send, a_recv, l_send, l_recv, s_send, s_recv,
):
    sp, tp = lax.axis_index("sp"), lax.axis_index("tp")
    planes = n // group
    g, plane = lax.rem(sp, group), sp // group
    rows = tok_ref.shape[0]
    own = group * rows
    base = plane * own
    half = rows // 2
    unit_rows = half // n_tp
    part = mixed_ref.shape[0]
    cut, width = o_ref.shape
    half_cut = cut // 2
    behind = far * own

    above = lax.rem(sp + group, n)
    below = lax.rem(sp + n - group, n)

    def mate(i):
        return plane * group + (g ^ i)

    near = [i for i in (1, 2) if i < group]

    barrier = pltpu.get_barrier_semaphore()
    greeted = 0

    def greet(sp_to, tp_to):
        pl.semaphore_signal(barrier, inc=1, device_id=at(sp_to, tp_to), device_id_type=MESH)
        return 1

    for i in range(1, group):
        greeted += greet(mate(i), tp)
    if planes > 1:
        for h in range(1, max(far, 1) + 1):
            greeted += greet(lax.rem(sp + h * group, n), tp)
            greeted += greet(lax.rem(sp + n - h * group, n), tp)
    for j in range(1, n_tp):
        greeted += greet(sp, lax.rem(tp + j, n_tp))

    own_t = pltpu.make_async_copy(tok_ref, tok_all.at[g], own_sem.at[0])

    def strip(q, i, part_of=None):
        origin = q * group + (g ^ i)
        if part_of is None:
            return o_all.at[pl.ds(pl.multiple_of(origin * cut, cut), cut)]
        return o_all.at[pl.ds(pl.multiple_of(origin * cut + part_of * half_cut, half_cut), half_cut)]

    own_o = pltpu.make_async_copy(o_ref, strip(plane, 0), own_sem.at[3])

    def pack(t, i):
        source = (wq_ref, wk_ref, wv_ref)[t].at[:, pl.ds(pl.multiple_of((g ^ i) * LANES, LANES), LANES)]
        lanes = pl.ds(t * LANES, LANES)
        to = w_all.at[sp, :, lanes] if i == 0 else w_ref.at[i, :, lanes]
        return pltpu.make_async_copy(source, to, pack_sem.at[t, i])

    for i in list(range(1, group)) + [0]:
        for t in range(3):
            pack(t, i).start()
    own_o.start()
    own_t.start()
    pl.semaphore_wait(barrier, greeted)

    def w_in_plane(i):
        return pltpu.make_async_remote_copy(
            src_ref=w_ref.at[i], dst_ref=w_all.at[sp], send_sem=w1_send.at[i], recv_sem=w1_recv.at[i],
            device_id=at(mate(i), tp), device_id_type=MESH)

    def w_in_plane_arrives(i):
        return pltpu.make_async_remote_copy(
            src_ref=w_ref.at[i], dst_ref=w_all.at[mate(i)], send_sem=w1_send.at[i], recv_sem=w1_recv.at[i],
            device_id=at(mate(i), tp), device_id_type=MESH)

    def slab(p, i):
        return w_all.at[lax.rem(p + 2 * planes, planes) * group + (g ^ i)]

    def up(i, k, p):
        return pltpu.make_async_remote_copy(
            src_ref=slab(p, i), dst_ref=slab(p, i), send_sem=up_send.at[i, k], recv_sem=up_recv.at[i, k],
            device_id=at(above, tp), device_id_type=MESH)

    def down(i, k, p):
        return pltpu.make_async_remote_copy(
            src_ref=slab(p, i), dst_ref=slab(p, i), send_sem=down_send.at[i, k], recv_sem=down_recv.at[i, k],
            device_id=at(below, tp), device_id_type=MESH)

    def o_up(k, p):
        ref = strip(lax.rem(p + 2 * planes, planes), 0)
        return pltpu.make_async_remote_copy(
            src_ref=ref, dst_ref=ref, send_sem=ou_send.at[k], recv_sem=ou_recv.at[k],
            device_id=at(above, tp), device_id_type=MESH)

    def o_down(k, p):
        ref = strip(lax.rem(p + 2 * planes, planes), 0)
        return pltpu.make_async_remote_copy(
            src_ref=ref, dst_ref=ref, send_sem=od_send.at[k], recv_sem=od_recv.at[k],
            device_id=at(below, tp), device_id_type=MESH)

    def when(condition, action):
        @pl.when(condition)
        def _():
            action()

    first, last = plane == 0, plane == planes - 1

    def relay(k, i):
        when(~last & (plane - k + 1 >= 0), lambda: up(i, k, plane - k + 1).start())
        when(~first & (plane + k - 1 < planes), lambda: down(i, k, plane + k - 1).start())

    def relayed(k, i):
        when(plane - k >= 0, lambda: up(i, k, plane - k).wait_recv())
        when(plane + k < planes, lambda: down(i, k, plane + k).wait_recv())

    def relay_left(k, i):
        when(~last & (plane - k + 1 >= 0), lambda: up(i, k, plane - k + 1).wait_send())
        when(~first & (plane + k - 1 < planes), lambda: down(i, k, plane + k - 1).wait_send())

    def o_relay(k):
        when(~last & (plane - k + 1 >= 0), lambda: o_up(k, plane - k + 1).start())
        when(~first & (plane + k - 1 < planes), lambda: o_down(k, plane + k - 1).start())

    def o_relay_left(k):
        when(~last & (plane - k + 1 >= 0), lambda: o_up(k, plane - k + 1).wait_send())
        when(~first & (plane + k - 1 < planes), lambda: o_down(k, plane + k - 1).wait_send())

    def hops(body):
        def one(k, _):
            for i in range(group):
                body(k, i)
            return _

        return one

    def nearest(m):
        left, right = plane, planes - 1 - plane
        short = jnp.minimum(left, right)
        zigzag = plane + (m // 2 if m % 2 == 0 else -((m + 1) // 2))
        return jnp.where(m <= 2 * short, zigzag, jnp.where(left < right, m, planes - 1 - m))

    def back(q):
        return lax.rem(plane - q + planes, planes)

    def side_out(q, i):
        k = back(q)
        return pltpu.make_async_remote_copy(
            src_ref=strip(q, 0), dst_ref=strip(q, 0), send_sem=b_send.at[k, i], recv_sem=b_recv.at[k, i],
            device_id=at(mate(i), tp), device_id_type=MESH)

    def side_in(q, i):
        k = back(q)
        return pltpu.make_async_remote_copy(
            src_ref=strip(q, i), dst_ref=strip(q, i), send_sem=b_send.at[k, i], recv_sem=b_recv.at[k, i],
            device_id=at(mate(i), tp), device_id_type=MESH)

    def edge_out(q, i):
        k = back(q)
        return pltpu.make_async_remote_copy(
            src_ref=strip(q, i, i - 1), dst_ref=strip(q, i, i - 1), send_sem=c_send.at[k, i], recv_sem=c_recv.at[k, i],
            device_id=at(mate(3 - i), tp), device_id_type=MESH)

    def edge_in(q, i):
        k = back(q)
        return pltpu.make_async_remote_copy(
            src_ref=strip(q, 3, i - 1), dst_ref=strip(q, 3, i - 1), send_sem=c_send.at[k, i], recv_sem=c_recv.at[k, i],
            device_id=at(mate(3 - i), tp), device_id_type=MESH)

    def sides(q):
        for i in near:
            side_out(q, i).start()

    corner_hops = min(2, planes - 1) if group == 4 else 0

    def edge_goes(m, action):
        if group == 4:
            if m == 0:
                action()
            elif m > corner_hops:
                when(jnp.abs(nearest(m) - plane) > corner_hops, action)

    def edges(m):
        q = nearest(m)
        for i in near:
            side_in(q, i).wait_recv()
        edge_goes(m, lambda: [edge_out(q, i).start() for i in near])

    def edges_arrive(m):
        edge_goes(m, lambda: [edge_in(nearest(m), i).wait_recv() for i in near])

    def z_up(k, p):
        ref = strip(lax.rem(p + 2 * planes, planes), 3)
        return pltpu.make_async_remote_copy(
            src_ref=ref, dst_ref=ref, send_sem=zu_send.at[k], recv_sem=zu_recv.at[k],
            device_id=at(above, tp), device_id_type=MESH)

    def z_down(k, p):
        ref = strip(lax.rem(p + 2 * planes, planes), 3)
        return pltpu.make_async_remote_copy(
            src_ref=ref, dst_ref=ref, send_sem=zd_send.at[k], recv_sem=zd_recv.at[k],
            device_id=at(below, tp), device_id_type=MESH)

    def z_relay(k):
        when(~last & (plane - k + 1 >= 0), lambda: z_up(k, plane - k + 1).start())
        when(~first & (plane + k - 1 < planes), lambda: z_down(k, plane + k - 1).start())

    def z_relayed(k):
        when(plane - k >= 0, lambda: z_up(k, plane - k).wait_recv())
        when(plane + k < planes, lambda: z_down(k, plane + k).wait_recv())

    def z_relay_left(k):
        when(~last & (plane - k + 1 >= 0), lambda: z_up(k, plane - k + 1).wait_send())
        when(~first & (plane + k - 1 < planes), lambda: z_down(k, plane + k - 1).wait_send())

    def o_relayed(k):
        def from_below():
            o_up(k, plane - k).wait_recv()

        def from_above():
            o_down(k, plane + k).wait_recv()

        when(plane - k >= 0, from_below)
        when(plane + k < planes, from_above)

    def o_sides(k):
        if near:
            when(plane - k >= 0, lambda: sides(plane - k))
            when(plane + k < planes, lambda: sides(plane + k))

    def unit(k, t):
        return pl.ds(pl.multiple_of(k * half + t * unit_rows, unit_rows), unit_rows)

    def bit(k, t, s):
        size = unit_rows // 2
        return pl.ds(pl.multiple_of(k * half + t * unit_rows + s * size, size), size)

    def tokens_out(i, k):
        return pltpu.make_async_remote_copy(
            src_ref=tok_ref.at[unit(k, tp)], dst_ref=tok_all.at[g, unit(k, tp)],
            send_sem=t_send.at[i, k], recv_sem=t_recv.at[i, k], device_id=at(mate(i), tp), device_id_type=MESH)

    def tokens_in(i, k):
        return pltpu.make_async_remote_copy(
            src_ref=tok_ref.at[unit(k, tp)], dst_ref=tok_all.at[g ^ i, unit(k, tp)],
            send_sem=t_send.at[i, k], recv_sem=t_recv.at[i, k], device_id=at(mate(i), tp), device_id_type=MESH)

    def corner_out(i, s):
        ref = tok_all.at[g ^ i, bit(i - 1, tp, s)]
        return pltpu.make_async_remote_copy(
            src_ref=ref, dst_ref=ref, send_sem=d_send.at[i, s], recv_sem=d_recv.at[i, s],
            device_id=at(mate(3 - i), tp), device_id_type=MESH)

    def corner_in(i, s):
        ref = tok_all.at[g ^ 3, bit(i - 1, tp, s)]
        return pltpu.make_async_remote_copy(
            src_ref=ref, dst_ref=ref, send_sem=d_send.at[i, s], recv_sem=d_recv.at[i, s],
            device_id=at(mate(3 - i), tp), device_id_type=MESH)

    def across(i, k, s, j):
        ref = tok_all.at[g ^ i, bit(k, tp, s)]
        return pltpu.make_async_remote_copy(
            src_ref=ref, dst_ref=ref, send_sem=f_send.at[i, k, s, j], recv_sem=f_recv.at[i, k, s, j],
            device_id=at(sp, lax.rem(tp + j, n_tp)), device_id_type=MESH)

    def across_in(i, k, s, j):
        ref = tok_all.at[g ^ i, bit(k, lax.rem(tp + n_tp - j, n_tp), s)]
        return pltpu.make_async_remote_copy(
            src_ref=ref, dst_ref=ref, send_sem=f_send.at[i, k, s, j], recv_sem=f_recv.at[i, k, s, j],
            device_id=at(sp, lax.rem(tp + j, n_tp)), device_id_type=MESH)

    def to_other_cores(i, k, s):
        for j in range(1, n_tp):
            across(i, k, s, j).start()

    def piece(i, s):
        return s if i == 1 else 1 - s

    for i in range(1, group):
        for t in range(3):
            pack(t, i).wait()
        w_in_plane(i).start()
    for t in range(3):
        pack(t, 0).wait()
    if planes > 1:
        relay(1, 0)
    for s in range(2):
        for i in near:
            tokens_out(i, piece(i, s)).start()
    for i in range(1, group):
        w_in_plane_arrives(i).wait_recv()
        if planes > 1:
            relay(1, i)

    def pass_on(k, i):
        relayed(k, i)
        relay(k + 1, i)

    row = lax.broadcasted_iota(jnp.int32, (KEYS_BEHIND, 2 * KEYS_BEHIND), 0)
    col = lax.broadcasted_iota(jnp.int32, (KEYS_BEHIND, 2 * KEYS_BEHIND), 1)
    dist = KEYS_BEHIND + row - col
    band = (dist >= 0) & (dist <= KEYS_BEHIND)
    bias[0] = jnp.where(band, 0.0, neg_big)
    for number, d in enumerate(dilation_rates):
        bias[1 + number] = jnp.where(band & (base // d - KEYS_BEHIND + col >= 0), 0.0, neg_big)
    for h in range(1, far + 1):
        @pl.when(plane - h < 0)
        def _():
            ks[(far - h) * own : (far - h + 1) * own] = jnp.zeros((own, LANES), jnp.float32)
            vs[(far - h) * own : (far - h + 1) * own] = jnp.zeros((own, LANES), jnp.float32)

    if planes > 1:
        lax.fori_loop(1, planes - 1, hops(pass_on), 0)
    own_o.wait()
    if planes > 1:
        o_relay(1)
    for i in near:
        tokens_in(i, piece(i, 0)).wait_recv()
        for s in range(2):
            if group == 4:
                corner_out(i, s).start()
            to_other_cores(i, piece(i, 0), s)
    if planes > 1:
        for i in range(group):
            relayed(planes - 1, i)
    for i in near:
        tokens_in(i, piece(i, 1)).wait_recv()
        for s in range(2):
            to_other_cores(i, piece(i, 1), s)
    if near:
        sides(plane)
    own_t.wait()

    def halo_out(h, i, k):
        view = pl.ds(pl.multiple_of((g ^ i) * rows + k * half, half), half)
        return pltpu.make_async_remote_copy(
            src_ref=kv_ref.at[view], dst_ref=halo_ref.at[far - h, view],
            send_sem=h_send.at[h, i, k], recv_sem=h_recv.at[h, i, k],
            device_id=at(lax.rem(sp + h * group, n), tp), device_id_type=MESH)

    def tile(i, k):
        block = g ^ i
        x = tok_all[block, pl.ds(pl.multiple_of(k * half, half), half), :]
        w = w_all[...].reshape(-1, 3 * LANES)
        y = jnp.dot(x, w, preferred_element_type=jnp.float32).astype(jnp.bfloat16)
        start = block * rows + k * half
        to = pl.ds(pl.multiple_of(start, half), half)
        past = pl.ds(pl.multiple_of(behind + start, half), half)
        kv_ref[to, :] = y[:, LANES:]
        qs[to, :] = y[:, :LANES].astype(jnp.float32) * HEAD_SIZE ** (-0.5)
        ks[past, :] = y[:, LANES : 2 * LANES].astype(jnp.float32)
        vs[past, :] = y[:, 2 * LANES :].astype(jnp.float32)
        for h in range(1, far + 1):
            @pl.when(plane + h < planes)
            def _():
                halo_out(h, i, k).start()

    def tiles(picks, ready):
        def one(s, _):
            i, k = picks(s)
            ready(i, k)
            tile(i, k)
            return _

        lax.fori_loop(0, 2, one, 0)

    def crossed(i, k):
        for s in range(2):
            for j in range(1, n_tp):
                across_in(i, k, s, j).wait_recv()

    def o_pass(k):
        if k < planes:
            o_relayed(k)
            if k + 1 < planes:
                o_relay(k + 1)

    def o_spread(k):
        if k < planes:
            o_sides(k)

    tiles(lambda s: (0, s), lambda i, k: None)
    if group > 1:
        o_pass(1)
        o_spread(1)
    if group == 2:
        tiles(lambda s: (1, s), crossed)
    if group == 4:
        tiles(lambda s: (1 + s, s), crossed)
        tiles(lambda s: (1 + s, 1 - s), crossed)
        o_pass(2)
        for s in range(2):
            for i in near:
                corner_in(i, s).wait_recv()
                to_other_cores(3, i - 1, s)
        tiles(lambda s: (3, s), crossed)

    by_plane = group > 1
    def attention(number, begin, end, unroll):
        d = dilation_rates[number]
        step = min(KEYS_BEHIND, own // d)
        span = step + KEYS_BEHIND
        mask_at = 1 + number if begin == 0 else 0

        def block(index, _):
            cls, b = lax.rem(index, d), index // d
            start = b * (step * d) + cls
            q_at = pl.ds(start, step, stride=d) if d > 1 else pl.ds(pl.multiple_of(start, step), step)
            k_start = behind - KEYS_BEHIND * d + start
            k_at = pl.ds(k_start, span, stride=d) if d > 1 else pl.ds(pl.multiple_of(k_start, step), span)
            q = qs[q_at, :]
            k = ks[k_at, :].astype(jnp.bfloat16)
            v = vs[k_at, :].astype(jnp.bfloat16)
            v = jnp.concatenate([v, jnp.ones((span, LANES), jnp.bfloat16)], axis=1)
            low = lax.broadcasted_iota(jnp.int32, (step, LANES), 1) < HEAD_SIZE
            q2 = jnp.concatenate([jnp.where(low, q, 0.0), jnp.where(low, 0.0, q)], axis=0).astype(jnp.bfloat16)
            s = lax.dot_general(q2, k, (((1,), (1,)), ((), ())), preferred_element_type=jnp.float32)
            seen = bias[mask_at, :step, :span]
            s = s + jnp.concatenate([seen, seen], axis=0)
            top = jnp.max(s, axis=1, keepdims=True)
            p = jnp.exp(s - top)
            o = jnp.dot(p.astype(jnp.bfloat16), v, preferred_element_type=jnp.float32)
            top = jnp.where(low, top[:step], top[step:])
            den = jnp.where(low, o[:step, LANES:], o[step:, LANES:])
            o = jnp.where(low, o[:step, :LANES], o[step:, :LANES])
            if number == 0:
                top_s[q_at, :] = top
                den_s[q_at, :] = den
                acc_s[q_at, :] = o
            else:
                was = top_s[q_at, :]
                new = jnp.maximum(was, top)
                old_scale, scale = jnp.exp(was - new), jnp.exp(top - new)
                top_s[q_at, :] = new
                den_s[q_at, :] = den_s[q_at, :] * old_scale + den * scale
                acc_s[q_at, :] = acc_s[q_at, :] * old_scale + o * scale
            return _

        lax.fori_loop(begin * d, end * d, block, 0, unroll=unroll)

    counts = [own // d // min(KEYS_BEHIND, own // d) for d in dilation_rates]

    def unroll_of(trips):
        return next(u for u in (2, 3, 1) if trips % u == 0)

    def later(k, _):
        o_relayed(k)
        when(k + 1 < planes, lambda: o_relay(k + 1))
        o_sides(k)
        return _

    def before_second():
        if by_plane:
            edges(0)
        if group == 4:
            o_spread(2)
        started = {1: 1, 2: 2, 4: 3}[group]
        if started < planes:
            lax.fori_loop(started, planes, later, 0)

    def before_halo():
        edges_arrive(0)
        if corner_hops > 0:
            z_relay(1)

    for number, d in enumerate(dilation_rates):
        if counts[number] > 1:
            attention(number, 1, counts[number], unroll_of((counts[number] - 1) * d))
        if number == 0:
            before_second()
    before_halo()

    for h in range(1, far + 1):
        @pl.when(plane - h >= 0)
        def _():
            for i in range(group):
                for k in range(2):
                    halo_out(h, i, k).wait_recv()
            to = slice((far - h) * own, (far - h + 1) * own)
            ks[to] = halo_ref[far - h, :, :LANES].astype(jnp.float32)
            vs[to] = halo_ref[far - h, :, LANES:].astype(jnp.float32)

    for number, d in enumerate(dilation_rates):
        attention(number, 0, 1, unroll_of(d))
    for k in range(1, corner_hops):
        z_relayed(k)
        z_relay(k + 1)

    att[...] = (acc_s[...] / den_s[...]).astype(jnp.bfloat16)

    def att_lanes(i):
        return att_all.at[:, pl.ds(pl.multiple_of((g ^ i) * LANES, LANES), LANES)]

    def att_out(i):
        mine = pl.ds(pl.multiple_of((g ^ i) * rows, rows), rows)
        return pltpu.make_async_remote_copy(
            src_ref=att.at[mine], dst_ref=att_lanes(0), send_sem=a_send.at[i], recv_sem=a_recv.at[i],
            device_id=at(mate(i), tp), device_id_type=MESH)

    def att_in(i):
        return pltpu.make_async_remote_copy(
            src_ref=att.at[pl.ds(0, rows)], dst_ref=att_lanes(i), send_sem=a_send.at[i], recv_sem=a_recv.at[i],
            device_id=at(mate(i), tp), device_id_type=MESH)

    def lse_out(i):
        return pltpu.make_async_remote_copy(
            src_ref=lse_ref.at[g ^ i], dst_ref=lse_all.at[g], send_sem=l_send.at[i], recv_sem=l_recv.at[i],
            device_id=at(mate(i), tp), device_id_type=MESH)

    def lse_in(i):
        return pltpu.make_async_remote_copy(
            src_ref=lse_ref.at[g ^ i], dst_ref=lse_all.at[g ^ i], send_sem=l_send.at[i], recv_sem=l_recv.at[i],
            device_id=at(mate(i), tp), device_id_type=MESH)

    for i in range(1, group):
        att_out(i).start()
    own_a = pltpu.make_async_copy(att.at[pl.ds(pl.multiple_of(g * rows, rows), rows)], att_lanes(0), own_sem.at[1])
    own_a.start()
    if by_plane:
        for m in range(corner_hops + 1, planes):
            edges(m)

    for t in range(own // LANES):
        at_rows = pl.ds(t * LANES, LANES)
        lse = (top_s[at_rows, :] + jnp.log(den_s[at_rows, :])).T
        b, off = (t * LANES) // rows, (t * LANES) % rows
        for h in range(heads):
            lse_ref[b, h : h + 1, off : off + LANES] = lse[h * HEAD_SIZE : h * HEAD_SIZE + 1, :]
    for i in range(1, group):
        lse_out(i).start()
    own_l = pltpu.make_async_copy(lse_ref.at[g], lse_all.at[g], own_sem.at[2])
    own_l.start()

    own_a.wait()
    for i in range(1, group):
        att_in(i).wait_recv()

    chunks, chunk = sums.shape[0], sums.shape[2]

    def columns_of(m):
        if by_plane:
            return pl.ds(pl.multiple_of(nearest(m) * chunk, chunk), chunk)
        return pl.ds(m * chunk, chunk)

    def rows_of(j):
        return pl.ds(pl.multiple_of(lax.rem(tp + j, n_tp) * part, part), part)

    def sum_out(c, j):
        return pltpu.make_async_remote_copy(
            src_ref=sums.at[c, rows_of(j)], dst_ref=sums_in.at[j, c], send_sem=s_send.at[j, c], recv_sem=s_recv.at[j, c],
            device_id=at(sp, lax.rem(tp + j, n_tp)), device_id_type=MESH)

    def multiply(c):
        w = o_all[columns_of(c), :]
        product = lax.dot_general(att_all[...], w, (((1,), (1,)), ((), ())), preferred_element_type=jnp.float32)
        sums[c] = product.astype(jnp.bfloat16)
        for j in range(1, n_tp):
            sum_out(c, j).start()

    def add_up(c):
        total = sums[c, rows_of(0), :].astype(jnp.float32)
        for j in range(1, n_tp):
            sum_out(c, j).wait_recv()
            total += sums_in[j, c].astype(jnp.float32)
        mixed_ref[:, columns_of(c)] = total.astype(jnp.bfloat16)

    for c in range(chunks):
        if by_plane:
            if 0 < c <= corner_hops:
                for i in near:
                    side_in(nearest(c), i).wait_recv()
            if c == 1 and corner_hops > 0:
                z_relayed(corner_hops)
            if c > 0:
                edges_arrive(c)
        multiply(c)
        if c > 0:
            add_up(c - 1)
    add_up(chunks - 1)

    own_l.wait()
    for i in range(1, group):
        lse_in(i).wait_recv()
    for b in range(group):
        lse_out_ref[b * heads : (b + 1) * heads, :] = lse_all[b]

    for i in range(1, group):
        w_in_plane(i).wait_send()
        for k in range(2):
            for s in range(2):
                for j in range(1, n_tp):
                    across(i, k, s, j).wait_send()
    for i in near:
        for k in range(2):
            tokens_out(i, k).wait_send()
            if group == 4:
                corner_out(i, k).wait_send()
    if planes > 1:
        lax.fori_loop(1, planes, hops(relay_left), 0)
        lax.fori_loop(1, planes, lambda k, _: (o_relay_left(k), _)[1], 0)
    for h in range(1, far + 1):
        @pl.when(plane + h < planes)
        def _():
            for i in range(group):
                for k in range(2):
                    halo_out(h, i, k).wait_send()
    for j in range(1, n_tp):
        for c in range(chunks):
            sum_out(c, j).wait_send()
    for i in range(1, group):
        att_out(i).wait_send()
        lse_out(i).wait_send()
    if by_plane:
        for m in range(planes):
            for i in near:
                side_out(nearest(m), i).wait_send()
            edge_goes(m, lambda m=m: [edge_out(nearest(m), i).wait_send() for i in near])
        for k in range(1, corner_hops + 1):
            z_relay_left(k)


def shards(n, n_tp, tokens, w_query, w_key, w_value, w_out):
    rows, model = tokens.shape
    depth, width = w_query.shape
    slabs = width // LANES
    reach = KEYS_BEHIND * dilation_rates[-1]
    group = 1
    while group < 4 and group * rows < reach and slabs % (2 * group) == 0 and n % (2 * group) == 0:
        group *= 2
    assert slabs == group
    far = (reach + group * rows - 1) // (group * rows)
    planes = n // group
    own = group * rows
    part = rows // n_tp
    heads = LANES // HEAD_SIZE

    turned = w_out.T
    cut = w_out.shape[1]
    behind = far * own
    chunks = planes if group > 1 else (4 if (n * cut) % (4 * LANES) == 0 else 1)
    chunk = n * cut // chunks

    f32, bf16 = jnp.float32, jnp.bfloat16
    dma = pltpu.SemaphoreType.DMA
    vmem = pl.BlockSpec(memory_space=VMEM)
    mixed, lse = pl.pallas_call(
        functools.partial(layer_kernel, n, n_tp, group, far, heads),
        out_shape=(
            jax.ShapeDtypeStruct((part, n * cut), bf16),
            jax.ShapeDtypeStruct((group * heads, rows), f32),
        ),
        in_specs=[pl.BlockSpec(memory_space=pltpu.HBM)] * 5,
        out_specs=(vmem, vmem),
        scratch_shapes=[
            VMEM((group, rows, model), bf16),
            VMEM((n, depth, 3 * LANES), bf16),
            VMEM((group, depth, 3 * LANES), bf16),
            VMEM((own, 2 * LANES), bf16), VMEM((far, own, 2 * LANES), bf16),
            VMEM((n * cut, width), bf16),
            VMEM((own, LANES), f32), VMEM((behind + own, LANES), f32), VMEM((behind + own, LANES), f32),
            VMEM((1 + len(dilation_rates), KEYS_BEHIND, 2 * KEYS_BEHIND), f32),
            VMEM((own, LANES), f32), VMEM((own, LANES), f32), VMEM((own, LANES), f32),
            VMEM((own, LANES), bf16), VMEM((group, heads, rows), f32), VMEM((group, heads, rows), f32),
            VMEM((rows, group * LANES), bf16),
            VMEM((chunks, rows, chunk), bf16), VMEM((n_tp, chunks, part, chunk), bf16),
            dma((3, group)), dma((4,)),
            dma((group,)), dma((group,)),
            dma((group, planes)), dma((group, planes)),
            dma((group, planes)), dma((group, planes)),
            dma((group, 2)), dma((group, 2)),
            dma((group, 2)), dma((group, 2)),
            dma((group, 2, 2, n_tp)), dma((group, 2, 2, n_tp)),
            dma((far + 1, group, 2)), dma((far + 1, group, 2)),
            dma((planes,)), dma((planes,)), dma((planes,)), dma((planes,)),
            dma((planes, group)), dma((planes, group)),
            dma((planes, group)), dma((planes, group)),
            dma((3,)), dma((3,)), dma((3,)), dma((3,)),
            dma((group,)), dma((group,)), dma((group,)), dma((group,)),
            dma((n_tp, chunks)), dma((n_tp, chunks)),
        ],
        compiler_params=pltpu.CompilerParams(collective_id=0, has_side_effects=True, vmem_limit_bytes=46 << 20),
        cost_estimate=pl.CostEstimate(
            flops=2 * own * model * 3 * LANES, bytes_accessed=1 << 24, transcendentals=1 << 22),
        name="layer",
    )(w_query, w_key, w_value, tokens, turned)
    return mixed, lse


def solution(mesh):
    placed = (P("sp", None), P("sp", "tp"), P("sp", "tp"), P("sp", "tp"), P("tp", "sp"))
    return jax.shard_map(
        functools.partial(shards, mesh.shape["sp"], mesh.shape["tp"]),
        mesh=mesh,
        in_specs=placed,
        out_specs=(P(("sp", "tp"), None), P("tp", "sp")),
        check_vma=False,
    )
```

```python
import functools

import jax
import jax.numpy as jnp
from jax import lax
from jax.experimental import pallas as pl
from jax.experimental.pallas import tpu as pltpu
from jax.sharding import PartitionSpec as P

HEAD_SIZE = 64
KEYS_BEHIND = 128
LANES = 128

dilation_rates = (1, 4, 16)
neg_big = -1e30

MESH = pl.DeviceIdType.MESH
VMEM = pltpu.VMEM


def at(sp, tp):
    return {"sp": sp, "tp": tp}


def layer_kernel(
    n, n_tp, group, far, heads, wq_ref, wk_ref, wv_ref, tok_ref, o_ref, mixed_ref, lse_out_ref,
    tok_all, w_all, w_ref, kv_ref, halo_ref, o_all, qs, ks, vs, bias, top_s, den_s, acc_s, att, lse_ref, lse_all,
    att_all, sums, sums_in,
    pack_sem, own_sem, w1_send, w1_recv, up_send, up_recv, down_send, down_recv, t_send, t_recv, d_send, d_recv,
    f_send, f_recv, h_send, h_recv, ou_send, ou_recv, od_send, od_recv, b_send, b_recv, c_send, c_recv,
    zu_send, zu_recv, zd_send, zd_recv, a_send, a_recv, l_send, l_recv, s_send, s_recv,
):
    sp, tp = lax.axis_index("sp"), lax.axis_index("tp")
    planes = n // group
    g, plane = lax.rem(sp, group), sp // group
    rows = tok_ref.shape[0]
    own = group * rows
    base = plane * own
    half = rows // 2
    bit_rows = half // (2 * n_tp)
    part = mixed_ref.shape[0]
    cut, width = o_ref.shape
    half_cut = cut // 2
    behind = far * own

    above = lax.rem(sp + group, n)
    below = lax.rem(sp + n - group, n)

    def mate(i):
        return plane * group + (g ^ i)

    near = [i for i in (1, 2) if i < group]

    barrier = pltpu.get_barrier_semaphore()
    greeted = 0

    def greet(sp_to, tp_to):
        pl.semaphore_signal(barrier, inc=1, device_id=at(sp_to, tp_to), device_id_type=MESH)
        return 1

    for i in range(1, group):
        greeted += greet(mate(i), tp)
    if planes > 1:
        for h in range(1, max(far, 1) + 1):
            greeted += greet(lax.rem(sp + h * group, n), tp)
            greeted += greet(lax.rem(sp + n - h * group, n), tp)
    for j in range(1, n_tp):
        greeted += greet(sp, lax.rem(tp + j, n_tp))

    own_t = pltpu.make_async_copy(tok_ref, tok_all.at[g], own_sem.at[0])

    def strip(q, i, part_of=None):
        origin = q * group + (g ^ i)
        if part_of is None:
            return o_all.at[pl.ds(pl.multiple_of(origin * cut, cut), cut)]
        return o_all.at[pl.ds(pl.multiple_of(origin * cut + part_of * half_cut, half_cut), half_cut)]

    own_o = pltpu.make_async_copy(o_ref, strip(plane, 0), own_sem.at[3])

    def pack(t, i):
        source = (wq_ref, wk_ref, wv_ref)[t].at[:, pl.ds(pl.multiple_of((g ^ i) * LANES, LANES), LANES)]
        lanes = pl.ds(t * LANES, LANES)
        to = w_all.at[sp, :, lanes] if i == 0 else w_ref.at[i, :, lanes]
        return pltpu.make_async_copy(source, to, pack_sem.at[t, i])

    for i in list(range(1, group)) + [0]:
        for t in range(3):
            pack(t, i).start()
    own_o.start()
    own_t.start()
    pl.semaphore_wait(barrier, greeted)

    def w_in_plane(i):
        return pltpu.make_async_remote_copy(
            src_ref=w_ref.at[i], dst_ref=w_all.at[sp], send_sem=w1_send.at[i], recv_sem=w1_recv.at[i],
            device_id=at(mate(i), tp), device_id_type=MESH)

    def w_in_plane_arrives(i):
        return pltpu.make_async_remote_copy(
            src_ref=w_ref.at[i], dst_ref=w_all.at[mate(i)], send_sem=w1_send.at[i], recv_sem=w1_recv.at[i],
            device_id=at(mate(i), tp), device_id_type=MESH)

    def slab(p, i):
        return w_all.at[lax.rem(p + 2 * planes, planes) * group + (g ^ i)]

    def up(i, k, p):
        return pltpu.make_async_remote_copy(
            src_ref=slab(p, i), dst_ref=slab(p, i), send_sem=up_send.at[i, k], recv_sem=up_recv.at[i, k],
            device_id=at(above, tp), device_id_type=MESH)

    def down(i, k, p):
        return pltpu.make_async_remote_copy(
            src_ref=slab(p, i), dst_ref=slab(p, i), send_sem=down_send.at[i, k], recv_sem=down_recv.at[i, k],
            device_id=at(below, tp), device_id_type=MESH)

    def o_up(k, p):
        ref = strip(lax.rem(p + 2 * planes, planes), 0)
        return pltpu.make_async_remote_copy(
            src_ref=ref, dst_ref=ref, send_sem=ou_send.at[k], recv_sem=ou_recv.at[k],
            device_id=at(above, tp), device_id_type=MESH)

    def o_down(k, p):
        ref = strip(lax.rem(p + 2 * planes, planes), 0)
        return pltpu.make_async_remote_copy(
            src_ref=ref, dst_ref=ref, send_sem=od_send.at[k], recv_sem=od_recv.at[k],
            device_id=at(below, tp), device_id_type=MESH)

    def when(condition, action):
        @pl.when(condition)
        def _():
            action()

    first, last = plane == 0, plane == planes - 1

    def relay(k, i):
        when(~last & (plane - k + 1 >= 0), lambda: up(i, k, plane - k + 1).start())
        when(~first & (plane + k - 1 < planes), lambda: down(i, k, plane + k - 1).start())

    def relayed(k, i):
        when(plane - k >= 0, lambda: up(i, k, plane - k).wait_recv())
        when(plane + k < planes, lambda: down(i, k, plane + k).wait_recv())

    def relay_left(k, i):
        when(~last & (plane - k + 1 >= 0), lambda: up(i, k, plane - k + 1).wait_send())
        when(~first & (plane + k - 1 < planes), lambda: down(i, k, plane + k - 1).wait_send())

    def o_relay(k):
        when(~last & (plane - k + 1 >= 0), lambda: o_up(k, plane - k + 1).start())
        when(~first & (plane + k - 1 < planes), lambda: o_down(k, plane + k - 1).start())

    def o_relay_left(k):
        when(~last & (plane - k + 1 >= 0), lambda: o_up(k, plane - k + 1).wait_send())
        when(~first & (plane + k - 1 < planes), lambda: o_down(k, plane + k - 1).wait_send())

    def hops(body):
        def one(k, _):
            for i in range(group):
                body(k, i)
            return _

        return one

    def nearest(m):
        left, right = plane, planes - 1 - plane
        short = jnp.minimum(left, right)
        zigzag = plane + (m // 2 if m % 2 == 0 else -((m + 1) // 2))
        return jnp.where(m <= 2 * short, zigzag, jnp.where(left < right, m, planes - 1 - m))

    def back(q):
        return lax.rem(plane - q + planes, planes)

    def side_out(q, i):
        k = back(q)
        return pltpu.make_async_remote_copy(
            src_ref=strip(q, 0), dst_ref=strip(q, 0), send_sem=b_send.at[k, i], recv_sem=b_recv.at[k, i],
            device_id=at(mate(i), tp), device_id_type=MESH)

    def side_in(q, i):
        k = back(q)
        return pltpu.make_async_remote_copy(
            src_ref=strip(q, i), dst_ref=strip(q, i), send_sem=b_send.at[k, i], recv_sem=b_recv.at[k, i],
            device_id=at(mate(i), tp), device_id_type=MESH)

    def edge_out(q, i):
        k = back(q)
        return pltpu.make_async_remote_copy(
            src_ref=strip(q, i, i - 1), dst_ref=strip(q, i, i - 1), send_sem=c_send.at[k, i], recv_sem=c_recv.at[k, i],
            device_id=at(mate(3 - i), tp), device_id_type=MESH)

    def edge_in(q, i):
        k = back(q)
        return pltpu.make_async_remote_copy(
            src_ref=strip(q, 3, i - 1), dst_ref=strip(q, 3, i - 1), send_sem=c_send.at[k, i], recv_sem=c_recv.at[k, i],
            device_id=at(mate(3 - i), tp), device_id_type=MESH)

    def sides(m):
        for i in near:
            side_out(nearest(m), i).start()

    corner_hops = min(2, planes - 1) if group == 4 else 0

    def edge_goes(m, action):
        if group == 4:
            if m == 0:
                action()
            elif m > corner_hops:
                when(jnp.abs(nearest(m) - plane) > corner_hops, action)

    def edges(m):
        for i in near:
            side_in(nearest(m), i).wait_recv()
        edge_goes(m, lambda: [edge_out(nearest(m), i).start() for i in near])

    def edges_arrive(m):
        edge_goes(m, lambda: [edge_in(nearest(m), i).wait_recv() for i in near])

    def z_up(k, p):
        ref = strip(lax.rem(p + 2 * planes, planes), 3)
        return pltpu.make_async_remote_copy(
            src_ref=ref, dst_ref=ref, send_sem=zu_send.at[k], recv_sem=zu_recv.at[k],
            device_id=at(above, tp), device_id_type=MESH)

    def z_down(k, p):
        ref = strip(lax.rem(p + 2 * planes, planes), 3)
        return pltpu.make_async_remote_copy(
            src_ref=ref, dst_ref=ref, send_sem=zd_send.at[k], recv_sem=zd_recv.at[k],
            device_id=at(below, tp), device_id_type=MESH)

    def z_relay(k):
        when(~last & (plane - k + 1 >= 0), lambda: z_up(k, plane - k + 1).start())
        when(~first & (plane + k - 1 < planes), lambda: z_down(k, plane + k - 1).start())

    def z_forward(k):
        def up_on():
            z_up(k, plane - k).wait_recv()
            z_up(k + 1, plane - k).start()

        def down_on():
            z_down(k, plane + k).wait_recv()
            z_down(k + 1, plane + k).start()

        when(~last & (plane - k >= 0), up_on)
        when(~first & (plane + k < planes), down_on)

    def z_relayed(k):
        ends = (True, True) if k == corner_hops else (last, first)
        when(ends[0] & (plane - k >= 0), lambda: z_up(k, plane - k).wait_recv())
        when(ends[1] & (plane + k < planes), lambda: z_down(k, plane + k).wait_recv())

    def z_relay_left(k):
        when(~last & (plane - k + 1 >= 0), lambda: z_up(k, plane - k + 1).wait_send())
        when(~first & (plane + k - 1 < planes), lambda: z_down(k, plane + k - 1).wait_send())

    def o_relayed(k):
        def from_below():
            o_up(k, plane - k).wait_recv()

        def from_above():
            o_down(k, plane + k).wait_recv()

        when(plane - k >= 0, from_below)
        when(plane + k < planes, from_above)

    def bit(s, p, t):
        return pl.ds(pl.multiple_of(s * half + (p * n_tp + t) * bit_rows, bit_rows), bit_rows)

    def tokens_out(i, p, s):
        return pltpu.make_async_remote_copy(
            src_ref=tok_ref.at[bit(s, p, tp)], dst_ref=tok_all.at[g, bit(s, p, tp)],
            send_sem=t_send.at[i, p, s], recv_sem=t_recv.at[i, p, s], device_id=at(mate(i), tp), device_id_type=MESH)

    def tokens_in(i, p, s):
        return pltpu.make_async_remote_copy(
            src_ref=tok_ref.at[bit(s, p, tp)], dst_ref=tok_all.at[g ^ i, bit(s, p, tp)],
            send_sem=t_send.at[i, p, s], recv_sem=t_recv.at[i, p, s], device_id=at(mate(i), tp), device_id_type=MESH)

    def corner_out(i, s):
        ref = tok_all.at[g ^ i, bit(s, i - 1, tp)]
        return pltpu.make_async_remote_copy(
            src_ref=ref, dst_ref=ref, send_sem=d_send.at[i, s], recv_sem=d_recv.at[i, s],
            device_id=at(mate(3 - i), tp), device_id_type=MESH)

    def corner_in(i, s):
        ref = tok_all.at[g ^ 3, bit(s, i - 1, tp)]
        return pltpu.make_async_remote_copy(
            src_ref=ref, dst_ref=ref, send_sem=d_send.at[i, s], recv_sem=d_recv.at[i, s],
            device_id=at(mate(3 - i), tp), device_id_type=MESH)

    def across(i, p, s, j):
        ref = tok_all.at[g ^ i, bit(s, p, tp)]
        return pltpu.make_async_remote_copy(
            src_ref=ref, dst_ref=ref, send_sem=f_send.at[i, p, s, j], recv_sem=f_recv.at[i, p, s, j],
            device_id=at(sp, lax.rem(tp + j, n_tp)), device_id_type=MESH)

    def across_in(i, p, s, j):
        ref = tok_all.at[g ^ i, bit(s, p, lax.rem(tp + n_tp - j, n_tp))]
        return pltpu.make_async_remote_copy(
            src_ref=ref, dst_ref=ref, send_sem=f_send.at[i, p, s, j], recv_sem=f_recv.at[i, p, s, j],
            device_id=at(sp, lax.rem(tp + j, n_tp)), device_id_type=MESH)

    def to_other_cores(i, p, s):
        for j in range(1, n_tp):
            across(i, p, s, j).start()

    def piece(i, step):
        return step if i == 1 else 1 - step

    for i in range(1, group):
        for t in range(3):
            pack(t, i).wait()
        w_in_plane(i).start()
    for t in range(3):
        pack(t, 0).wait()
    if planes > 1:
        relay(1, 0)
    for step in range(2):
        for s in range(2):
            for i in near:
                tokens_out(i, piece(i, step), s).start()
    for i in range(1, group):
        w_in_plane_arrives(i).wait_recv()
        if planes > 1:
            relay(1, i)

    def pass_on(k, i):
        relayed(k, i)
        relay(k + 1, i)

    row = lax.broadcasted_iota(jnp.int32, (KEYS_BEHIND, 2 * KEYS_BEHIND), 0)
    col = lax.broadcasted_iota(jnp.int32, (KEYS_BEHIND, 2 * KEYS_BEHIND), 1)
    dist = KEYS_BEHIND + row - col
    band = (dist >= 0) & (dist <= KEYS_BEHIND)
    bias[0] = jnp.where(band, 0.0, neg_big)
    for number, d in enumerate(dilation_rates):
        bias[1 + number] = jnp.where(band & (base // d - KEYS_BEHIND + col >= 0), 0.0, neg_big)
    for h in range(1, far + 1):
        @pl.when(plane - h < 0)
        def _():
            ks[(far - h) * own : (far - h + 1) * own] = jnp.zeros((own, LANES), jnp.float32)
            vs[(far - h) * own : (far - h + 1) * own] = jnp.zeros((own, LANES), jnp.float32)

    if planes > 1:
        lax.fori_loop(1, planes - 1, hops(pass_on), 0)
    own_o.wait()
    if planes > 1:
        o_relay(1)
    for s in range(2):
        for i in near:
            tokens_in(i, piece(i, 0), s).wait_recv()
            if group == 4:
                corner_out(i, s).start()
            to_other_cores(i, piece(i, 0), s)
    if planes > 1:
        for i in range(group):
            relayed(planes - 1, i)
    for s in range(2):
        for i in near:
            tokens_in(i, piece(i, 1), s).wait_recv()
            to_other_cores(i, piece(i, 1), s)
    if near:
        sides(0)
    own_t.wait()

    def halo_out(h, i, k):
        view = pl.ds(pl.multiple_of((g ^ i) * rows + k * half, half), half)
        return pltpu.make_async_remote_copy(
            src_ref=kv_ref.at[view], dst_ref=halo_ref.at[far - h, view],
            send_sem=h_send.at[h, i, k], recv_sem=h_recv.at[h, i, k],
            device_id=at(lax.rem(sp + h * group, n), tp), device_id_type=MESH)

    def tile(i, k):
        block = g ^ i
        x = tok_all[block, pl.ds(pl.multiple_of(k * half, half), half), :]
        w = w_all[...].reshape(-1, 3 * LANES)
        y = jnp.dot(x, w, preferred_element_type=jnp.float32).astype(jnp.bfloat16)
        start = block * rows + k * half
        to = pl.ds(pl.multiple_of(start, half), half)
        past = pl.ds(pl.multiple_of(behind + start, half), half)
        kv_ref[to, :] = y[:, LANES:]
        qs[to, :] = y[:, :LANES].astype(jnp.float32) * HEAD_SIZE ** (-0.5)
        ks[past, :] = y[:, LANES : 2 * LANES].astype(jnp.float32)
        vs[past, :] = y[:, 2 * LANES :].astype(jnp.float32)
        for h in range(1, far + 1):
            @pl.when(plane + h < planes)
            def _():
                halo_out(h, i, k).start()

    def tiles(picks, ready):
        def one(s, _):
            i, k = picks(s)
            ready(i, k)
            tile(i, k)
            return _

        lax.fori_loop(0, 2, one, 0)

    def crossed(i, k):
        for p in range(2):
            for j in range(1, n_tp):
                across_in(i, p, k, j).wait_recv()

    def o_pass(k):
        if k < planes:
            o_relayed(k)
            if k + 1 < planes:
                o_relay(k + 1)

    tiles(lambda s: (0, s), lambda i, k: None)
    if group > 1:
        o_pass(1)
    if group == 2:
        tiles(lambda s: (1, s), crossed)
    if group == 4:
        tiles(lambda s: (1 + s, 0), crossed)
        tiles(lambda s: (1 + s, 1), crossed)
        for s in range(2):
            for i in near:
                corner_in(i, s).wait_recv()
                to_other_cores(3, i - 1, s)
            crossed(3, s)
            tile(3, s)
            if s == 0:
                o_pass(2)

    by_plane = group > 1
    def attention(number, begin, end, unroll):
        d = dilation_rates[number]
        step = min(KEYS_BEHIND, own // d)
        span = step + KEYS_BEHIND
        mask_at = 1 + number if begin == 0 else 0

        def block(index, _):
            cls, b = lax.rem(index, d), index // d
            start = b * (step * d) + cls
            q_at = pl.ds(start, step, stride=d) if d > 1 else pl.ds(pl.multiple_of(start, step), step)
            k_start = behind - KEYS_BEHIND * d + start
            k_at = pl.ds(k_start, span, stride=d) if d > 1 else pl.ds(pl.multiple_of(k_start, step), span)
            q = qs[q_at, :]
            k = ks[k_at, :].astype(jnp.bfloat16)
            v = vs[k_at, :].astype(jnp.bfloat16)
            v = jnp.concatenate([v, jnp.ones((span, LANES), jnp.bfloat16)], axis=1)
            low = lax.broadcasted_iota(jnp.int32, (step, LANES), 1) < HEAD_SIZE
            q2 = jnp.concatenate([jnp.where(low, q, 0.0), jnp.where(low, 0.0, q)], axis=0).astype(jnp.bfloat16)
            s = lax.dot_general(q2, k, (((1,), (1,)), ((), ())), preferred_element_type=jnp.float32)
            seen = bias[mask_at, :step, :span]
            s = s + jnp.concatenate([seen, seen], axis=0)
            top = jnp.max(s, axis=1, keepdims=True)
            p = jnp.exp(s - top)
            o = jnp.dot(p.astype(jnp.bfloat16), v, preferred_element_type=jnp.float32)
            top = jnp.where(low, top[:step], top[step:])
            den = jnp.where(low, o[:step, LANES:], o[step:, LANES:])
            o = jnp.where(low, o[:step, :LANES], o[step:, :LANES])
            if number == 0:
                top_s[q_at, :] = top
                den_s[q_at, :] = den
                acc_s[q_at, :] = o
            else:
                was = top_s[q_at, :]
                new = jnp.maximum(was, top)
                old_scale, scale = jnp.exp(was - new), jnp.exp(top - new)
                top_s[q_at, :] = new
                den_s[q_at, :] = den_s[q_at, :] * old_scale + den * scale
                acc_s[q_at, :] = acc_s[q_at, :] * old_scale + o * scale
            return _

        lax.fori_loop(begin * d, end * d, block, 0, unroll=unroll)

    counts = [own // d // min(KEYS_BEHIND, own // d) for d in dilation_rates]

    def unroll_of(trips):
        return next(u for u in (2, 3, 1) if trips % u == 0)

    strips = list(range(planes)) if by_plane else []
    if 0 < corner_hops < planes - 1:
        strips.remove(corner_hops)
        strips.append(corner_hops)
    early, late = strips[1:3], strips[3:]

    def later(k, _):
        o_relayed(k)
        when(k + 1 < planes, lambda: o_relay(k + 1))
        return _

    def before_second():
        if by_plane:
            edges(0)
            for m in early[:1]:
                sides(m)

    def before_halo():
        started = {1: 1, 2: 2, 4: 3}[group]
        if started < planes:
            lax.fori_loop(started, planes, later, 0)
        for m in early[1:]:
            sides(m)
        edges_arrive(0)
        if corner_hops > 0:
            z_relay(1)

    for number, d in enumerate(dilation_rates):
        if counts[number] > 1:
            attention(number, 1, counts[number], unroll_of((counts[number] - 1) * d))
        if number == 0:
            before_second()
    before_halo()

    for h in range(1, far + 1):
        @pl.when(plane - h >= 0)
        def _():
            for i in range(group):
                for k in range(2):
                    halo_out(h, i, k).wait_recv()
            to = slice((far - h) * own, (far - h + 1) * own)
            ks[to] = halo_ref[far - h, :, :LANES].astype(jnp.float32)
            vs[to] = halo_ref[far - h, :, LANES:].astype(jnp.float32)

    for number, d in enumerate(dilation_rates):
        if number == 2:
            for m in late:
                sides(m)
        attention(number, 0, 1, unroll_of(d))
    for k in range(1, corner_hops):
        z_forward(k)

    att[...] = (acc_s[...] / den_s[...]).astype(jnp.bfloat16)

    def att_lanes(i):
        return att_all.at[:, pl.ds(pl.multiple_of((g ^ i) * LANES, LANES), LANES)]

    def att_out(i):
        mine = pl.ds(pl.multiple_of((g ^ i) * rows, rows), rows)
        return pltpu.make_async_remote_copy(
            src_ref=att.at[mine], dst_ref=att_lanes(0), send_sem=a_send.at[i], recv_sem=a_recv.at[i],
            device_id=at(mate(i), tp), device_id_type=MESH)

    def att_in(i):
        return pltpu.make_async_remote_copy(
            src_ref=att.at[pl.ds(0, rows)], dst_ref=att_lanes(i), send_sem=a_send.at[i], recv_sem=a_recv.at[i],
            device_id=at(mate(i), tp), device_id_type=MESH)

    def lse_out(i):
        return pltpu.make_async_remote_copy(
            src_ref=lse_ref.at[g ^ i], dst_ref=lse_all.at[g], send_sem=l_send.at[i], recv_sem=l_recv.at[i],
            device_id=at(mate(i), tp), device_id_type=MESH)

    def lse_in(i):
        return pltpu.make_async_remote_copy(
            src_ref=lse_ref.at[g ^ i], dst_ref=lse_all.at[g ^ i], send_sem=l_send.at[i], recv_sem=l_recv.at[i],
            device_id=at(mate(i), tp), device_id_type=MESH)

    for i in range(1, group):
        att_out(i).start()
    own_a = pltpu.make_async_copy(att.at[pl.ds(pl.multiple_of(g * rows, rows), rows)], att_lanes(0), own_sem.at[1])
    own_a.start()
    for m in early:
        edges(m)

    for t in range(own // LANES):
        at_rows = pl.ds(t * LANES, LANES)
        lse = (top_s[at_rows, :] + jnp.log(den_s[at_rows, :])).T
        b, off = (t * LANES) // rows, (t * LANES) % rows
        for h in range(heads):
            lse_ref[b, h : h + 1, off : off + LANES] = lse[h * HEAD_SIZE : h * HEAD_SIZE + 1, :]
    for i in range(1, group):
        lse_out(i).start()
    own_l = pltpu.make_async_copy(lse_ref.at[g], lse_all.at[g], own_sem.at[2])
    own_l.start()

    own_a.wait()
    for i in range(1, group):
        att_in(i).wait_recv()

    chunks, chunk = sums.shape[0], sums.shape[2]

    per_strip = chunks // planes if by_plane else 1

    def columns_of(c):
        if by_plane:
            m, side = strips[c // per_strip], c % per_strip
            side = side ^ (g // (group // per_strip)) if per_strip > 1 else 0
            return pl.ds(pl.multiple_of((nearest(m) * per_strip + side) * chunk, chunk), chunk)
        return pl.ds(c * chunk, chunk)

    def rows_of(j):
        return pl.ds(pl.multiple_of(lax.rem(tp + j, n_tp) * part, part), part)

    def sum_out(c, j):
        return pltpu.make_async_remote_copy(
            src_ref=sums.at[c, rows_of(j)], dst_ref=sums_in.at[j, c], send_sem=s_send.at[j, c], recv_sem=s_recv.at[j, c],
            device_id=at(sp, lax.rem(tp + j, n_tp)), device_id_type=MESH)

    def multiply(c):
        w = o_all[columns_of(c), :]
        product = lax.dot_general(att_all[...], w, (((1,), (1,)), ((), ())), preferred_element_type=jnp.float32)
        sums[c] = product.astype(jnp.bfloat16)
        for j in range(1, n_tp):
            sum_out(c, j).start()

    def add_up(c):
        total = sums[c, rows_of(0), :].astype(jnp.float32)
        for j in range(1, n_tp):
            sum_out(c, j).wait_recv()
            total += sums_in[j, c].astype(jnp.float32)
        mixed_ref[:, columns_of(c)] = total.astype(jnp.bfloat16)

    def edges_arrive_late(m):
        if m > 0:
            edges_arrive(m)
        if m == 1 and corner_hops > 0:
            z_relayed(1)
        if m > 1 and m == strips[2] and corner_hops > 1:
            z_relayed(2)

    for c in range(chunks):
        if by_plane:
            m, side = strips[c // per_strip], c % per_strip
            if side == 0:
                if m in late:
                    edges(m)
            if side == per_strip - 1:
                edges_arrive_late(m)
        multiply(c)
        if c > 0:
            add_up(c - 1)
    add_up(chunks - 1)

    own_l.wait()
    for i in range(1, group):
        lse_in(i).wait_recv()
    for b in range(group):
        lse_out_ref[b * heads : (b + 1) * heads, :] = lse_all[b]

    for i in range(1, group):
        w_in_plane(i).wait_send()
        for k in range(2):
            for s in range(2):
                for j in range(1, n_tp):
                    across(i, k, s, j).wait_send()
    for i in near:
        for s in range(2):
            for p in range(2):
                tokens_out(i, p, s).wait_send()
            if group == 4:
                corner_out(i, s).wait_send()
    if planes > 1:
        lax.fori_loop(1, planes, hops(relay_left), 0)
        lax.fori_loop(1, planes, lambda k, _: (o_relay_left(k), _)[1], 0)
    for h in range(1, far + 1):
        @pl.when(plane + h < planes)
        def _():
            for i in range(group):
                for k in range(2):
                    halo_out(h, i, k).wait_send()
    for j in range(1, n_tp):
        for c in range(chunks):
            sum_out(c, j).wait_send()
    for i in range(1, group):
        att_out(i).wait_send()
        lse_out(i).wait_send()
    if by_plane:
        for m in range(planes):
            for i in near:
                side_out(nearest(m), i).wait_send()
            edge_goes(m, lambda m=m: [edge_out(nearest(m), i).wait_send() for i in near])
        for k in range(1, corner_hops + 1):
            z_relay_left(k)


def shards(n, n_tp, tokens, w_query, w_key, w_value, w_out):
    rows, model = tokens.shape
    depth, width = w_query.shape
    slabs = width // LANES
    reach = KEYS_BEHIND * dilation_rates[-1]
    group = 1
    while group < 4 and group * rows < reach and slabs % (2 * group) == 0 and n % (2 * group) == 0:
        group *= 2
    assert slabs == group
    far = (reach + group * rows - 1) // (group * rows)
    planes = n // group
    own = group * rows
    part = rows // n_tp
    heads = LANES // HEAD_SIZE

    turned = w_out.T
    cut = w_out.shape[1]
    behind = far * own
    chunks = planes * (2 if group == 4 and 2 * cut % LANES == 0 else 1) if group > 1 else (4 if (n * cut) % (4 * LANES) == 0 else 1)
    chunk = n * cut // chunks

    f32, bf16 = jnp.float32, jnp.bfloat16
    dma = pltpu.SemaphoreType.DMA
    vmem = pl.BlockSpec(memory_space=VMEM)
    mixed, lse = pl.pallas_call(
        functools.partial(layer_kernel, n, n_tp, group, far, heads),
        out_shape=(
            jax.ShapeDtypeStruct((part, n * cut), bf16),
            jax.ShapeDtypeStruct((group * heads, rows), f32),
        ),
        in_specs=[pl.BlockSpec(memory_space=pltpu.HBM)] * 5,
        out_specs=(vmem, vmem),
        scratch_shapes=[
            VMEM((group, rows, model), bf16),
            VMEM((n, depth, 3 * LANES), bf16),
            VMEM((group, depth, 3 * LANES), bf16),
            VMEM((own, 2 * LANES), bf16), VMEM((far, own, 2 * LANES), bf16),
            VMEM((n * cut, width), bf16),
            VMEM((own, LANES), f32), VMEM((behind + own, LANES), f32), VMEM((behind + own, LANES), f32),
            VMEM((1 + len(dilation_rates), KEYS_BEHIND, 2 * KEYS_BEHIND), f32),
            VMEM((own, LANES), f32), VMEM((own, LANES), f32), VMEM((own, LANES), f32),
            VMEM((own, LANES), bf16), VMEM((group, heads, rows), f32), VMEM((group, heads, rows), f32),
            VMEM((rows, group * LANES), bf16),
            VMEM((chunks, rows, chunk), bf16), VMEM((n_tp, chunks, part, chunk), bf16),
            dma((3, group)), dma((4,)),
            dma((group,)), dma((group,)),
            dma((group, planes)), dma((group, planes)),
            dma((group, planes)), dma((group, planes)),
            dma((group, 2, 2)), dma((group, 2, 2)),
            dma((group, 2)), dma((group, 2)),
            dma((group, 2, 2, n_tp)), dma((group, 2, 2, n_tp)),
            dma((far + 1, group, 2)), dma((far + 1, group, 2)),
            dma((planes,)), dma((planes,)), dma((planes,)), dma((planes,)),
            dma((planes, group)), dma((planes, group)),
            dma((planes, group)), dma((planes, group)),
            dma((3,)), dma((3,)), dma((3,)), dma((3,)),
            dma((group,)), dma((group,)), dma((group,)), dma((group,)),
            dma((n_tp, chunks)), dma((n_tp, chunks)),
        ],
        compiler_params=pltpu.CompilerParams(collective_id=0, has_side_effects=True, vmem_limit_bytes=46 << 20),
        cost_estimate=pl.CostEstimate(
            flops=2 * own * model * 3 * LANES, bytes_accessed=1 << 24, transcendentals=1 << 22),
        name="layer",
    )(*[pltpu.with_memory_space_constraint(x, pltpu.HBM) for x in (w_query, w_key, w_value, tokens, turned)])
    return mixed, lse


def solution(mesh):
    placed = (P("sp", None), P("sp", "tp"), P("sp", "tp"), P("sp", "tp"), P("tp", "sp"))
    return jax.shard_map(
        functools.partial(shards, mesh.shape["sp"], mesh.shape["tp"]),
        mesh=mesh,
        in_specs=placed,
        out_specs=(P(("sp", "tp"), None), P("tp", "sp")),
        check_vma=False,
    )
```

```python
import functools

import jax
import jax.numpy as jnp
from jax import lax
from jax.experimental import pallas as pl
from jax.experimental.pallas import tpu as pltpu
from jax.sharding import PartitionSpec as P

HEAD_SIZE = 64
KEYS_BEHIND = 128
LANES = 128

dilation_rates = (1, 4, 16)
neg_big = -1e30

MESH = pl.DeviceIdType.MESH
VMEM = pltpu.VMEM


def at(sp, tp):
    return {"sp": sp, "tp": tp}


def layer_kernel(
    n, n_tp, group, far, heads, wq_ref, wk_ref, wv_ref, tok_ref, o_ref, mixed_ref, lse_out_ref,
    tok_all, w_all, w_ref, kv_ref, halo_ref, o_all, qs, ks, vs, q_cls, k_cls, v_cls, out_cls, lse_cls, turn, bias,
    top_s, den_s, acc_s, att, lse_ref, lse_all, att_all, sums, sums_in,
    pack_sem, own_sem, w1_send, w1_recv, up_send, up_recv, down_send, down_recv, t_send, t_recv, d_send, d_recv,
    f_send, f_recv, h_send, h_recv, ou_send, ou_recv, od_send, od_recv, b_send, b_recv, c_send, c_recv,
    zu_send, zu_recv, zd_send, zd_recv, a_send, a_recv, l_send, l_recv, s_send, s_recv,
):
    sp, tp = lax.axis_index("sp"), lax.axis_index("tp")
    planes = n // group
    g, plane = lax.rem(sp, group), sp // group
    rows = tok_ref.shape[0]
    own = group * rows
    base = plane * own
    half = rows // 2
    bit_rows = half // (2 * n_tp)
    part = mixed_ref.shape[0]
    cut, width = o_ref.shape
    half_cut = cut // 2
    wide = dilation_rates[-1]
    behind = KEYS_BEHIND * dilation_rates[-2]
    run = half // wide
    old = far * own // wide

    above = lax.rem(sp + group, n)
    below = lax.rem(sp + n - group, n)

    def mate(i):
        return plane * group + (g ^ i)

    near = [i for i in (1, 2) if i < group]

    barrier = pltpu.get_barrier_semaphore()
    greeted = 0

    def greet(sp_to, tp_to):
        pl.semaphore_signal(barrier, inc=1, device_id=at(sp_to, tp_to), device_id_type=MESH)
        return 1

    for i in range(1, group):
        greeted += greet(mate(i), tp)
    if planes > 1:
        for h in range(1, max(far, 1) + 1):
            greeted += greet(lax.rem(sp + h * group, n), tp)
            greeted += greet(lax.rem(sp + n - h * group, n), tp)
    for j in range(1, n_tp):
        greeted += greet(sp, lax.rem(tp + j, n_tp))

    own_t = pltpu.make_async_copy(tok_ref, tok_all.at[g], own_sem.at[0])

    def strip(q, i, part_of=None):
        origin = q * group + (g ^ i)
        if part_of is None:
            return o_all.at[pl.ds(pl.multiple_of(origin * cut, cut), cut)]
        return o_all.at[pl.ds(pl.multiple_of(origin * cut + part_of * half_cut, half_cut), half_cut)]

    own_o = pltpu.make_async_copy(o_ref, strip(plane, 0), own_sem.at[3])

    def pack(t, i):
        source = (wq_ref, wk_ref, wv_ref)[t].at[:, pl.ds(pl.multiple_of((g ^ i) * LANES, LANES), LANES)]
        lanes = pl.ds(t * LANES, LANES)
        to = w_all.at[sp, :, lanes] if i == 0 else w_ref.at[i, :, lanes]
        return pltpu.make_async_copy(source, to, pack_sem.at[t, i])

    for i in list(range(1, group)) + [0]:
        for t in range(3):
            pack(t, i).start()
    own_o.start()
    own_t.start()
    pl.semaphore_wait(barrier, greeted)

    def w_in_plane(i):
        return pltpu.make_async_remote_copy(
            src_ref=w_ref.at[i], dst_ref=w_all.at[sp], send_sem=w1_send.at[i], recv_sem=w1_recv.at[i],
            device_id=at(mate(i), tp), device_id_type=MESH)

    def w_in_plane_arrives(i):
        return pltpu.make_async_remote_copy(
            src_ref=w_ref.at[i], dst_ref=w_all.at[mate(i)], send_sem=w1_send.at[i], recv_sem=w1_recv.at[i],
            device_id=at(mate(i), tp), device_id_type=MESH)

    def slab(p, i):
        return w_all.at[lax.rem(p + 2 * planes, planes) * group + (g ^ i)]

    def up(i, k, p):
        return pltpu.make_async_remote_copy(
            src_ref=slab(p, i), dst_ref=slab(p, i), send_sem=up_send.at[i, k], recv_sem=up_recv.at[i, k],
            device_id=at(above, tp), device_id_type=MESH)

    def down(i, k, p):
        return pltpu.make_async_remote_copy(
            src_ref=slab(p, i), dst_ref=slab(p, i), send_sem=down_send.at[i, k], recv_sem=down_recv.at[i, k],
            device_id=at(below, tp), device_id_type=MESH)

    def o_up(k, p):
        ref = strip(lax.rem(p + 2 * planes, planes), 0)
        return pltpu.make_async_remote_copy(
            src_ref=ref, dst_ref=ref, send_sem=ou_send.at[k], recv_sem=ou_recv.at[k],
            device_id=at(above, tp), device_id_type=MESH)

    def o_down(k, p):
        ref = strip(lax.rem(p + 2 * planes, planes), 0)
        return pltpu.make_async_remote_copy(
            src_ref=ref, dst_ref=ref, send_sem=od_send.at[k], recv_sem=od_recv.at[k],
            device_id=at(below, tp), device_id_type=MESH)

    def when(condition, action):
        @pl.when(condition)
        def _():
            action()

    first, last = plane == 0, plane == planes - 1

    def relay(k, i):
        when(~last & (plane - k + 1 >= 0), lambda: up(i, k, plane - k + 1).start())
        when(~first & (plane + k - 1 < planes), lambda: down(i, k, plane + k - 1).start())

    def relayed(k, i):
        when(plane - k >= 0, lambda: up(i, k, plane - k).wait_recv())
        when(plane + k < planes, lambda: down(i, k, plane + k).wait_recv())

    def relay_left(k, i):
        when(~last & (plane - k + 1 >= 0), lambda: up(i, k, plane - k + 1).wait_send())
        when(~first & (plane + k - 1 < planes), lambda: down(i, k, plane + k - 1).wait_send())

    def o_relay(k):
        when(~last & (plane - k + 1 >= 0), lambda: o_up(k, plane - k + 1).start())
        when(~first & (plane + k - 1 < planes), lambda: o_down(k, plane + k - 1).start())

    def o_relay_left(k):
        when(~last & (plane - k + 1 >= 0), lambda: o_up(k, plane - k + 1).wait_send())
        when(~first & (plane + k - 1 < planes), lambda: o_down(k, plane + k - 1).wait_send())

    def hops(body):
        def one(k, _):
            for i in range(group):
                body(k, i)
            return _

        return one

    def nearest(m):
        left, right = plane, planes - 1 - plane
        short = jnp.minimum(left, right)
        zigzag = plane + (m // 2 if m % 2 == 0 else -((m + 1) // 2))
        return jnp.where(m <= 2 * short, zigzag, jnp.where(left < right, m, planes - 1 - m))

    def back(q):
        return lax.rem(plane - q + planes, planes)

    def side_out(q, i):
        k = back(q)
        return pltpu.make_async_remote_copy(
            src_ref=strip(q, 0), dst_ref=strip(q, 0), send_sem=b_send.at[k, i], recv_sem=b_recv.at[k, i],
            device_id=at(mate(i), tp), device_id_type=MESH)

    def side_in(q, i):
        k = back(q)
        return pltpu.make_async_remote_copy(
            src_ref=strip(q, i), dst_ref=strip(q, i), send_sem=b_send.at[k, i], recv_sem=b_recv.at[k, i],
            device_id=at(mate(i), tp), device_id_type=MESH)

    def edge_out(q, i):
        k = back(q)
        return pltpu.make_async_remote_copy(
            src_ref=strip(q, i, i - 1), dst_ref=strip(q, i, i - 1), send_sem=c_send.at[k, i], recv_sem=c_recv.at[k, i],
            device_id=at(mate(3 - i), tp), device_id_type=MESH)

    def edge_in(q, i):
        k = back(q)
        return pltpu.make_async_remote_copy(
            src_ref=strip(q, 3, i - 1), dst_ref=strip(q, 3, i - 1), send_sem=c_send.at[k, i], recv_sem=c_recv.at[k, i],
            device_id=at(mate(3 - i), tp), device_id_type=MESH)

    def sides(m):
        for i in near:
            side_out(nearest(m), i).start()

    corner_hops = min(2, planes - 1) if group == 4 else 0

    def edge_goes(m, action):
        if group == 4:
            if m == 0:
                action()
            elif m > corner_hops:
                when(jnp.abs(nearest(m) - plane) > corner_hops, action)

    def edges(m):
        for i in near:
            side_in(nearest(m), i).wait_recv()
        edge_goes(m, lambda: [edge_out(nearest(m), i).start() for i in near])

    def edges_arrive(m):
        edge_goes(m, lambda: [edge_in(nearest(m), i).wait_recv() for i in near])

    def z_up(k, p):
        ref = strip(lax.rem(p + 2 * planes, planes), 3)
        return pltpu.make_async_remote_copy(
            src_ref=ref, dst_ref=ref, send_sem=zu_send.at[k], recv_sem=zu_recv.at[k],
            device_id=at(above, tp), device_id_type=MESH)

    def z_down(k, p):
        ref = strip(lax.rem(p + 2 * planes, planes), 3)
        return pltpu.make_async_remote_copy(
            src_ref=ref, dst_ref=ref, send_sem=zd_send.at[k], recv_sem=zd_recv.at[k],
            device_id=at(below, tp), device_id_type=MESH)

    def z_relay(k):
        when(~last & (plane - k + 1 >= 0), lambda: z_up(k, plane - k + 1).start())
        when(~first & (plane + k - 1 < planes), lambda: z_down(k, plane + k - 1).start())

    def z_forward(k):
        def up_on():
            z_up(k, plane - k).wait_recv()
            z_up(k + 1, plane - k).start()

        def down_on():
            z_down(k, plane + k).wait_recv()
            z_down(k + 1, plane + k).start()

        when(~last & (plane - k >= 0), up_on)
        when(~first & (plane + k < planes), down_on)

    def z_relayed(k):
        ends = (True, True) if k == corner_hops else (last, first)
        when(ends[0] & (plane - k >= 0), lambda: z_up(k, plane - k).wait_recv())
        when(ends[1] & (plane + k < planes), lambda: z_down(k, plane + k).wait_recv())

    def z_relay_left(k):
        when(~last & (plane - k + 1 >= 0), lambda: z_up(k, plane - k + 1).wait_send())
        when(~first & (plane + k - 1 < planes), lambda: z_down(k, plane + k - 1).wait_send())

    def o_relayed(k):
        def from_below():
            o_up(k, plane - k).wait_recv()

        def from_above():
            o_down(k, plane + k).wait_recv()

        when(plane - k >= 0, from_below)
        when(plane + k < planes, from_above)

    def bit(s, p, t):
        return pl.ds(pl.multiple_of(s * half + (p * n_tp + t) * bit_rows, bit_rows), bit_rows)

    def tokens_out(i, p, s):
        return pltpu.make_async_remote_copy(
            src_ref=tok_ref.at[bit(s, p, tp)], dst_ref=tok_all.at[g, bit(s, p, tp)],
            send_sem=t_send.at[i, p, s], recv_sem=t_recv.at[i, p, s], device_id=at(mate(i), tp), device_id_type=MESH)

    def tokens_in(i, p, s):
        return pltpu.make_async_remote_copy(
            src_ref=tok_ref.at[bit(s, p, tp)], dst_ref=tok_all.at[g ^ i, bit(s, p, tp)],
            send_sem=t_send.at[i, p, s], recv_sem=t_recv.at[i, p, s], device_id=at(mate(i), tp), device_id_type=MESH)

    def corner_out(i, s):
        ref = tok_all.at[g ^ i, bit(s, i - 1, tp)]
        return pltpu.make_async_remote_copy(
            src_ref=ref, dst_ref=ref, send_sem=d_send.at[i, s], recv_sem=d_recv.at[i, s],
            device_id=at(mate(3 - i), tp), device_id_type=MESH)

    def corner_in(i, s):
        ref = tok_all.at[g ^ 3, bit(s, i - 1, tp)]
        return pltpu.make_async_remote_copy(
            src_ref=ref, dst_ref=ref, send_sem=d_send.at[i, s], recv_sem=d_recv.at[i, s],
            device_id=at(mate(3 - i), tp), device_id_type=MESH)

    def across(i, p, s, j):
        ref = tok_all.at[g ^ i, bit(s, p, tp)]
        return pltpu.make_async_remote_copy(
            src_ref=ref, dst_ref=ref, send_sem=f_send.at[i, p, s, j], recv_sem=f_recv.at[i, p, s, j],
            device_id=at(sp, lax.rem(tp + j, n_tp)), device_id_type=MESH)

    def across_in(i, p, s, j):
        ref = tok_all.at[g ^ i, bit(s, p, lax.rem(tp + n_tp - j, n_tp))]
        return pltpu.make_async_remote_copy(
            src_ref=ref, dst_ref=ref, send_sem=f_send.at[i, p, s, j], recv_sem=f_recv.at[i, p, s, j],
            device_id=at(sp, lax.rem(tp + j, n_tp)), device_id_type=MESH)

    def to_other_cores(i, p, s):
        for j in range(1, n_tp):
            across(i, p, s, j).start()

    def piece(i, step):
        return step if i == 1 else 1 - step

    for i in range(1, group):
        for t in range(3):
            pack(t, i).wait()
        w_in_plane(i).start()
    for t in range(3):
        pack(t, 0).wait()
    if planes > 1:
        relay(1, 0)
    for step in range(2):
        for s in range(2):
            for i in near:
                tokens_out(i, piece(i, step), s).start()
    for i in range(1, group):
        w_in_plane_arrives(i).wait_recv()
        if planes > 1:
            relay(1, i)

    def pass_on(k, i):
        relayed(k, i)
        relay(k + 1, i)

    row = lax.broadcasted_iota(jnp.int32, (KEYS_BEHIND, 2 * KEYS_BEHIND), 0)
    col = lax.broadcasted_iota(jnp.int32, (KEYS_BEHIND, 2 * KEYS_BEHIND), 1)
    dist = KEYS_BEHIND + row - col
    band = (dist >= 0) & (dist <= KEYS_BEHIND)
    bias[0] = jnp.where(band, 0.0, neg_big)
    for number, d in enumerate(dilation_rates):
        bias[1 + number] = jnp.where(band & (base // d - KEYS_BEHIND + col >= 0), 0.0, neg_big)
    to_row = lax.broadcasted_iota(jnp.int32, (half, half), 0)
    from_row = lax.broadcasted_iota(jnp.int32, (half, half), 1)
    turn[0] = (from_row == to_row % run * wide + to_row // run).astype(jnp.float32).astype(jnp.bfloat16)
    turn[1] = (from_row == to_row % wide * run + to_row // wide).astype(jnp.float32).astype(jnp.bfloat16)

    @pl.when(plane == 0)
    def _():
        ks[:behind] = jnp.zeros((behind, LANES), jnp.float32)
        vs[:behind] = jnp.zeros((behind, LANES), jnp.float32)

    for h in range(1, far + 1):
        @pl.when(plane - h < 0)
        def _():
            gone = slice((far - h) * own // wide, (far - h + 1) * own // wide)
            k_cls[:, gone] = jnp.zeros((wide, own // wide, LANES), jnp.bfloat16)
            v_cls[:, gone] = jnp.zeros((wide, own // wide, LANES), jnp.bfloat16)

    if planes > 1:
        lax.fori_loop(1, planes - 1, hops(pass_on), 0)
    own_o.wait()
    if planes > 1:
        o_relay(1)
    for s in range(2):
        for i in near:
            tokens_in(i, piece(i, 0), s).wait_recv()
            if group == 4:
                corner_out(i, s).start()
            to_other_cores(i, piece(i, 0), s)
    if planes > 1:
        for i in range(group):
            relayed(planes - 1, i)
    for s in range(2):
        for i in near:
            tokens_in(i, piece(i, 1), s).wait_recv()
            to_other_cores(i, piece(i, 1), s)
    if near:
        sides(0)
    own_t.wait()

    def halo_out(h, i, k):
        view = pl.ds(pl.multiple_of((g ^ i) * rows + k * half, half), half)
        return pltpu.make_async_remote_copy(
            src_ref=kv_ref.at[view], dst_ref=halo_ref.at[far - h, view],
            send_sem=h_send.at[h, i, k], recv_sem=h_recv.at[h, i, k],
            device_id=at(lax.rem(sp + h * group, n), tp), device_id_type=MESH)

    def by_classes(y):
        sorted_rows = jnp.dot(turn[0], y, preferred_element_type=jnp.float32).astype(jnp.bfloat16)
        return sorted_rows.reshape(wide, run, y.shape[1])

    def tile(i, k):
        block = g ^ i
        x = tok_all[block, pl.ds(pl.multiple_of(k * half, half), half), :]
        w = w_all[...].reshape(-1, 3 * LANES)
        y = jnp.dot(x, w, preferred_element_type=jnp.float32).astype(jnp.bfloat16)
        start = block * rows + k * half
        to = pl.ds(pl.multiple_of(start, half), half)
        past = pl.ds(pl.multiple_of(behind + start, half), half)
        kv_ref[to, :] = y[:, LANES:]
        qs[to, :] = y[:, :LANES].astype(jnp.float32) * HEAD_SIZE ** (-0.5)
        ks[past, :] = y[:, LANES : 2 * LANES].astype(jnp.float32)
        vs[past, :] = y[:, 2 * LANES :].astype(jnp.float32)
        by_class = by_classes(y)
        at_run = pl.ds(pl.multiple_of(start // wide, run), run)
        q_cls[:, at_run, :] = by_class[:, :, :LANES] * HEAD_SIZE ** (-0.5)
        past_run = pl.ds(pl.multiple_of(old + start // wide, run), run)
        k_cls[:, past_run, :] = by_class[:, :, LANES : 2 * LANES]
        v_cls[:, past_run, :] = by_class[:, :, 2 * LANES :]
        for h in range(1, far + 1):
            @pl.when(plane + h < planes)
            def _():
                halo_out(h, i, k).start()

    def tiles(picks, ready):
        def one(s, _):
            i, k = picks(s)
            ready(i, k)
            tile(i, k)
            return _

        lax.fori_loop(0, 2, one, 0)

    def crossed(i, k):
        for p in range(2):
            for j in range(1, n_tp):
                across_in(i, p, k, j).wait_recv()

    def o_pass(k):
        if k < planes:
            o_relayed(k)
            if k + 1 < planes:
                o_relay(k + 1)

    tiles(lambda s: (0, s), lambda i, k: None)
    if group > 1:
        o_pass(1)
    if group == 2:
        tiles(lambda s: (1, s), crossed)
    if group == 4:
        tiles(lambda s: (1 + s, 0), crossed)
        tiles(lambda s: (1 + s, 1), crossed)
        for s in range(2):
            for i in near:
                corner_in(i, s).wait_recv()
                to_other_cores(3, i - 1, s)
            crossed(3, s)
            tile(3, s)
            if s == 0:
                o_pass(2)

    by_plane = group > 1
    def attention(number, begin, end, unroll):
        d = dilation_rates[number]
        step = min(KEYS_BEHIND, own // d)
        span = step + KEYS_BEHIND
        mask_at = 1 + number if begin == 0 else 0

        def block(index, _):
            cls, b = lax.rem(index, d), index // d
            start = b * (step * d) + cls
            q_at = pl.ds(start, step, stride=d) if d > 1 else pl.ds(pl.multiple_of(start, step), step)
            k_start = behind - KEYS_BEHIND * d + start
            k_at = pl.ds(k_start, span, stride=d) if d > 1 else pl.ds(pl.multiple_of(k_start, step), span)
            q = qs[q_at, :]
            k = ks[k_at, :].astype(jnp.bfloat16)
            v = vs[k_at, :].astype(jnp.bfloat16)
            v = jnp.concatenate([v, jnp.ones((span, LANES), jnp.bfloat16)], axis=1)
            low = lax.broadcasted_iota(jnp.int32, (step, LANES), 1) < HEAD_SIZE
            q2 = jnp.concatenate([jnp.where(low, q, 0.0), jnp.where(low, 0.0, q)], axis=0).astype(jnp.bfloat16)
            s = lax.dot_general(q2, k, (((1,), (1,)), ((), ())), preferred_element_type=jnp.float32)
            seen = bias[mask_at, :step, :span]
            s = s + jnp.concatenate([seen, seen], axis=0)
            top = jnp.max(s, axis=1, keepdims=True)
            p = jnp.exp(s - top)
            o = jnp.dot(p.astype(jnp.bfloat16), v, preferred_element_type=jnp.float32)
            top = jnp.where(low, top[:step], top[step:])
            den = jnp.where(low, o[:step, LANES:], o[step:, LANES:])
            o = jnp.where(low, o[:step, :LANES], o[step:, :LANES])
            if number == 0:
                top_s[q_at, :] = top
                den_s[q_at, :] = den
                acc_s[q_at, :] = o
            else:
                was = top_s[q_at, :]
                new = jnp.maximum(was, top)
                old_scale, scale = jnp.exp(was - new), jnp.exp(top - new)
                top_s[q_at, :] = new
                den_s[q_at, :] = den_s[q_at, :] * old_scale + den * scale
                acc_s[q_at, :] = acc_s[q_at, :] * old_scale + o * scale
            return _

        lax.fori_loop(begin * d, end * d, block, 0, unroll=unroll)

    def wide_attention(cls, _):
        step = own // wide
        span = step + KEYS_BEHIND
        q = q_cls[cls].astype(jnp.float32)
        k = k_cls[cls, old - KEYS_BEHIND :, :]
        v = v_cls[cls, old - KEYS_BEHIND :, :]
        v = jnp.concatenate([v, jnp.ones((span, LANES), jnp.bfloat16)], axis=1)
        low = lax.broadcasted_iota(jnp.int32, (step, LANES), 1) < HEAD_SIZE
        q2 = jnp.concatenate([jnp.where(low, q, 0.0), jnp.where(low, 0.0, q)], axis=0).astype(jnp.bfloat16)
        s = lax.dot_general(q2, k, (((1,), (1,)), ((), ())), preferred_element_type=jnp.float32)
        seen = bias[len(dilation_rates), :step, :span]
        s = s + jnp.concatenate([seen, seen], axis=0)
        top = jnp.max(s, axis=1, keepdims=True)
        p = jnp.exp(s - top)
        o = jnp.dot(p.astype(jnp.bfloat16), v, preferred_element_type=jnp.float32)
        top = jnp.where(low, top[:step], top[step:])
        den = jnp.where(low, o[:step, LANES:], o[step:, LANES:])
        out_cls[cls] = jnp.where(low, o[:step, :LANES], o[step:, :LANES]) / den
        lse_cls[cls] = top + jnp.log(den)
        return _

    counts = [own // d // min(KEYS_BEHIND, own // d) for d in dilation_rates[:-1]]

    def unroll_of(trips):
        return next(u for u in (2, 3, 1) if trips % u == 0)

    strips = list(range(planes)) if by_plane else []
    if 0 < corner_hops < planes - 1:
        strips.remove(corner_hops)
        strips.append(corner_hops)
    early, late = strips[1:3], strips[3:]

    def later(k, _):
        o_relayed(k)
        when(k + 1 < planes, lambda: o_relay(k + 1))
        return _

    def before_second():
        if by_plane:
            edges(0)
            for m in early[:1]:
                sides(m)

    def before_halo():
        started = {1: 1, 2: 2, 4: 3}[group]
        if started < planes:
            lax.fori_loop(started, planes, later, 0)
        for m in early[1:]:
            sides(m)
        edges_arrive(0)
        if corner_hops > 0:
            z_relay(1)

    for number, d in enumerate(dilation_rates[:-1]):
        if counts[number] > 1:
            attention(number, 1, counts[number], unroll_of((counts[number] - 1) * d))
        if number == 0:
            before_second()
    before_halo()

    for h in range(1, far + 1):
        @pl.when(plane - h >= 0)
        def _():
            def sort(u, _):
                i, k = u // 2, lax.rem(u, 2)
                halo_out(h, i, k).wait_recv()
                start = (g ^ i) * rows + k * half
                by_class = by_classes(halo_ref[far - h, pl.ds(pl.multiple_of(start, half), half), :])
                at_run = pl.ds(pl.multiple_of((far - h) * (own // wide) + start // wide, run), run)
                k_cls[:, at_run, :] = by_class[:, :, :LANES]
                v_cls[:, at_run, :] = by_class[:, :, LANES:]
                return _

            lax.fori_loop(0, 2 * group, sort, 0)
            if h == 1:
                ks[:behind] = halo_ref[far - 1, own - behind :, :LANES].astype(jnp.float32)
                vs[:behind] = halo_ref[far - 1, own - behind :, LANES:].astype(jnp.float32)

    for number, d in enumerate(dilation_rates[:-1]):
        attention(number, 0, 1, unroll_of(d))
    lax.fori_loop(0, wide, wide_attention, 0, unroll=2)
    for k in range(1, corner_hops):
        z_forward(k)

    def att_lanes(i):
        return att_all.at[:, pl.ds(pl.multiple_of((g ^ i) * LANES, LANES), LANES)]

    def att_out(i):
        mine = pl.ds(pl.multiple_of((g ^ i) * rows, rows), rows)
        return pltpu.make_async_remote_copy(
            src_ref=att.at[mine], dst_ref=att_lanes(0), send_sem=a_send.at[i], recv_sem=a_recv.at[i],
            device_id=at(mate(i), tp), device_id_type=MESH)

    def att_in(i):
        return pltpu.make_async_remote_copy(
            src_ref=att.at[pl.ds(0, rows)], dst_ref=att_lanes(i), send_sem=a_send.at[i], recv_sem=a_recv.at[i],
            device_id=at(mate(i), tp), device_id_type=MESH)

    def lse_out(i):
        return pltpu.make_async_remote_copy(
            src_ref=lse_ref.at[g ^ i], dst_ref=lse_all.at[g], send_sem=l_send.at[i], recv_sem=l_recv.at[i],
            device_id=at(mate(i), tp), device_id_type=MESH)

    def lse_in(i):
        return pltpu.make_async_remote_copy(
            src_ref=lse_ref.at[g ^ i], dst_ref=lse_all.at[g ^ i], send_sem=l_send.at[i], recv_sem=l_recv.at[i],
            device_id=at(mate(i), tp), device_id_type=MESH)

    def split(x):
        high = x.astype(jnp.bfloat16)
        return [high, (x - high.astype(jnp.float32)).astype(jnp.bfloat16)]

    def finish(index, carry):
        i = lax.rem(index + 1, group)
        block = g ^ i
        for k in range(2):
            start = block * rows + k * half
            at_run = pl.ds(pl.multiple_of(start // wide, run), run)
            here = pl.ds(pl.multiple_of(start, half), half)
            terms = split(out_cls[:, at_run, :].reshape(half, LANES)) + split(lse_cls[:, at_run, :].reshape(half, LANES))
            back_in_order = jnp.dot(turn[1], jnp.concatenate(terms, axis=1), preferred_element_type=jnp.float32)
            out = back_in_order[:, :LANES] + back_in_order[:, LANES : 2 * LANES]
            lse = back_in_order[:, 2 * LANES : 3 * LANES] + back_in_order[:, 3 * LANES :]
            was = top_s[here, :]
            new = jnp.maximum(was, lse)
            old_scale, scale = jnp.exp(was - new), jnp.exp(lse - new)
            den = den_s[here, :] * old_scale + scale
            att[here, :] = ((acc_s[here, :] * old_scale + out * scale) / den).astype(jnp.bfloat16)
            lse = new + jnp.log(den)
            for t in range(half // LANES):
                columns = lse[t * LANES : (t + 1) * LANES].T
                off = k * half + t * LANES
                for h in range(heads):
                    lse_ref[block, h : h + 1, off : off + LANES] = columns[h * HEAD_SIZE : h * HEAD_SIZE + 1, :]

        @pl.when(i > 0)
        def _():
            att_out(i).start()
            lse_out(i).start()

        return carry

    lax.fori_loop(0, group, finish, 0)
    own_a = pltpu.make_async_copy(att.at[pl.ds(pl.multiple_of(g * rows, rows), rows)], att_lanes(0), own_sem.at[1])
    own_a.start()
    own_l = pltpu.make_async_copy(lse_ref.at[g], lse_all.at[g], own_sem.at[2])
    own_l.start()
    for m in early:
        edges(m)
    for m in late:
        sides(m)
    own_a.wait()
    for i in range(1, group):
        att_in(i).wait_recv()

    chunks, chunk = sums.shape[0], sums.shape[2]

    per_strip = chunks // planes if by_plane else 1

    def columns_of(c):
        if by_plane:
            m, side = strips[c // per_strip], c % per_strip
            side = side ^ (g // (group // per_strip)) if per_strip > 1 else 0
            return pl.ds(pl.multiple_of((nearest(m) * per_strip + side) * chunk, chunk), chunk)
        return pl.ds(c * chunk, chunk)

    def rows_of(j):
        return pl.ds(pl.multiple_of(lax.rem(tp + j, n_tp) * part, part), part)

    def sum_out(c, j):
        return pltpu.make_async_remote_copy(
            src_ref=sums.at[c, rows_of(j)], dst_ref=sums_in.at[j, c], send_sem=s_send.at[j, c], recv_sem=s_recv.at[j, c],
            device_id=at(sp, lax.rem(tp + j, n_tp)), device_id_type=MESH)

    def multiply(c):
        w = o_all[columns_of(c), :]
        product = lax.dot_general(att_all[...], w, (((1,), (1,)), ((), ())), preferred_element_type=jnp.float32)
        sums[c] = product.astype(jnp.bfloat16)
        for j in range(1, n_tp):
            sum_out(c, j).start()

    def add_up(c):
        total = sums[c, rows_of(0), :].astype(jnp.float32)
        for j in range(1, n_tp):
            sum_out(c, j).wait_recv()
            total += sums_in[j, c].astype(jnp.float32)
        mixed_ref[:, columns_of(c)] = total.astype(jnp.bfloat16)

    def edges_arrive_late(m):
        if m > 0:
            edges_arrive(m)
        if m == 1 and corner_hops > 0:
            z_relayed(1)
        if m > 1 and m == strips[2] and corner_hops > 1:
            z_relayed(2)

    lag = 3
    for c in range(chunks):
        if by_plane:
            m, side = strips[c // per_strip], c % per_strip
            if side == 0:
                if m in late:
                    edges(m)
            if side == per_strip - 1:
                edges_arrive_late(m)
        multiply(c)
        if c >= lag:
            add_up(c - lag)
    for c in range(max(chunks - lag, 0), chunks):
        add_up(c)

    own_l.wait()
    for i in range(1, group):
        lse_in(i).wait_recv()
    for b in range(group):
        lse_out_ref[b * heads : (b + 1) * heads, :] = lse_all[b]

    for i in range(1, group):
        w_in_plane(i).wait_send()
        for k in range(2):
            for s in range(2):
                for j in range(1, n_tp):
                    across(i, k, s, j).wait_send()
    for i in near:
        for s in range(2):
            for p in range(2):
                tokens_out(i, p, s).wait_send()
            if group == 4:
                corner_out(i, s).wait_send()
    if planes > 1:
        lax.fori_loop(1, planes, hops(relay_left), 0)
        lax.fori_loop(1, planes, lambda k, _: (o_relay_left(k), _)[1], 0)
    for h in range(1, far + 1):
        @pl.when(plane + h < planes)
        def _():
            for i in range(group):
                for k in range(2):
                    halo_out(h, i, k).wait_send()
    for j in range(1, n_tp):
        for c in range(chunks):
            sum_out(c, j).wait_send()
    for i in range(1, group):
        att_out(i).wait_send()
        lse_out(i).wait_send()
    if by_plane:
        for m in range(planes):
            for i in near:
                side_out(nearest(m), i).wait_send()
            edge_goes(m, lambda m=m: [edge_out(nearest(m), i).wait_send() for i in near])
        for k in range(1, corner_hops + 1):
            z_relay_left(k)


def shards(n, n_tp, tokens, w_query, w_key, w_value, w_out):
    rows, model = tokens.shape
    depth, width = w_query.shape
    slabs = width // LANES
    reach = KEYS_BEHIND * dilation_rates[-1]
    group = 1
    while group < 4 and group * rows < reach and slabs % (2 * group) == 0 and n % (2 * group) == 0:
        group *= 2
    assert slabs == group
    far = (reach + group * rows - 1) // (group * rows)
    planes = n // group
    own = group * rows
    part = rows // n_tp
    heads = LANES // HEAD_SIZE

    turned = w_out.T
    cut = w_out.shape[1]
    wide = dilation_rates[-1]
    behind = KEYS_BEHIND * dilation_rates[-2]
    chunks = planes * (2 if group == 4 and 2 * cut % LANES == 0 else 1) if group > 1 else (4 if (n * cut) % (4 * LANES) == 0 else 1)
    chunk = n * cut // chunks

    f32, bf16 = jnp.float32, jnp.bfloat16
    dma = pltpu.SemaphoreType.DMA
    vmem = pl.BlockSpec(memory_space=VMEM)
    mixed, lse = pl.pallas_call(
        functools.partial(layer_kernel, n, n_tp, group, far, heads),
        out_shape=(
            jax.ShapeDtypeStruct((part, n * cut), bf16),
            jax.ShapeDtypeStruct((group * heads, rows), f32),
        ),
        in_specs=[pl.BlockSpec(memory_space=pltpu.HBM)] * 5,
        out_specs=(vmem, vmem),
        scratch_shapes=[
            VMEM((group, rows, model), bf16),
            VMEM((n, depth, 3 * LANES), bf16),
            VMEM((group, depth, 3 * LANES), bf16),
            VMEM((own, 2 * LANES), bf16), VMEM((far, own, 2 * LANES), bf16),
            VMEM((n * cut, width), bf16),
            VMEM((own, LANES), f32), VMEM((behind + own, LANES), f32), VMEM((behind + own, LANES), f32),
            VMEM((wide, own // wide, LANES), bf16),
            VMEM((wide, (far + 1) * own // wide, LANES), bf16), VMEM((wide, (far + 1) * own // wide, LANES), bf16),
            VMEM((wide, own // wide, LANES), f32), VMEM((wide, own // wide, LANES), f32),
            VMEM((2, rows // 2, rows // 2), bf16),
            VMEM((1 + len(dilation_rates), KEYS_BEHIND, 2 * KEYS_BEHIND), f32),
            VMEM((own, LANES), f32), VMEM((own, LANES), f32), VMEM((own, LANES), f32),
            VMEM((own, LANES), bf16), VMEM((group, heads, rows), f32), VMEM((group, heads, rows), f32),
            VMEM((rows, group * LANES), bf16),
            VMEM((chunks, rows, chunk), bf16), VMEM((n_tp, chunks, part, chunk), bf16),
            dma((3, group)), dma((4,)),
            dma((group,)), dma((group,)),
            dma((group, planes)), dma((group, planes)),
            dma((group, planes)), dma((group, planes)),
            dma((group, 2, 2)), dma((group, 2, 2)),
            dma((group, 2)), dma((group, 2)),
            dma((group, 2, 2, n_tp)), dma((group, 2, 2, n_tp)),
            dma((far + 1, group, 2)), dma((far + 1, group, 2)),
            dma((planes,)), dma((planes,)), dma((planes,)), dma((planes,)),
            dma((planes, group)), dma((planes, group)),
            dma((planes, group)), dma((planes, group)),
            dma((3,)), dma((3,)), dma((3,)), dma((3,)),
            dma((group,)), dma((group,)), dma((group,)), dma((group,)),
            dma((n_tp, chunks)), dma((n_tp, chunks)),
        ],
        compiler_params=pltpu.CompilerParams(collective_id=0, has_side_effects=True, vmem_limit_bytes=46 << 20),
        cost_estimate=pl.CostEstimate(
            flops=2 * own * model * 3 * LANES, bytes_accessed=1 << 24, transcendentals=1 << 22),
        name="layer",
    )(*[pltpu.with_memory_space_constraint(x, pltpu.HBM) for x in (w_query, w_key, w_value, tokens, turned)])
    return mixed, lse


def solution(mesh):
    placed = (P("sp", None), P("sp", "tp"), P("sp", "tp"), P("sp", "tp"), P("tp", "sp"))
    return jax.shard_map(
        functools.partial(shards, mesh.shape["sp"], mesh.shape["tp"]),
        mesh=mesh,
        in_specs=placed,
        out_specs=(P(("sp", "tp"), None), P("tp", "sp")),
        check_vma=False,
    )
```

```python
import functools

import jax
import jax.numpy as jnp
from jax import lax
from jax.experimental import pallas as pl
from jax.experimental.pallas import tpu as pltpu
from jax.sharding import PartitionSpec as P

HEAD_SIZE = 64
KEYS_BEHIND = 128
LANES = 128

dilation_rates = (1, 4, 16)
neg_big = -1e30

MESH = pl.DeviceIdType.MESH
VMEM = pltpu.VMEM


def at(sp, tp):
    return {"sp": sp, "tp": tp}


def layer_kernel(
    n, n_tp, group, far, heads, wq_ref, wk_ref, wv_ref, tok_ref, o_ref, mixed_ref, lse_out_ref,
    tok_all, w_all, w_ref, kv_ref, halo_ref, o_all, qs, ks, vs, q_cls, k_cls, v_cls, out_cls, lse_cls, turn, bias,
    top_s, den_s, acc_s, att, lse_ref, lse_all, att_all, sums, sums_in,
    pack_sem, own_sem, w1_send, w1_recv, up_send, up_recv, down_send, down_recv, t_send, t_recv, d_send, d_recv,
    f_send, f_recv, h_send, h_recv, ou_send, ou_recv, od_send, od_recv, b_send, b_recv, c_send, c_recv,
    zu_send, zu_recv, zd_send, zd_recv, a_send, a_recv, l_send, l_recv, s_send, s_recv,
):
    sp, tp = lax.axis_index("sp"), lax.axis_index("tp")
    planes = n // group
    g, plane = lax.rem(sp, group), sp // group
    rows = tok_ref.shape[0]
    own = group * rows
    base = plane * own
    half = rows // 2
    bit_rows = half // (2 * n_tp)
    part = mixed_ref.shape[0]
    cut, width = o_ref.shape
    half_cut = cut // 2
    wide = dilation_rates[-1]
    behind = KEYS_BEHIND * dilation_rates[-2]
    run = half // wide
    old = far * own // wide

    above = lax.rem(sp + group, n)
    below = lax.rem(sp + n - group, n)

    def mate(i):
        return plane * group + (g ^ i)

    near = [i for i in (1, 2) if i < group]

    barrier = pltpu.get_barrier_semaphore()
    greeted = 0

    def greet(sp_to, tp_to):
        pl.semaphore_signal(barrier, inc=1, device_id=at(sp_to, tp_to), device_id_type=MESH)
        return 1

    for i in range(1, group):
        greeted += greet(mate(i), tp)
    if planes > 1:
        for h in range(1, max(far, 1) + 1):
            greeted += greet(lax.rem(sp + h * group, n), tp)
            greeted += greet(lax.rem(sp + n - h * group, n), tp)
    for j in range(1, n_tp):
        greeted += greet(sp, lax.rem(tp + j, n_tp))

    own_t = pltpu.make_async_copy(tok_ref, tok_all.at[g], own_sem.at[0])

    def strip(q, i, part_of=None):
        origin = q * group + (g ^ i)
        if part_of is None:
            return o_all.at[pl.ds(pl.multiple_of(origin * cut, cut), cut)]
        return o_all.at[pl.ds(pl.multiple_of(origin * cut + part_of * half_cut, half_cut), half_cut)]

    own_o = pltpu.make_async_copy(o_ref, strip(plane, 0), own_sem.at[3])

    def pack(t, i):
        source = (wq_ref, wk_ref, wv_ref)[t].at[:, pl.ds(pl.multiple_of((g ^ i) * LANES, LANES), LANES)]
        lanes = pl.ds(t * LANES, LANES)
        to = w_all.at[sp, :, lanes] if i == 0 else w_ref.at[i, :, lanes]
        return pltpu.make_async_copy(source, to, pack_sem.at[t, i])

    for i in list(range(1, group)) + [0]:
        for t in range(3):
            pack(t, i).start()
    own_o.start()
    own_t.start()
    pl.semaphore_wait(barrier, greeted)

    def w_in_plane(i):
        return pltpu.make_async_remote_copy(
            src_ref=w_ref.at[i], dst_ref=w_all.at[sp], send_sem=w1_send.at[i], recv_sem=w1_recv.at[i],
            device_id=at(mate(i), tp), device_id_type=MESH)

    def w_in_plane_arrives(i):
        return pltpu.make_async_remote_copy(
            src_ref=w_ref.at[i], dst_ref=w_all.at[mate(i)], send_sem=w1_send.at[i], recv_sem=w1_recv.at[i],
            device_id=at(mate(i), tp), device_id_type=MESH)

    def slab(p, i):
        return w_all.at[lax.rem(p + 2 * planes, planes) * group + (g ^ i)]

    def up(i, k, p):
        return pltpu.make_async_remote_copy(
            src_ref=slab(p, i), dst_ref=slab(p, i), send_sem=up_send.at[i, k], recv_sem=up_recv.at[i, k],
            device_id=at(above, tp), device_id_type=MESH)

    def down(i, k, p):
        return pltpu.make_async_remote_copy(
            src_ref=slab(p, i), dst_ref=slab(p, i), send_sem=down_send.at[i, k], recv_sem=down_recv.at[i, k],
            device_id=at(below, tp), device_id_type=MESH)

    def o_up(k, p):
        ref = strip(lax.rem(p + 2 * planes, planes), 0)
        return pltpu.make_async_remote_copy(
            src_ref=ref, dst_ref=ref, send_sem=ou_send.at[k], recv_sem=ou_recv.at[k],
            device_id=at(above, tp), device_id_type=MESH)

    def o_down(k, p):
        ref = strip(lax.rem(p + 2 * planes, planes), 0)
        return pltpu.make_async_remote_copy(
            src_ref=ref, dst_ref=ref, send_sem=od_send.at[k], recv_sem=od_recv.at[k],
            device_id=at(below, tp), device_id_type=MESH)

    def when(condition, action):
        @pl.when(condition)
        def _():
            action()

    first, last = plane == 0, plane == planes - 1

    def relay(k, i):
        when(~last & (plane - k + 1 >= 0), lambda: up(i, k, plane - k + 1).start())
        when(~first & (plane + k - 1 < planes), lambda: down(i, k, plane + k - 1).start())

    def relayed(k, i):
        when(plane - k >= 0, lambda: up(i, k, plane - k).wait_recv())
        when(plane + k < planes, lambda: down(i, k, plane + k).wait_recv())

    def relay_left(k, i):
        when(~last & (plane - k + 1 >= 0), lambda: up(i, k, plane - k + 1).wait_send())
        when(~first & (plane + k - 1 < planes), lambda: down(i, k, plane + k - 1).wait_send())

    def o_relay(k):
        when(~last & (plane - k + 1 >= 0), lambda: o_up(k, plane - k + 1).start())
        when(~first & (plane + k - 1 < planes), lambda: o_down(k, plane + k - 1).start())

    def o_relay_left(k):
        when(~last & (plane - k + 1 >= 0), lambda: o_up(k, plane - k + 1).wait_send())
        when(~first & (plane + k - 1 < planes), lambda: o_down(k, plane + k - 1).wait_send())

    def hops(body):
        def one(k, _):
            for i in range(group):
                body(k, i)
            return _

        return one

    def nearest(m):
        left, right = plane, planes - 1 - plane
        short = jnp.minimum(left, right)
        zigzag = plane + (m // 2 if m % 2 == 0 else -((m + 1) // 2))
        return jnp.where(m <= 2 * short, zigzag, jnp.where(left < right, m, planes - 1 - m))

    def back(q):
        return lax.rem(plane - q + planes, planes)

    def side_out(q, i):
        k = back(q)
        return pltpu.make_async_remote_copy(
            src_ref=strip(q, 0), dst_ref=strip(q, 0), send_sem=b_send.at[k, i], recv_sem=b_recv.at[k, i],
            device_id=at(mate(i), tp), device_id_type=MESH)

    def side_in(q, i):
        k = back(q)
        return pltpu.make_async_remote_copy(
            src_ref=strip(q, i), dst_ref=strip(q, i), send_sem=b_send.at[k, i], recv_sem=b_recv.at[k, i],
            device_id=at(mate(i), tp), device_id_type=MESH)

    def edge_out(q, i):
        k = back(q)
        return pltpu.make_async_remote_copy(
            src_ref=strip(q, i, i - 1), dst_ref=strip(q, i, i - 1), send_sem=c_send.at[k, i], recv_sem=c_recv.at[k, i],
            device_id=at(mate(3 - i), tp), device_id_type=MESH)

    def edge_in(q, i):
        k = back(q)
        return pltpu.make_async_remote_copy(
            src_ref=strip(q, 3, i - 1), dst_ref=strip(q, 3, i - 1), send_sem=c_send.at[k, i], recv_sem=c_recv.at[k, i],
            device_id=at(mate(3 - i), tp), device_id_type=MESH)

    def sides(m):
        for i in near:
            side_out(nearest(m), i).start()

    corner_hops = min(2, planes - 1) if group == 4 else 0

    def edge_goes(m, action):
        if group == 4:
            if m == 0:
                action()
            elif m > corner_hops:
                when(jnp.abs(nearest(m) - plane) > corner_hops, action)

    def edges(m):
        for i in near:
            side_in(nearest(m), i).wait_recv()
        edge_goes(m, lambda: [edge_out(nearest(m), i).start() for i in near])

    def edges_arrive(m):
        edge_goes(m, lambda: [edge_in(nearest(m), i).wait_recv() for i in near])

    def z_up(k, p):
        ref = strip(lax.rem(p + 2 * planes, planes), 3)
        return pltpu.make_async_remote_copy(
            src_ref=ref, dst_ref=ref, send_sem=zu_send.at[k], recv_sem=zu_recv.at[k],
            device_id=at(above, tp), device_id_type=MESH)

    def z_down(k, p):
        ref = strip(lax.rem(p + 2 * planes, planes), 3)
        return pltpu.make_async_remote_copy(
            src_ref=ref, dst_ref=ref, send_sem=zd_send.at[k], recv_sem=zd_recv.at[k],
            device_id=at(below, tp), device_id_type=MESH)

    def z_relay(k):
        when(~last & (plane - k + 1 >= 0), lambda: z_up(k, plane - k + 1).start())
        when(~first & (plane + k - 1 < planes), lambda: z_down(k, plane + k - 1).start())

    def z_forward(k):
        def up_on():
            z_up(k, plane - k).wait_recv()
            z_up(k + 1, plane - k).start()

        def down_on():
            z_down(k, plane + k).wait_recv()
            z_down(k + 1, plane + k).start()

        when(~last & (plane - k >= 0), up_on)
        when(~first & (plane + k < planes), down_on)

    def z_relayed(k):
        ends = (True, True) if k == corner_hops else (last, first)
        when(ends[0] & (plane - k >= 0), lambda: z_up(k, plane - k).wait_recv())
        when(ends[1] & (plane + k < planes), lambda: z_down(k, plane + k).wait_recv())

    def z_relay_left(k):
        when(~last & (plane - k + 1 >= 0), lambda: z_up(k, plane - k + 1).wait_send())
        when(~first & (plane + k - 1 < planes), lambda: z_down(k, plane + k - 1).wait_send())

    def o_relayed(k):
        def from_below():
            o_up(k, plane - k).wait_recv()

        def from_above():
            o_down(k, plane + k).wait_recv()

        when(plane - k >= 0, from_below)
        when(plane + k < planes, from_above)

    def bit(s, p, t):
        return pl.ds(pl.multiple_of(s * half + (p * n_tp + t) * bit_rows, bit_rows), bit_rows)

    def tokens_out(i, p, s):
        return pltpu.make_async_remote_copy(
            src_ref=tok_ref.at[bit(s, p, tp)], dst_ref=tok_all.at[g, bit(s, p, tp)],
            send_sem=t_send.at[i, p, s], recv_sem=t_recv.at[i, p, s], device_id=at(mate(i), tp), device_id_type=MESH)

    def tokens_in(i, p, s):
        return pltpu.make_async_remote_copy(
            src_ref=tok_ref.at[bit(s, p, tp)], dst_ref=tok_all.at[g ^ i, bit(s, p, tp)],
            send_sem=t_send.at[i, p, s], recv_sem=t_recv.at[i, p, s], device_id=at(mate(i), tp), device_id_type=MESH)

    def corner_out(i, s):
        ref = tok_all.at[g ^ i, bit(s, i - 1, tp)]
        return pltpu.make_async_remote_copy(
            src_ref=ref, dst_ref=ref, send_sem=d_send.at[i, s], recv_sem=d_recv.at[i, s],
            device_id=at(mate(3 - i), tp), device_id_type=MESH)

    def corner_in(i, s):
        ref = tok_all.at[g ^ 3, bit(s, i - 1, tp)]
        return pltpu.make_async_remote_copy(
            src_ref=ref, dst_ref=ref, send_sem=d_send.at[i, s], recv_sem=d_recv.at[i, s],
            device_id=at(mate(3 - i), tp), device_id_type=MESH)

    def across(i, p, s, j):
        ref = tok_all.at[g ^ i, bit(s, p, tp)]
        return pltpu.make_async_remote_copy(
            src_ref=ref, dst_ref=ref, send_sem=f_send.at[i, p, s, j], recv_sem=f_recv.at[i, p, s, j],
            device_id=at(sp, lax.rem(tp + j, n_tp)), device_id_type=MESH)

    def across_in(i, p, s, j):
        ref = tok_all.at[g ^ i, bit(s, p, lax.rem(tp + n_tp - j, n_tp))]
        return pltpu.make_async_remote_copy(
            src_ref=ref, dst_ref=ref, send_sem=f_send.at[i, p, s, j], recv_sem=f_recv.at[i, p, s, j],
            device_id=at(sp, lax.rem(tp + j, n_tp)), device_id_type=MESH)

    def to_other_cores(i, p, s):
        for j in range(1, n_tp):
            across(i, p, s, j).start()

    def piece(i, step):
        return step if i == 1 else 1 - step

    for i in range(1, group):
        for t in range(3):
            pack(t, i).wait()
        w_in_plane(i).start()
    for t in range(3):
        pack(t, 0).wait()
    if planes > 1:
        relay(1, 0)
    for step in range(2):
        for s in range(2):
            for i in near:
                tokens_out(i, piece(i, step), s).start()
    for i in range(1, group):
        w_in_plane_arrives(i).wait_recv()
        if planes > 1:
            relay(1, i)

    def pass_on(k, i):
        relayed(k, i)
        relay(k + 1, i)

    row = lax.broadcasted_iota(jnp.int32, (KEYS_BEHIND, 2 * KEYS_BEHIND), 0)
    col = lax.broadcasted_iota(jnp.int32, (KEYS_BEHIND, 2 * KEYS_BEHIND), 1)
    dist = KEYS_BEHIND + row - col
    band = (dist >= 0) & (dist <= KEYS_BEHIND)
    bias[0] = jnp.where(band, 0.0, neg_big)
    for number, d in enumerate(dilation_rates):
        bias[1 + number] = jnp.where(band & (base // d - KEYS_BEHIND + col >= 0), 0.0, neg_big)
    to_row = lax.broadcasted_iota(jnp.int32, (half, half), 0)
    from_row = lax.broadcasted_iota(jnp.int32, (half, half), 1)
    turn[0] = (from_row == to_row % run * wide + to_row // run).astype(jnp.float32).astype(jnp.bfloat16)
    turn[1] = (from_row == to_row % wide * run + to_row // wide).astype(jnp.float32).astype(jnp.bfloat16)

    @pl.when(plane == 0)
    def _():
        ks[:behind] = jnp.zeros((behind, LANES), jnp.float32)
        vs[:behind] = jnp.zeros((behind, LANES), jnp.float32)

    for h in range(1, far + 1):
        @pl.when(plane - h < 0)
        def _():
            gone = slice((far - h) * own // wide, (far - h + 1) * own // wide)
            k_cls[:, gone] = jnp.zeros((wide, own // wide, LANES), jnp.bfloat16)
            v_cls[:, gone] = jnp.zeros((wide, own // wide, LANES), jnp.bfloat16)

    if planes > 1:
        lax.fori_loop(1, planes - 1, hops(pass_on), 0)
    own_o.wait()
    if planes > 1:
        o_relay(1)
    for s in range(2):
        for i in near:
            tokens_in(i, piece(i, 0), s).wait_recv()
            if group == 4:
                corner_out(i, s).start()
            to_other_cores(i, piece(i, 0), s)
    if planes > 1:
        for i in range(group):
            relayed(planes - 1, i)
    for s in range(2):
        for i in near:
            tokens_in(i, piece(i, 1), s).wait_recv()
            to_other_cores(i, piece(i, 1), s)
    if near:
        sides(0)
    own_t.wait()

    def halo_out(h, i, k):
        view = pl.ds(pl.multiple_of((g ^ i) * rows + k * half, half), half)
        return pltpu.make_async_remote_copy(
            src_ref=kv_ref.at[view], dst_ref=halo_ref.at[far - h, view],
            send_sem=h_send.at[h, i, k], recv_sem=h_recv.at[h, i, k],
            device_id=at(lax.rem(sp + h * group, n), tp), device_id_type=MESH)

    def by_classes(y):
        sorted_rows = jnp.dot(turn[0], y, preferred_element_type=jnp.float32).astype(jnp.bfloat16)
        return sorted_rows.reshape(wide, run, y.shape[1])

    def tile(i, k):
        block = g ^ i
        x = tok_all[block, pl.ds(pl.multiple_of(k * half, half), half), :]
        w = w_all[...].reshape(-1, 3 * LANES)
        y = jnp.dot(x, w, preferred_element_type=jnp.float32).astype(jnp.bfloat16)
        start = block * rows + k * half
        to = pl.ds(pl.multiple_of(start, half), half)
        past = pl.ds(pl.multiple_of(behind + start, half), half)
        kv_ref[to, :] = y[:, LANES:]
        qs[to, :] = y[:, :LANES].astype(jnp.float32) * HEAD_SIZE ** (-0.5)
        ks[past, :] = y[:, LANES : 2 * LANES].astype(jnp.float32)
        vs[past, :] = y[:, 2 * LANES :].astype(jnp.float32)
        by_class = by_classes(y)
        at_run = pl.ds(pl.multiple_of(start // wide, run), run)
        q_cls[:, at_run, :] = by_class[:, :, :LANES] * HEAD_SIZE ** (-0.5)
        past_run = pl.ds(pl.multiple_of(old + start // wide, run), run)
        k_cls[:, past_run, :] = by_class[:, :, LANES : 2 * LANES]
        v_cls[:, past_run, :] = by_class[:, :, 2 * LANES :]
        for h in range(1, far + 1):
            @pl.when(plane + h < planes)
            def _():
                halo_out(h, i, k).start()

    def tiles(picks, ready):
        def one(s, _):
            i, k = picks(s)
            ready(i, k)
            tile(i, k)
            return _

        lax.fori_loop(0, 2, one, 0)

    def crossed(i, k):
        for p in range(2):
            for j in range(1, n_tp):
                across_in(i, p, k, j).wait_recv()

    def o_pass(k):
        if k < planes:
            o_relayed(k)
            if k + 1 < planes:
                o_relay(k + 1)

    def unroll_of(trips):
        return next(u for u in (3, 2, 5, 1) if trips % u == 0)

    def attention(number, trips, place, opening=False):
        d = dilation_rates[number]
        step = min(KEYS_BEHIND, own // d)
        span = step + KEYS_BEHIND
        mask_at = 1 + number if opening else 0

        def block(index, _):
            cls, b = place(index)
            start = b * (step * d) + cls
            q_at = pl.ds(start, step, stride=d) if d > 1 else pl.ds(pl.multiple_of(start, step), step)
            k_start = behind - KEYS_BEHIND * d + start
            k_at = pl.ds(k_start, span, stride=d) if d > 1 else pl.ds(pl.multiple_of(k_start, step), span)
            q = qs[q_at, :]
            k = ks[k_at, :].astype(jnp.bfloat16)
            v = vs[k_at, :].astype(jnp.bfloat16)
            v = jnp.concatenate([v, jnp.ones((span, LANES), jnp.bfloat16)], axis=1)
            low = lax.broadcasted_iota(jnp.int32, (step, LANES), 1) < HEAD_SIZE
            q2 = jnp.concatenate([jnp.where(low, q, 0.0), jnp.where(low, 0.0, q)], axis=0).astype(jnp.bfloat16)
            s = lax.dot_general(q2, k, (((1,), (1,)), ((), ())), preferred_element_type=jnp.float32)
            seen = bias[mask_at, :step, :span]
            s = s + jnp.concatenate([seen, seen], axis=0)
            top = jnp.max(s, axis=1, keepdims=True)
            p = jnp.exp(s - top)
            o = jnp.dot(p.astype(jnp.bfloat16), v, preferred_element_type=jnp.float32)
            top = jnp.where(low, top[:step], top[step:])
            den = jnp.where(low, o[:step, LANES:], o[step:, LANES:])
            o = jnp.where(low, o[:step, :LANES], o[step:, :LANES])
            if number == 0:
                top_s[q_at, :] = top
                den_s[q_at, :] = den
                acc_s[q_at, :] = o
            else:
                was = top_s[q_at, :]
                new = jnp.maximum(was, top)
                old_scale, scale = jnp.exp(was - new), jnp.exp(top - new)
                top_s[q_at, :] = new
                den_s[q_at, :] = den_s[q_at, :] * old_scale + den * scale
                acc_s[q_at, :] = acc_s[q_at, :] * old_scale + o * scale
            return _

        lax.fori_loop(0, trips, block, 0, unroll=unroll_of(trips))

    ahead = group == 4 and rows == KEYS_BEHIND * dilation_rates[1]
    per = rows // KEYS_BEHIND
    ready_row = 1 + 2 * (g // 2)

    def early_near(u):
        return 0, jnp.where(u < 9, (g ^ (u // 3)) * per + 1 + lax.rem(u, 3), per * ready_row)

    def late_near(u):
        rest = jnp.where(u == 3, 2, 4 - ready_row)
        return 0, jnp.where(u < 3, (g ^ 3) * per + 1 + u, per * rest)

    def early_middle(u):
        return u, ready_row

    def late_middle(u):
        return lax.rem(u, 4), jnp.where(u < 4, 2, 4 - ready_row)

    tiles(lambda s: (0, s), lambda i, k: None)
    if group > 1:
        o_pass(1)
    if group == 2:
        tiles(lambda s: (1, s), crossed)
    if group == 4:
        tiles(lambda s: (1 + s, 0), crossed)
        tiles(lambda s: (1 + s, 1), crossed)
        if ahead:
            attention(0, 10, early_near)
        for s in range(2):
            for i in near:
                corner_in(i, s).wait_recv()
                to_other_cores(3, i - 1, s)
            if s == 0:
                if ahead:
                    attention(1, 4, early_middle)
            crossed(3, s)
            tile(3, s)
            if s == 0 and 2 < planes:
                o_relayed(2)
        if 3 < planes:
            o_relay(3)

    by_plane = group > 1
    def wide_attention(cls, _):
        step = own // wide
        span = step + KEYS_BEHIND
        q = q_cls[cls].astype(jnp.float32)
        k = k_cls[cls, old - KEYS_BEHIND :, :]
        v = v_cls[cls, old - KEYS_BEHIND :, :]
        v = jnp.concatenate([v, jnp.ones((span, LANES), jnp.bfloat16)], axis=1)
        low = lax.broadcasted_iota(jnp.int32, (step, LANES), 1) < HEAD_SIZE
        q2 = jnp.concatenate([jnp.where(low, q, 0.0), jnp.where(low, 0.0, q)], axis=0).astype(jnp.bfloat16)
        s = lax.dot_general(q2, k, (((1,), (1,)), ((), ())), preferred_element_type=jnp.float32)
        seen = bias[len(dilation_rates), :step, :span]
        s = s + jnp.concatenate([seen, seen], axis=0)
        top = jnp.max(s, axis=1, keepdims=True)
        p = jnp.exp(s - top)
        o = jnp.dot(p.astype(jnp.bfloat16), v, preferred_element_type=jnp.float32)
        top = jnp.where(low, top[:step], top[step:])
        den = jnp.where(low, o[:step, LANES:], o[step:, LANES:])
        out_cls[cls] = jnp.where(low, o[:step, :LANES], o[step:, :LANES]) / den
        lse_cls[cls] = top + jnp.log(den)
        return _

    counts = [own // d // min(KEYS_BEHIND, own // d) for d in dilation_rates[:-1]]

    strips = list(range(planes)) if by_plane else []
    early, late = strips[1:3], strips[3:]

    def later(k, _):
        o_relayed(k)
        when(k + 1 < planes, lambda: o_relay(k + 1))
        return _

    def spread_first():
        if by_plane:
            edges(0)
            for m in early:
                sides(m)

    def spread_rest():
        started = {1: 1, 2: 2, 4: 3}[group]
        if started < planes:
            lax.fori_loop(started, planes, later, 0)
        for m in late:
            sides(m)

    def sort(h):
        def unit(u, carry):
            i, k = u // 2, lax.rem(u, 2)
            halo_out(h, i, k).wait_recv()
            start = (g ^ i) * rows + k * half
            by_class = by_classes(halo_ref[far - h, pl.ds(pl.multiple_of(start, half), half), :])
            at_run = pl.ds(pl.multiple_of((far - h) * (own // wide) + start // wide, run), run)
            k_cls[:, at_run, :] = by_class[:, :, :LANES]
            v_cls[:, at_run, :] = by_class[:, :, LANES:]
            return carry

        lax.fori_loop(0, 2 * group, unit, 0)
        if h == 1:
            ks[:behind] = halo_ref[far - 1, own - behind :, :LANES].astype(jnp.float32)
            vs[:behind] = halo_ref[far - 1, own - behind :, LANES:].astype(jnp.float32)

    if ahead:
        attention(0, 5, late_near)
    else:
        for number, d in enumerate(dilation_rates[:-1]):
            if counts[number] > 1:
                attention(number, (counts[number] - 1) * d, lambda u, d=d: (lax.rem(u, d), 1 + u // d))
    spread_first()
    if ahead:
        attention(1, 8, late_middle)
    for h in range(1, far + 1):
        when(plane - h >= 0, functools.partial(sort, h))

    for number, d in enumerate(dilation_rates[:-1]):
        attention(number, d, lambda u: (u, 0), opening=True)
    edges_arrive(0)
    if corner_hops > 0:
        z_relay(1)
    lax.fori_loop(0, wide, wide_attention, 0, unroll=4)
    spread_rest()
    def att_lanes(i):
        return att_all.at[:, pl.ds(pl.multiple_of((g ^ i) * LANES, LANES), LANES)]

    def att_out(i):
        mine = pl.ds(pl.multiple_of((g ^ i) * rows, rows), rows)
        return pltpu.make_async_remote_copy(
            src_ref=att.at[mine], dst_ref=att_lanes(0), send_sem=a_send.at[i], recv_sem=a_recv.at[i],
            device_id=at(mate(i), tp), device_id_type=MESH)

    def att_in(i):
        return pltpu.make_async_remote_copy(
            src_ref=att.at[pl.ds(0, rows)], dst_ref=att_lanes(i), send_sem=a_send.at[i], recv_sem=a_recv.at[i],
            device_id=at(mate(i), tp), device_id_type=MESH)

    def lse_out(i):
        return pltpu.make_async_remote_copy(
            src_ref=lse_ref.at[g ^ i], dst_ref=lse_all.at[g], send_sem=l_send.at[i], recv_sem=l_recv.at[i],
            device_id=at(mate(i), tp), device_id_type=MESH)

    def lse_in(i):
        return pltpu.make_async_remote_copy(
            src_ref=lse_ref.at[g ^ i], dst_ref=lse_all.at[g ^ i], send_sem=l_send.at[i], recv_sem=l_recv.at[i],
            device_id=at(mate(i), tp), device_id_type=MESH)

    def split(x):
        high = x.astype(jnp.bfloat16)
        return [high, (x - high.astype(jnp.float32)).astype(jnp.bfloat16)]

    def finish(index, carry):
        i = lax.rem(index + 1, group)
        block = g ^ i
        for k in range(2):
            start = block * rows + k * half
            at_run = pl.ds(pl.multiple_of(start // wide, run), run)
            here = pl.ds(pl.multiple_of(start, half), half)
            terms = split(out_cls[:, at_run, :].reshape(half, LANES)) + split(lse_cls[:, at_run, :].reshape(half, LANES))
            back_in_order = jnp.dot(turn[1], jnp.concatenate(terms, axis=1), preferred_element_type=jnp.float32)
            out = back_in_order[:, :LANES] + back_in_order[:, LANES : 2 * LANES]
            lse = back_in_order[:, 2 * LANES : 3 * LANES] + back_in_order[:, 3 * LANES :]
            was = top_s[here, :]
            new = jnp.maximum(was, lse)
            old_scale, scale = jnp.exp(was - new), jnp.exp(lse - new)
            den = den_s[here, :] * old_scale + scale
            att[here, :] = ((acc_s[here, :] * old_scale + out * scale) / den).astype(jnp.bfloat16)
            lse = new + jnp.log(den)
            for t in range(half // LANES):
                columns = lse[t * LANES : (t + 1) * LANES].T
                off = k * half + t * LANES
                for h in range(heads):
                    lse_ref[block, h : h + 1, off : off + LANES] = columns[h * HEAD_SIZE : h * HEAD_SIZE + 1, :]

        @pl.when(i > 0)
        def _():
            att_out(i).start()
            lse_out(i).start()

        return carry

    lax.fori_loop(0, group, finish, 0)
    own_a = pltpu.make_async_copy(att.at[pl.ds(pl.multiple_of(g * rows, rows), rows)], att_lanes(0), own_sem.at[1])
    own_a.start()
    own_l = pltpu.make_async_copy(lse_ref.at[g], lse_all.at[g], own_sem.at[2])
    own_l.start()
    for m in early:
        edges(m)
    for k in range(1, corner_hops):
        z_forward(k)
    for m in late:
        edges(m)
    own_a.wait()
    for i in range(1, group):
        att_in(i).wait_recv()

    chunks, chunk = sums.shape[0], sums.shape[2]

    per_strip = chunks // planes if by_plane else 1

    def columns_of(c):
        if by_plane:
            m, side = strips[c // per_strip], c % per_strip
            side = side ^ (g // (group // per_strip)) if per_strip > 1 else 0
            return pl.ds(pl.multiple_of((nearest(m) * per_strip + side) * chunk, chunk), chunk)
        return pl.ds(c * chunk, chunk)

    def rows_of(j):
        return pl.ds(pl.multiple_of(lax.rem(tp + j, n_tp) * part, part), part)

    def sum_out(c, j):
        return pltpu.make_async_remote_copy(
            src_ref=sums.at[c, rows_of(j)], dst_ref=sums_in.at[j, c], send_sem=s_send.at[j, c], recv_sem=s_recv.at[j, c],
            device_id=at(sp, lax.rem(tp + j, n_tp)), device_id_type=MESH)

    def multiply(c):
        w = o_all[columns_of(c), :]
        product = lax.dot_general(att_all[...], w, (((1,), (1,)), ((), ())), preferred_element_type=jnp.float32)
        sums[c] = product.astype(jnp.bfloat16)
        for j in range(1, n_tp):
            sum_out(c, j).start()

    def add_up(c):
        total = sums[c, rows_of(0), :].astype(jnp.float32)
        for j in range(1, n_tp):
            sum_out(c, j).wait_recv()
            total += sums_in[j, c].astype(jnp.float32)
        mixed_ref[:, columns_of(c)] = total.astype(jnp.bfloat16)

    def edges_arrive_late(m):
        if m > 0:
            edges_arrive(m)
        if m == 1 and corner_hops > 0:
            z_relayed(1)
        if m > 1 and m == strips[2] and corner_hops > 1:
            z_relayed(2)

    lag = 3
    for c in range(chunks):
        if by_plane:
            m, side = strips[c // per_strip], c % per_strip
            if side == per_strip - 1:
                edges_arrive_late(m)
        multiply(c)
        if c >= lag:
            add_up(c - lag)
    for c in range(max(chunks - lag, 0), chunks):
        add_up(c)

    own_l.wait()
    for i in range(1, group):
        lse_in(i).wait_recv()
    for b in range(group):
        lse_out_ref[b * heads : (b + 1) * heads, :] = lse_all[b]

    for i in range(1, group):
        w_in_plane(i).wait_send()
        for k in range(2):
            for s in range(2):
                for j in range(1, n_tp):
                    across(i, k, s, j).wait_send()
    for i in near:
        for s in range(2):
            for p in range(2):
                tokens_out(i, p, s).wait_send()
            if group == 4:
                corner_out(i, s).wait_send()
    if planes > 1:
        lax.fori_loop(1, planes, hops(relay_left), 0)
        lax.fori_loop(1, planes, lambda k, _: (o_relay_left(k), _)[1], 0)
    for h in range(1, far + 1):
        @pl.when(plane + h < planes)
        def _():
            for i in range(group):
                for k in range(2):
                    halo_out(h, i, k).wait_send()
    for j in range(1, n_tp):
        for c in range(chunks):
            sum_out(c, j).wait_send()
    for i in range(1, group):
        att_out(i).wait_send()
        lse_out(i).wait_send()
    if by_plane:
        for m in range(planes):
            for i in near:
                side_out(nearest(m), i).wait_send()
            edge_goes(m, lambda m=m: [edge_out(nearest(m), i).wait_send() for i in near])
        for k in range(1, corner_hops + 1):
            z_relay_left(k)


def shards(n, n_tp, tokens, w_query, w_key, w_value, w_out):
    rows, model = tokens.shape
    depth, width = w_query.shape
    slabs = width // LANES
    reach = KEYS_BEHIND * dilation_rates[-1]
    group = 1
    while group < 4 and group * rows < reach and slabs % (2 * group) == 0 and n % (2 * group) == 0:
        group *= 2
    assert slabs == group
    far = (reach + group * rows - 1) // (group * rows)
    planes = n // group
    own = group * rows
    part = rows // n_tp
    heads = LANES // HEAD_SIZE

    turned = w_out.T
    cut = w_out.shape[1]
    wide = dilation_rates[-1]
    behind = KEYS_BEHIND * dilation_rates[-2]
    chunks = planes * (2 if group == 4 and 2 * cut % LANES == 0 else 1) if group > 1 else (4 if (n * cut) % (4 * LANES) == 0 else 1)
    chunk = n * cut // chunks

    f32, bf16 = jnp.float32, jnp.bfloat16
    dma = pltpu.SemaphoreType.DMA
    vmem = pl.BlockSpec(memory_space=VMEM)
    mixed, lse = pl.pallas_call(
        functools.partial(layer_kernel, n, n_tp, group, far, heads),
        out_shape=(
            jax.ShapeDtypeStruct((part, n * cut), bf16),
            jax.ShapeDtypeStruct((group * heads, rows), f32),
        ),
        in_specs=[pl.BlockSpec(memory_space=pltpu.HBM)] * 5,
        out_specs=(vmem, vmem),
        scratch_shapes=[
            VMEM((group, rows, model), bf16),
            VMEM((n, depth, 3 * LANES), bf16),
            VMEM((group, depth, 3 * LANES), bf16),
            VMEM((own, 2 * LANES), bf16), VMEM((far, own, 2 * LANES), bf16),
            VMEM((n * cut, width), bf16),
            VMEM((own, LANES), f32), VMEM((behind + own, LANES), f32), VMEM((behind + own, LANES), f32),
            VMEM((wide, own // wide, LANES), bf16),
            VMEM((wide, (far + 1) * own // wide, LANES), bf16), VMEM((wide, (far + 1) * own // wide, LANES), bf16),
            VMEM((wide, own // wide, LANES), f32), VMEM((wide, own // wide, LANES), f32),
            VMEM((2, rows // 2, rows // 2), bf16),
            VMEM((1 + len(dilation_rates), KEYS_BEHIND, 2 * KEYS_BEHIND), f32),
            VMEM((own, LANES), f32), VMEM((own, LANES), f32), VMEM((own, LANES), f32),
            VMEM((own, LANES), bf16), VMEM((group, heads, rows), f32), VMEM((group, heads, rows), f32),
            VMEM((rows, group * LANES), bf16),
            VMEM((chunks, rows, chunk), bf16), VMEM((n_tp, chunks, part, chunk), bf16),
            dma((3, group)), dma((4,)),
            dma((group,)), dma((group,)),
            dma((group, planes)), dma((group, planes)),
            dma((group, planes)), dma((group, planes)),
            dma((group, 2, 2)), dma((group, 2, 2)),
            dma((group, 2)), dma((group, 2)),
            dma((group, 2, 2, n_tp)), dma((group, 2, 2, n_tp)),
            dma((far + 1, group, 2)), dma((far + 1, group, 2)),
            dma((planes,)), dma((planes,)), dma((planes,)), dma((planes,)),
            dma((planes, group)), dma((planes, group)),
            dma((planes, group)), dma((planes, group)),
            dma((3,)), dma((3,)), dma((3,)), dma((3,)),
            dma((group,)), dma((group,)), dma((group,)), dma((group,)),
            dma((n_tp, chunks)), dma((n_tp, chunks)),
        ],
        compiler_params=pltpu.CompilerParams(collective_id=0, has_side_effects=True, vmem_limit_bytes=46 << 20),
        cost_estimate=pl.CostEstimate(
            flops=2 * own * model * 3 * LANES, bytes_accessed=1 << 24, transcendentals=1 << 22),
        name="layer",
    )(*[pltpu.with_memory_space_constraint(x, pltpu.HBM) for x in (w_query, w_key, w_value, tokens, turned)])
    return mixed, lse


def solution(mesh):
    placed = (P("sp", None), P("sp", "tp"), P("sp", "tp"), P("sp", "tp"), P("tp", "sp"))
    return jax.shard_map(
        functools.partial(shards, mesh.shape["sp"], mesh.shape["tp"]),
        mesh=mesh,
        in_specs=placed,
        out_specs=(P(("sp", "tp"), None), P("tp", "sp")),
        check_vma=False,
    )
```

```python
import functools

import jax
import jax.numpy as jnp
from jax import lax
from jax.experimental import pallas as pl
from jax.experimental.pallas import tpu as pltpu
from jax.sharding import PartitionSpec as P

HEAD_SIZE = 64
KEYS_BEHIND = 128
LANES = 128

dilation_rates = (1, 4, 16)
neg_big = -1e30

MESH = pl.DeviceIdType.MESH
VMEM = pltpu.VMEM


def at(sp, tp):
    return {"sp": sp, "tp": tp}


def layer_kernel(
    n, n_tp, group, far, heads, sum_pieces, wq_ref, wk_ref, wv_ref, tok_ref, o_ref, mixed_ref, lse_out_ref,
    tok_all, w_all, w_ref, kv_ref, halo_ref, o_all, qs, ks, vs, q_cls, k_cls, v_cls, out_cls, lse_cls, turn, bias,
    top_s, den_s, acc_s, att, lse_ref, lse_all, att_all, sums, sums_in,
    pack_sem, own_sem, w1_send, w1_recv, up_send, up_recv, down_send, down_recv, t_send, t_recv, d_send, d_recv,
    f_send, f_recv, h_send, h_recv, ou_send, ou_recv, od_send, od_recv, b_send, b_recv, c_send, c_recv,
    zu_send, zu_recv, zd_send, zd_recv, a_send, a_recv, l_send, l_recv, s_send, s_recv,
):
    sp, tp = lax.axis_index("sp"), lax.axis_index("tp")
    planes = n // group
    g, plane = lax.rem(sp, group), sp // group
    rows = tok_ref.shape[0]
    own = group * rows
    base = plane * own
    half = rows // 2
    bit_rows = half // (2 * n_tp)
    part = mixed_ref.shape[0]
    cut, width = o_ref.shape
    half_cut = cut // 2
    wide = dilation_rates[-1]
    behind = KEYS_BEHIND * dilation_rates[-2]
    run = half // wide
    old = far * own // wide

    above = lax.rem(sp + group, n)
    below = lax.rem(sp + n - group, n)

    def mate(i):
        return plane * group + (g ^ i)

    near = [i for i in (1, 2) if i < group]

    barrier = pltpu.get_barrier_semaphore()
    greeted = 0

    def greet(sp_to, tp_to):
        pl.semaphore_signal(barrier, inc=1, device_id=at(sp_to, tp_to), device_id_type=MESH)
        return 1

    for i in range(1, group):
        greeted += greet(mate(i), tp)
    if planes > 1:
        for h in range(1, max(far, 1) + 1):
            greeted += greet(lax.rem(sp + h * group, n), tp)
            greeted += greet(lax.rem(sp + n - h * group, n), tp)
    for j in range(1, n_tp):
        greeted += greet(sp, lax.rem(tp + j, n_tp))

    own_t = pltpu.make_async_copy(tok_ref, tok_all.at[g], own_sem.at[0])

    def strip(q, i, part_of=None):
        origin = q * group + (g ^ i)
        if part_of is None:
            return o_all.at[pl.ds(pl.multiple_of(origin * cut, cut), cut)]
        return o_all.at[pl.ds(pl.multiple_of(origin * cut + part_of * half_cut, half_cut), half_cut)]

    own_o = pltpu.make_async_copy(o_ref, strip(plane, 0), own_sem.at[3])

    def pack(t, i):
        source = (wq_ref, wk_ref, wv_ref)[t].at[:, pl.ds(pl.multiple_of((g ^ i) * LANES, LANES), LANES)]
        lanes = pl.ds(t * LANES, LANES)
        to = w_all.at[sp, :, lanes] if i == 0 else w_ref.at[i, :, lanes]
        return pltpu.make_async_copy(source, to, pack_sem.at[i])

    def all_of(view, sem):
        return pltpu.make_async_copy(view, view, sem)

    def packed(i):
        view = w_all.at[sp] if i == 0 else w_ref.at[i]
        all_of(view, pack_sem.at[i]).wait()

    for i in list(range(1, group)) + [0]:
        for t in range(3):
            pack(t, i).start()
    own_o.start()
    own_t.start()
    pl.semaphore_wait(barrier, greeted)

    def w_in_plane(i):
        return pltpu.make_async_remote_copy(
            src_ref=w_ref.at[i], dst_ref=w_all.at[sp], send_sem=w1_send.at[0], recv_sem=w1_recv.at[i - 1],
            device_id=at(mate(i), tp), device_id_type=MESH)

    def w_in_plane_arrives(i):
        return pltpu.make_async_remote_copy(
            src_ref=w_ref.at[i], dst_ref=w_all.at[mate(i)], send_sem=w1_send.at[0], recv_sem=w1_recv.at[i - 1],
            device_id=at(mate(i), tp), device_id_type=MESH)

    def slab(p, i):
        return w_all.at[lax.rem(p + 2 * planes, planes) * group + (g ^ i)]

    def up(i, k, p):
        return pltpu.make_async_remote_copy(
            src_ref=slab(p, i), dst_ref=slab(p, i), send_sem=up_send.at[k - 1], recv_sem=up_recv.at[i, k - 1],
            device_id=at(above, tp), device_id_type=MESH)

    def down(i, k, p):
        return pltpu.make_async_remote_copy(
            src_ref=slab(p, i), dst_ref=slab(p, i), send_sem=down_send.at[k - 1], recv_sem=down_recv.at[i, k - 1],
            device_id=at(below, tp), device_id_type=MESH)

    def o_up(k, p):
        ref = strip(lax.rem(p + 2 * planes, planes), 0)
        return pltpu.make_async_remote_copy(
            src_ref=ref, dst_ref=ref, send_sem=ou_send.at[k - 1], recv_sem=ou_recv.at[k - 1],
            device_id=at(above, tp), device_id_type=MESH)

    def o_down(k, p):
        ref = strip(lax.rem(p + 2 * planes, planes), 0)
        return pltpu.make_async_remote_copy(
            src_ref=ref, dst_ref=ref, send_sem=od_send.at[k - 1], recv_sem=od_recv.at[k - 1],
            device_id=at(below, tp), device_id_type=MESH)

    def when(condition, action):
        @pl.when(condition)
        def _():
            action()

    first, last = plane == 0, plane == planes - 1

    def relay(k, i):
        when(~last & (plane - k + 1 >= 0), lambda: up(i, k, plane - k + 1).start())
        when(~first & (plane + k - 1 < planes), lambda: down(i, k, plane + k - 1).start())

    def relayed(k, i):
        when(plane - k >= 0, lambda: up(i, k, plane - k).wait_recv())
        when(plane + k < planes, lambda: down(i, k, plane + k).wait_recv())

    def relay_left(k):
        slabs_of_a_plane = w_all.at[pl.ds(0, group)]
        when(~last & (plane - k + 1 >= 0), lambda: all_of(slabs_of_a_plane, up_send.at[k - 1]).wait())
        when(~first & (plane + k - 1 < planes), lambda: all_of(slabs_of_a_plane, down_send.at[k - 1]).wait())

    def o_relay(k):
        when(~last & (plane - k + 1 >= 0), lambda: o_up(k, plane - k + 1).start())
        when(~first & (plane + k - 1 < planes), lambda: o_down(k, plane + k - 1).start())

    def o_relay_left(k):
        when(~last & (plane - k + 1 >= 0), lambda: o_up(k, plane - k + 1).wait_send())
        when(~first & (plane + k - 1 < planes), lambda: o_down(k, plane + k - 1).wait_send())

    def hops(body):
        def one(k, _):
            for i in range(group):
                body(k, i)
            return _

        return one

    def nearest(m):
        left, right = plane, planes - 1 - plane
        short = jnp.minimum(left, right)
        zigzag = plane + (m // 2 if m % 2 == 0 else -((m + 1) // 2))
        return jnp.where(m <= 2 * short, zigzag, jnp.where(left < right, m, planes - 1 - m))

    def side_out(m, i):
        ref = strip(nearest(m), 0)
        return pltpu.make_async_remote_copy(
            src_ref=ref, dst_ref=ref, send_sem=b_send.at[0], recv_sem=b_recv.at[m, i - 1],
            device_id=at(mate(i), tp), device_id_type=MESH)

    def side_in(m, i):
        ref = strip(nearest(m), i)
        return pltpu.make_async_remote_copy(
            src_ref=ref, dst_ref=ref, send_sem=b_send.at[0], recv_sem=b_recv.at[m, i - 1],
            device_id=at(mate(i), tp), device_id_type=MESH)

    up_hops = min(2, planes - 1) if group == 4 else 0
    down_hops = min(3, planes - 1) if group == 4 else 0
    z_hops = max(up_hops, down_hops)
    z_least = min(up_hops, down_hops)

    def edge_at(m):
        return max(m - z_least, 0)

    def edge_out(m, i):
        ref = strip(nearest(m), i, i - 1)
        return pltpu.make_async_remote_copy(
            src_ref=ref, dst_ref=ref, send_sem=c_send.at[edge_at(m)], recv_sem=c_recv.at[edge_at(m), i - 1],
            device_id=at(mate(3 - i), tp), device_id_type=MESH)

    def edge_in(m, i):
        ref = strip(nearest(m), 3, i - 1)
        return pltpu.make_async_remote_copy(
            src_ref=ref, dst_ref=ref, send_sem=c_send.at[edge_at(m)], recv_sem=c_recv.at[edge_at(m), i - 1],
            device_id=at(mate(3 - i), tp), device_id_type=MESH)

    def sides(m):
        for i in near:
            side_out(m, i).start()

    def edge_goes(m, action):
        if group == 4:
            if m == 0:
                action()
            elif m > z_least:
                q = nearest(m)
                when((plane - q > up_hops) | (q - plane > down_hops), action)

    def edges(m):
        for i in near:
            side_in(m, i).wait_recv()
        edge_goes(m, lambda: [edge_out(m, i).start() for i in near])

    def edges_arrive(m):
        edge_goes(m, lambda: [edge_in(m, i).wait_recv() for i in near])

    def edges_left(m):
        edge_goes(m, lambda: all_of(strip(0, 0), c_send.at[edge_at(m)]).wait())

    def z_up(k, p):
        ref = strip(lax.rem(p + 2 * planes, planes), 3)
        return pltpu.make_async_remote_copy(
            src_ref=ref, dst_ref=ref, send_sem=zu_send.at[k - 1], recv_sem=zu_recv.at[k - 1],
            device_id=at(above, tp), device_id_type=MESH)

    def z_down(k, p):
        ref = strip(lax.rem(p + 2 * planes, planes), 3)
        return pltpu.make_async_remote_copy(
            src_ref=ref, dst_ref=ref, send_sem=zd_send.at[k - 1], recv_sem=zd_recv.at[k - 1],
            device_id=at(below, tp), device_id_type=MESH)

    def z_relay(k):
        if k <= up_hops:
            when(~last & (plane - k + 1 >= 0), lambda: z_up(k, plane - k + 1).start())
        if k <= down_hops:
            when(~first & (plane + k - 1 < planes), lambda: z_down(k, plane + k - 1).start())

    def z_forward(k):
        def up_on():
            z_up(k, plane - k).wait_recv()
            z_up(k + 1, plane - k).start()

        def down_on():
            z_down(k, plane + k).wait_recv()
            z_down(k + 1, plane + k).start()

        if k < up_hops:
            when(~last & (plane - k >= 0), up_on)
        if k < down_hops:
            when(~first & (plane + k < planes), down_on)

    def z_relayed(k):
        if k <= up_hops:
            ends = last if k < up_hops else True
            when(ends & (plane - k >= 0), lambda: z_up(k, plane - k).wait_recv())
        if k <= down_hops:
            ends = first if k < down_hops else True
            when(ends & (plane + k < planes), lambda: z_down(k, plane + k).wait_recv())

    def z_relay_left(k):
        if k <= up_hops:
            when(~last & (plane - k + 1 >= 0), lambda: z_up(k, plane - k + 1).wait_send())
        if k <= down_hops:
            when(~first & (plane + k - 1 < planes), lambda: z_down(k, plane + k - 1).wait_send())

    def o_relayed(k):
        def from_below():
            o_up(k, plane - k).wait_recv()

        def from_above():
            o_down(k, plane + k).wait_recv()

        when(plane - k >= 0, from_below)
        when(plane + k < planes, from_above)

    def bit(s, p, t):
        return pl.ds(pl.multiple_of(s * half + (p * n_tp + t) * bit_rows, bit_rows), bit_rows)

    def tokens_out(i, p, s):
        return pltpu.make_async_remote_copy(
            src_ref=tok_ref.at[bit(s, p, tp)], dst_ref=tok_all.at[g, bit(s, p, tp)],
            send_sem=t_send.at[0], recv_sem=t_recv.at[i - 1, p, s], device_id=at(mate(i), tp), device_id_type=MESH)

    def tokens_in(i, p, s):
        return pltpu.make_async_remote_copy(
            src_ref=tok_ref.at[bit(s, p, tp)], dst_ref=tok_all.at[g ^ i, bit(s, p, tp)],
            send_sem=t_send.at[0], recv_sem=t_recv.at[i - 1, p, s], device_id=at(mate(i), tp), device_id_type=MESH)

    def corner_out(i, s):
        ref = tok_all.at[g ^ i, bit(s, i - 1, tp)]
        return pltpu.make_async_remote_copy(
            src_ref=ref, dst_ref=ref, send_sem=d_send.at[0], recv_sem=d_recv.at[i - 1, s],
            device_id=at(mate(3 - i), tp), device_id_type=MESH)

    def corner_in(i, s):
        ref = tok_all.at[g ^ 3, bit(s, i - 1, tp)]
        return pltpu.make_async_remote_copy(
            src_ref=ref, dst_ref=ref, send_sem=d_send.at[0], recv_sem=d_recv.at[i - 1, s],
            device_id=at(mate(3 - i), tp), device_id_type=MESH)

    def across(i, p, s, j):
        ref = tok_all.at[g ^ i, bit(s, p, tp)]
        return pltpu.make_async_remote_copy(
            src_ref=ref, dst_ref=ref, send_sem=f_send.at[j - 1], recv_sem=f_recv.at[i - 1, s, j - 1],
            device_id=at(sp, lax.rem(tp + j, n_tp)), device_id_type=MESH)

    def to_other_cores(i, p, s):
        for j in range(1, n_tp):
            across(i, p, s, j).start()

    def piece(i, step):
        return step if i == 1 else 1 - step

    for i in range(1, group):
        packed(i)
        w_in_plane(i).start()
    packed(0)
    if planes > 1:
        relay(1, 0)
    for step in range(2):
        for s in range(2):
            for i in near:
                tokens_out(i, piece(i, step), s).start()
    for i in range(1, group):
        w_in_plane_arrives(i).wait_recv()
        if planes > 1:
            relay(1, i)

    def pass_on(k, i):
        relayed(k, i)
        relay(k + 1, i)

    row = lax.broadcasted_iota(jnp.int32, (KEYS_BEHIND, 2 * KEYS_BEHIND), 0)
    col = lax.broadcasted_iota(jnp.int32, (KEYS_BEHIND, 2 * KEYS_BEHIND), 1)
    dist = KEYS_BEHIND + row - col
    band = (dist >= 0) & (dist <= KEYS_BEHIND)
    bias[0] = jnp.where(band, 0.0, neg_big)
    for number, d in enumerate(dilation_rates):
        bias[1 + number] = jnp.where(band & (base // d - KEYS_BEHIND + col >= 0), 0.0, neg_big)
    to_row = lax.broadcasted_iota(jnp.int32, (half, half), 0)
    from_row = lax.broadcasted_iota(jnp.int32, (half, half), 1)
    turn[0] = (from_row == to_row % run * wide + to_row // run).astype(jnp.float32).astype(jnp.bfloat16)
    turn[1] = (from_row == to_row % wide * run + to_row // wide).astype(jnp.float32).astype(jnp.bfloat16)

    @pl.when(plane == 0)
    def _():
        ks[:behind] = jnp.zeros((behind, LANES), jnp.float32)
        vs[:behind] = jnp.zeros((behind, LANES), jnp.float32)

    for h in range(1, far + 1):
        @pl.when(plane - h < 0)
        def _():
            gone = slice((far - h) * own // wide, (far - h + 1) * own // wide)
            k_cls[:, gone] = jnp.zeros((wide, own // wide, LANES), jnp.bfloat16)
            v_cls[:, gone] = jnp.zeros((wide, own // wide, LANES), jnp.bfloat16)

    if planes > 1:
        lax.fori_loop(1, planes - 1, hops(pass_on), 0)
    own_o.wait()
    if planes > 1:
        o_relay(1)
    for s in range(2):
        for i in near:
            tokens_in(i, piece(i, 0), s).wait_recv()
            if group == 4:
                corner_out(i, s).start()
            to_other_cores(i, piece(i, 0), s)
    if planes > 1:
        for i in range(group):
            relayed(planes - 1, i)
    for s in range(2):
        for i in near:
            tokens_in(i, piece(i, 1), s).wait_recv()
            to_other_cores(i, piece(i, 1), s)
    if near:
        sides(0)
    own_t.wait()

    def halo_out(h, i, k):
        view = pl.ds(pl.multiple_of((g ^ i) * rows + k * half, half), half)
        return pltpu.make_async_remote_copy(
            src_ref=kv_ref.at[view], dst_ref=halo_ref.at[far - h, view],
            send_sem=h_send.at[h - 1], recv_sem=h_recv.at[h - 1, i, k],
            device_id=at(lax.rem(sp + h * group, n), tp), device_id_type=MESH)

    def by_classes(y):
        sorted_rows = jnp.dot(turn[0], y, preferred_element_type=jnp.float32).astype(jnp.bfloat16)
        return sorted_rows.reshape(wide, run, y.shape[1])

    def tile(i, k):
        block = g ^ i
        x = tok_all[block, pl.ds(pl.multiple_of(k * half, half), half), :]
        w = w_all[...].reshape(-1, 3 * LANES)
        y = jnp.dot(x, w, preferred_element_type=jnp.float32).astype(jnp.bfloat16)
        start = block * rows + k * half
        to = pl.ds(pl.multiple_of(start, half), half)
        past = pl.ds(pl.multiple_of(behind + start, half), half)
        kv_ref[to, :] = y[:, LANES:]
        qs[to, :] = y[:, :LANES].astype(jnp.float32) * HEAD_SIZE ** (-0.5)
        ks[past, :] = y[:, LANES : 2 * LANES].astype(jnp.float32)
        vs[past, :] = y[:, 2 * LANES :].astype(jnp.float32)
        by_class = by_classes(y)
        at_run = pl.ds(pl.multiple_of(start // wide, run), run)
        q_cls[:, at_run, :] = by_class[:, :, :LANES] * HEAD_SIZE ** (-0.5)
        past_run = pl.ds(pl.multiple_of(old + start // wide, run), run)
        k_cls[:, past_run, :] = by_class[:, :, LANES : 2 * LANES]
        v_cls[:, past_run, :] = by_class[:, :, 2 * LANES :]
        for h in range(1, far + 1):
            @pl.when(plane + h < planes)
            def _():
                halo_out(h, i, k).start()

    def tiles(picks, ready):
        def one(s, _):
            i, k = picks(s)
            ready(i, k)
            tile(i, k)
            return _

        lax.fori_loop(0, 2, one, 0)

    def crossed(i, k):
        for j in range(1, n_tp):
            all_of(tok_all.at[0, pl.ds(0, 2 * bit_rows)], f_recv.at[i - 1, k, j - 1]).wait()

    def o_pass(k):
        if k < planes:
            o_relayed(k)
            if k + 1 < planes:
                o_relay(k + 1)

    def unroll_of(trips):
        return next(u for u in (3, 2, 5, 1) if trips % u == 0)

    def attention(number, trips, place, opening=False):
        d = dilation_rates[number]
        step = min(KEYS_BEHIND, own // d)
        span = step + KEYS_BEHIND
        mask_at = 1 + number if opening else 0

        def block(index, _):
            cls, b = place(index)
            start = b * (step * d) + cls
            q_at = pl.ds(start, step, stride=d) if d > 1 else pl.ds(pl.multiple_of(start, step), step)
            k_start = behind - KEYS_BEHIND * d + start
            k_at = pl.ds(k_start, span, stride=d) if d > 1 else pl.ds(pl.multiple_of(k_start, step), span)
            q = qs[q_at, :]
            k = ks[k_at, :].astype(jnp.bfloat16)
            v = vs[k_at, :].astype(jnp.bfloat16)
            v = jnp.concatenate([v, jnp.ones((span, LANES), jnp.bfloat16)], axis=1)
            low = lax.broadcasted_iota(jnp.int32, (step, LANES), 1) < HEAD_SIZE
            q2 = jnp.concatenate([jnp.where(low, q, 0.0), jnp.where(low, 0.0, q)], axis=0).astype(jnp.bfloat16)
            s = lax.dot_general(q2, k, (((1,), (1,)), ((), ())), preferred_element_type=jnp.float32)
            seen = bias[mask_at, :step, :span]
            s = s + jnp.concatenate([seen, seen], axis=0)
            top = jnp.max(s, axis=1, keepdims=True)
            p = jnp.exp(s - top)
            o = jnp.dot(p.astype(jnp.bfloat16), v, preferred_element_type=jnp.float32)
            top = jnp.where(low, top[:step], top[step:])
            den = jnp.where(low, o[:step, LANES:], o[step:, LANES:])
            o = jnp.where(low, o[:step, :LANES], o[step:, :LANES])
            if number == 0:
                top_s[q_at, :] = top
                den_s[q_at, :] = den
                acc_s[q_at, :] = o
            else:
                was = top_s[q_at, :]
                new = jnp.maximum(was, top)
                old_scale, scale = jnp.exp(was - new), jnp.exp(top - new)
                top_s[q_at, :] = new
                den_s[q_at, :] = den_s[q_at, :] * old_scale + den * scale
                acc_s[q_at, :] = acc_s[q_at, :] * old_scale + o * scale
            return _

        lax.fori_loop(0, trips, block, 0, unroll=unroll_of(trips))

    ahead = group == 4 and rows == KEYS_BEHIND * dilation_rates[1]
    per = rows // KEYS_BEHIND
    ready_row = 1 + 2 * (g // 2)

    def early_near(u):
        return 0, jnp.where(u < 9, (g ^ (u // 3)) * per + 1 + lax.rem(u, 3), per * ready_row)

    def late_near(u):
        rest = jnp.where(u == 3, 2, 4 - ready_row)
        return 0, jnp.where(u < 3, (g ^ 3) * per + 1 + u, per * rest)

    def early_middle(u):
        return u, ready_row

    def late_middle(u):
        return lax.rem(u, 4), jnp.where(u < 4, 2, 4 - ready_row)

    tiles(lambda s: (0, s), lambda i, k: None)
    if group > 1:
        o_pass(1)
    if group == 2:
        tiles(lambda s: (1, s), crossed)
    if group == 4:
        tiles(lambda s: (1 + s, 0), crossed)
        tiles(lambda s: (1 + s, 1), crossed)
        if ahead:
            attention(0, 10, early_near)
        for s in range(2):
            for i in near:
                corner_in(i, s).wait_recv()
                to_other_cores(3, i - 1, s)
            if s == 0:
                if ahead:
                    attention(1, 4, early_middle)
            crossed(3, s)
            tile(3, s)
            if s == 0 and 2 < planes:
                o_relayed(2)
        if 3 < planes:
            o_relay(3)

    by_plane = group > 1
    def wide_attention(cls, _):
        step = own // wide
        span = step + KEYS_BEHIND
        q = q_cls[cls].astype(jnp.float32)
        k = k_cls[cls, old - KEYS_BEHIND :, :]
        v = v_cls[cls, old - KEYS_BEHIND :, :]
        v = jnp.concatenate([v, jnp.ones((span, LANES), jnp.bfloat16)], axis=1)
        low = lax.broadcasted_iota(jnp.int32, (step, LANES), 1) < HEAD_SIZE
        q2 = jnp.concatenate([jnp.where(low, q, 0.0), jnp.where(low, 0.0, q)], axis=0).astype(jnp.bfloat16)
        s = lax.dot_general(q2, k, (((1,), (1,)), ((), ())), preferred_element_type=jnp.float32)
        seen = bias[len(dilation_rates), :step, :span]
        s = s + jnp.concatenate([seen, seen], axis=0)
        top = jnp.max(s, axis=1, keepdims=True)
        p = jnp.exp(s - top)
        o = jnp.dot(p.astype(jnp.bfloat16), v, preferred_element_type=jnp.float32)
        top = jnp.where(low, top[:step], top[step:])
        den = jnp.where(low, o[:step, LANES:], o[step:, LANES:])
        out_cls[cls] = jnp.where(low, o[:step, :LANES], o[step:, :LANES]) / den
        lse_cls[cls] = top + jnp.log(den)
        return _

    counts = [own // d // min(KEYS_BEHIND, own // d) for d in dilation_rates[:-1]]

    strips = list(range(planes)) if by_plane else []
    early, late = strips[1:3], strips[3:]

    def later(k, _):
        o_relayed(k)
        when(k + 1 < planes, lambda: o_relay(k + 1))
        return _

    def spread_first():
        if by_plane:
            edges(0)
            for m in early:
                sides(m)

    def spread_rest():
        started = {1: 1, 2: 2, 4: 3}[group]
        if started < planes:
            lax.fori_loop(started, planes, later, 0)
        for m in late:
            sides(m)

    def sort(h):
        def unit(u, carry):
            i, k = u // 2, lax.rem(u, 2)
            halo_out(h, i, k).wait_recv()
            start = (g ^ i) * rows + k * half
            by_class = by_classes(halo_ref[far - h, pl.ds(pl.multiple_of(start, half), half), :])
            at_run = pl.ds(pl.multiple_of((far - h) * (own // wide) + start // wide, run), run)
            k_cls[:, at_run, :] = by_class[:, :, :LANES]
            v_cls[:, at_run, :] = by_class[:, :, LANES:]
            return carry

        lax.fori_loop(0, 2 * group, unit, 0)
        if h == 1:
            ks[:behind] = halo_ref[far - 1, own - behind :, :LANES].astype(jnp.float32)
            vs[:behind] = halo_ref[far - 1, own - behind :, LANES:].astype(jnp.float32)

    if ahead:
        attention(0, 5, late_near)
    else:
        for number, d in enumerate(dilation_rates[:-1]):
            if counts[number] > 1:
                attention(number, (counts[number] - 1) * d, lambda u, d=d: (lax.rem(u, d), 1 + u // d))
    spread_first()
    if ahead:
        attention(1, 8, late_middle)
    for h in range(1, far + 1):
        when(plane - h >= 0, functools.partial(sort, h))

    for number, d in enumerate(dilation_rates[:-1]):
        attention(number, d, lambda u: (u, 0), opening=True)
    edges_arrive(0)
    z_relay(1)
    lax.fori_loop(0, wide, wide_attention, 0, unroll=4)
    spread_rest()
    def att_lanes(i):
        return att_all.at[:, pl.ds(pl.multiple_of((g ^ i) * LANES, LANES), LANES)]

    def att_out(i):
        mine = pl.ds(pl.multiple_of((g ^ i) * rows, rows), rows)
        return pltpu.make_async_remote_copy(
            src_ref=att.at[mine], dst_ref=att_lanes(0), send_sem=a_send.at[0], recv_sem=a_recv.at[i - 1],
            device_id=at(mate(i), tp), device_id_type=MESH)

    def att_in(i):
        return pltpu.make_async_remote_copy(
            src_ref=att.at[pl.ds(0, rows)], dst_ref=att_lanes(i), send_sem=a_send.at[0], recv_sem=a_recv.at[i - 1],
            device_id=at(mate(i), tp), device_id_type=MESH)

    def lse_out(i):
        return pltpu.make_async_remote_copy(
            src_ref=lse_ref.at[g ^ i], dst_ref=lse_all.at[g], send_sem=l_send.at[0], recv_sem=l_recv.at[i - 1],
            device_id=at(mate(i), tp), device_id_type=MESH)

    def lse_in(i):
        return pltpu.make_async_remote_copy(
            src_ref=lse_ref.at[g ^ i], dst_ref=lse_all.at[g ^ i], send_sem=l_send.at[0], recv_sem=l_recv.at[i - 1],
            device_id=at(mate(i), tp), device_id_type=MESH)

    def split(x):
        high = x.astype(jnp.bfloat16)
        return [high, (x - high.astype(jnp.float32)).astype(jnp.bfloat16)]

    def finish(index, carry):
        i = lax.rem(index + 1, group)
        block = g ^ i
        for k in range(2):
            start = block * rows + k * half
            at_run = pl.ds(pl.multiple_of(start // wide, run), run)
            here = pl.ds(pl.multiple_of(start, half), half)
            terms = split(out_cls[:, at_run, :].reshape(half, LANES)) + split(lse_cls[:, at_run, :].reshape(half, LANES))
            back_in_order = jnp.dot(turn[1], jnp.concatenate(terms, axis=1), preferred_element_type=jnp.float32)
            out = back_in_order[:, :LANES] + back_in_order[:, LANES : 2 * LANES]
            lse = back_in_order[:, 2 * LANES : 3 * LANES] + back_in_order[:, 3 * LANES :]
            was = top_s[here, :]
            new = jnp.maximum(was, lse)
            old_scale, scale = jnp.exp(was - new), jnp.exp(lse - new)
            den = den_s[here, :] * old_scale + scale
            att[here, :] = ((acc_s[here, :] * old_scale + out * scale) / den).astype(jnp.bfloat16)
            lse = new + jnp.log(den)
            for t in range(half // LANES):
                columns = lse[t * LANES : (t + 1) * LANES].T
                off = k * half + t * LANES
                for h in range(heads):
                    lse_ref[block, h : h + 1, off : off + LANES] = columns[h * HEAD_SIZE : h * HEAD_SIZE + 1, :]

        @pl.when(i > 0)
        def _():
            att_out(i).start()
            lse_out(i).start()

        return carry

    lax.fori_loop(0, group, finish, 0)
    own_a = pltpu.make_async_copy(att.at[pl.ds(pl.multiple_of(g * rows, rows), rows)], att_lanes(0), own_sem.at[1])
    own_a.start()
    own_l = pltpu.make_async_copy(lse_ref.at[g], lse_all.at[g], own_sem.at[2])
    own_l.start()
    for m in early:
        edges(m)
    z_forward(1)
    for m in late:
        edges(m)
    for k in range(2, z_hops):
        z_forward(k)
    own_a.wait()
    for i in range(1, group):
        att_in(i).wait_recv()

    total_columns = sums.shape[1]
    if by_plane:
        strip_columns = group * cut
        pieces = [(m, 0, strip_columns) for m in strips]
        if group == 4 and 2 * cut % LANES == 0:
            pieces = pieces[:-1] + [(strips[-1], side, 2 * cut) for side in range(2)]
    else:
        pieces = [(c, 0, total_columns // sum_pieces) for c in range(sum_pieces)]

    def columns_of(c):
        m, side, size = pieces[c]
        if not by_plane:
            return pl.ds(m * size, size)
        start = nearest(m) * strip_columns
        if size < strip_columns:
            start = start + (side ^ (g // 2)) * size
        return pl.ds(pl.multiple_of(start, LANES), size)

    def rows_of(j):
        return pl.ds(pl.multiple_of(lax.rem(tp + j, n_tp) * part, part), part)

    def sum_out(c, j):
        return pltpu.make_async_remote_copy(
            src_ref=sums.at[rows_of(j), columns_of(c)], dst_ref=sums_in.at[j - 1, :, columns_of(c)],
            send_sem=s_send.at[j - 1], recv_sem=s_recv.at[j - 1, c],
            device_id=at(sp, lax.rem(tp + j, n_tp)), device_id_type=MESH)

    def multiply(c):
        w = o_all[columns_of(c), :]
        product = lax.dot_general(att_all[...], w, (((1,), (1,)), ((), ())), preferred_element_type=jnp.float32)
        sums[:, columns_of(c)] = product.astype(jnp.bfloat16)
        for j in range(1, n_tp):
            sum_out(c, j).start()

    def add_up(c):
        total = sums[rows_of(0), columns_of(c)].astype(jnp.float32)
        for j in range(1, n_tp):
            sum_out(c, j).wait_recv()
            total += sums_in[j - 1, :, columns_of(c)].astype(jnp.float32)
        mixed_ref[:, columns_of(c)] = total.astype(jnp.bfloat16)

    lag = 2
    for c, (m, side, size) in enumerate(pieces):
        if by_plane and (side == 1 or size == strip_columns):
            if m > 0:
                edges_arrive(m)
                z_relayed(m)
        multiply(c)
        if c >= lag:
            add_up(c - lag)
    for c in range(max(len(pieces) - lag, 0), len(pieces)):
        add_up(c)

    own_l.wait()
    for i in range(1, group):
        lse_in(i).wait_recv()
    for b in range(group):
        lse_out_ref[b * heads : (b + 1) * heads, :] = lse_all[b]

    if group > 1:
        all_of(w_ref.at[pl.ds(1, group - 1)], w1_send.at[0]).wait()
        for j in range(1, n_tp):
            all_of(tok_all.at[pl.ds(1, group - 1), pl.ds(0, 4 * bit_rows)], f_send.at[j - 1]).wait()
        all_of(tok_all.at[pl.ds(0, len(near)), pl.ds(0, 4 * bit_rows)], t_send.at[0]).wait()
        if group == 4:
            all_of(tok_all.at[0, pl.ds(0, 4 * bit_rows)], d_send.at[0]).wait()
    if planes > 1:
        lax.fori_loop(1, planes, lambda k, _: (relay_left(k), _)[1], 0)
        lax.fori_loop(1, planes, lambda k, _: (o_relay_left(k), _)[1], 0)
    for h in range(1, far + 1):
        when(plane + h < planes, lambda: all_of(kv_ref, h_send.at[h - 1]).wait())
    for j in range(1, n_tp):
        all_of(mixed_ref, s_send.at[j - 1]).wait()
    if group > 1:
        all_of(att.at[pl.ds(0, (group - 1) * rows)], a_send.at[0]).wait()
        all_of(lse_ref.at[pl.ds(0, group - 1)], l_send.at[0]).wait()
        all_of(o_all.at[pl.ds(0, planes * len(near) * cut)], b_send.at[0]).wait()
        for m in range(planes):
            edges_left(m)
        for k in range(1, z_hops + 1):
            z_relay_left(k)


def shards(n, n_tp, tokens, w_query, w_key, w_value, w_out):
    rows, model = tokens.shape
    depth, width = w_query.shape
    slabs = width // LANES
    reach = KEYS_BEHIND * dilation_rates[-1]
    group = 1
    while group < 4 and group * rows < reach and slabs % (2 * group) == 0 and n % (2 * group) == 0:
        group *= 2
    assert slabs == group
    far = (reach + group * rows - 1) // (group * rows)
    planes = n // group
    own = group * rows
    part = rows // n_tp
    heads = LANES // HEAD_SIZE

    turned = w_out.T
    cut = w_out.shape[1]
    wide = dilation_rates[-1]
    behind = KEYS_BEHIND * dilation_rates[-2]
    sum_pieces = 5 if group == 4 else planes if group > 1 else (4 if n * cut % (4 * LANES) == 0 else 1)
    sum_pieces = max(sum_pieces, planes + 1) if group > 1 else sum_pieces
    corners = max(planes - min(2, planes - 1), 1) if group == 4 else 1
    mates, others, hops, near = max(group - 1, 1), max(n_tp - 1, 1), max(planes - 1, 1), max(group // 2, 1)

    f32, bf16 = jnp.float32, jnp.bfloat16
    dma = pltpu.SemaphoreType.DMA
    vmem = pl.BlockSpec(memory_space=VMEM)
    mixed, lse = pl.pallas_call(
        functools.partial(layer_kernel, n, n_tp, group, far, heads, sum_pieces),
        out_shape=(
            jax.ShapeDtypeStruct((part, n * cut), bf16),
            jax.ShapeDtypeStruct((group * heads, rows), f32),
        ),
        in_specs=[pl.BlockSpec(memory_space=pltpu.HBM)] * 5,
        out_specs=(vmem, vmem),
        scratch_shapes=[
            VMEM((group, rows, model), bf16),
            VMEM((n, depth, 3 * LANES), bf16),
            VMEM((group, depth, 3 * LANES), bf16),
            VMEM((own, 2 * LANES), bf16), VMEM((far, own, 2 * LANES), bf16),
            VMEM((n * cut, width), bf16),
            VMEM((own, LANES), f32), VMEM((behind + own, LANES), f32), VMEM((behind + own, LANES), f32),
            VMEM((wide, own // wide, LANES), bf16),
            VMEM((wide, (far + 1) * own // wide, LANES), bf16), VMEM((wide, (far + 1) * own // wide, LANES), bf16),
            VMEM((wide, own // wide, LANES), f32), VMEM((wide, own // wide, LANES), f32),
            VMEM((2, rows // 2, rows // 2), bf16),
            VMEM((1 + len(dilation_rates), KEYS_BEHIND, 2 * KEYS_BEHIND), f32),
            VMEM((own, LANES), f32), VMEM((own, LANES), f32), VMEM((own, LANES), f32),
            VMEM((own, LANES), bf16), VMEM((group, heads, rows), f32), VMEM((group, heads, rows), f32),
            VMEM((rows, group * LANES), bf16),
            VMEM((rows, n * cut), bf16), VMEM((others, part, n * cut), bf16),
            dma((group,)), dma((4,)),
            dma((1,)), dma((mates,)),
            dma((hops,)), dma((group, hops)),
            dma((hops,)), dma((group, hops)),
            dma((1,)), dma((near, 2, 2)),
            dma((1,)), dma((near, 2)),
            dma((others,)), dma((mates, 2, others)),
            dma((far,)), dma((far, group, 2)),
            dma((hops,)), dma((hops,)), dma((hops,)), dma((hops,)),
            dma((1,)), dma((planes if group > 1 else 1, near)),
            dma((corners,)), dma((corners, near)),
            dma((2,)), dma((2,)), dma((3,)), dma((3,)),
            dma((1,)), dma((mates,)), dma((1,)), dma((mates,)),
            dma((others,)), dma((others, sum_pieces)),
        ],
        compiler_params=pltpu.CompilerParams(collective_id=0, has_side_effects=True, vmem_limit_bytes=46 << 20),
        cost_estimate=pl.CostEstimate(
            flops=2 * own * model * 3 * LANES, bytes_accessed=1 << 24, transcendentals=1 << 22),
        name="layer",
    )(*[pltpu.with_memory_space_constraint(x, pltpu.HBM) for x in (w_query, w_key, w_value, tokens, turned)])
    return mixed, lse


def solution(mesh):
    placed = (P("sp", None), P("sp", "tp"), P("sp", "tp"), P("sp", "tp"), P("tp", "sp"))
    return jax.shard_map(
        functools.partial(shards, mesh.shape["sp"], mesh.shape["tp"]),
        mesh=mesh,
        in_specs=placed,
        out_specs=(P(("sp", "tp"), None), P("tp", "sp")),
        check_vma=False,
    )
```

```python
import functools

import jax
import jax.numpy as jnp
from jax import lax
from jax.experimental import pallas as pl
from jax.experimental.pallas import tpu as pltpu
from jax.sharding import PartitionSpec as P

HEAD_SIZE = 64
KEYS_BEHIND = 128
LANES = 128

dilation_rates = (1, 4, 16)
neg_big = -1e30

MESH = pl.DeviceIdType.MESH
VMEM = pltpu.VMEM


def at(sp, tp):
    return {"sp": sp, "tp": tp}


def layer_kernel(
    n, n_tp, group, far, heads, sum_pieces, wq_ref, wk_ref, wv_ref, tok_ref, o_ref, mixed_ref, lse_out_ref,
    tok_all, w_all, w_ref, kv_ref, halo_ref, o_all, qs, ks, vs, q_cls, k_cls, v_cls, out_cls, lse_cls, turn, bias,
    top_s, den_s, acc_s, att, lse_ref, lse_all, att_all, sums, sums_in,
    pack_sem, own_sem, w1_send, w1_recv, up_send, up_recv, down_send, down_recv, t_send, t_recv, d_send, d_recv,
    f_send, f_recv, h_send, h_recv, ou_send, ou_recv, od_send, od_recv, b_send, b_recv, c_send, c_recv,
    zu_send, zu_recv, zd_send, zd_recv, a_send, a_recv, l_send, l_recv, s_send, s_recv,
):
    sp, tp = lax.axis_index("sp"), lax.axis_index("tp")
    planes = n // group
    g, plane = lax.rem(sp, group), sp // group
    rows = tok_ref.shape[0]
    own = group * rows
    base = plane * own
    half = rows // 2
    bit_rows = half // (2 * n_tp)
    part = mixed_ref.shape[0]
    cut, width = o_ref.shape
    half_cut = cut // 2
    wide = dilation_rates[-1]
    behind = KEYS_BEHIND * dilation_rates[-2]
    run = half // wide
    old = far * own // wide

    above = lax.rem(sp + group, n)
    below = lax.rem(sp + n - group, n)

    def mate(i):
        return plane * group + (g ^ i)

    near = [i for i in (1, 2) if i < group]

    barrier = pltpu.get_barrier_semaphore()
    greeted = 0

    def greet(sp_to, tp_to):
        pl.semaphore_signal(barrier, inc=1, device_id=at(sp_to, tp_to), device_id_type=MESH)
        return 1

    for i in range(1, group):
        greeted += greet(mate(i), tp)
    if planes > 1:
        for h in range(1, max(far, 1) + 1):
            greeted += greet(lax.rem(sp + h * group, n), tp)
            greeted += greet(lax.rem(sp + n - h * group, n), tp)
    for j in range(1, n_tp):
        greeted += greet(sp, lax.rem(tp + j, n_tp))

    own_t = pltpu.make_async_copy(tok_ref, tok_all.at[g], own_sem.at[0])

    def strip(q, i, part_of=None):
        origin = q * group + (g ^ i)
        if part_of is None:
            return o_all.at[pl.ds(pl.multiple_of(origin * cut, cut), cut)]
        return o_all.at[pl.ds(pl.multiple_of(origin * cut + part_of * half_cut, half_cut), half_cut)]

    own_o = pltpu.make_async_copy(o_ref, strip(plane, 0), own_sem.at[3])

    def pack(t, i):
        source = (wq_ref, wk_ref, wv_ref)[t].at[:, pl.ds(pl.multiple_of((g ^ i) * LANES, LANES), LANES)]
        lanes = pl.ds(t * LANES, LANES)
        to = w_all.at[sp, :, lanes] if i == 0 else w_ref.at[i, :, lanes]
        return pltpu.make_async_copy(source, to, pack_sem.at[i])

    def all_of(view, sem):
        return pltpu.make_async_copy(view, view, sem)

    def packed(i):
        view = w_all.at[sp] if i == 0 else w_ref.at[i]
        all_of(view, pack_sem.at[i]).wait()

    for i in list(range(1, group)) + [0]:
        for t in range(3):
            pack(t, i).start()
    own_o.start()
    own_t.start()
    pl.semaphore_wait(barrier, greeted)

    def w_in_plane(i):
        return pltpu.make_async_remote_copy(
            src_ref=w_ref.at[i], dst_ref=w_all.at[sp], send_sem=w1_send.at[0], recv_sem=w1_recv.at[i - 1],
            device_id=at(mate(i), tp), device_id_type=MESH)

    def w_in_plane_arrives(i):
        return pltpu.make_async_remote_copy(
            src_ref=w_ref.at[i], dst_ref=w_all.at[mate(i)], send_sem=w1_send.at[0], recv_sem=w1_recv.at[i - 1],
            device_id=at(mate(i), tp), device_id_type=MESH)

    def slab(p, i):
        return w_all.at[lax.rem(p + 2 * planes, planes) * group + (g ^ i)]

    def up(i, k, p):
        return pltpu.make_async_remote_copy(
            src_ref=slab(p, i), dst_ref=slab(p, i), send_sem=up_send.at[k - 1], recv_sem=up_recv.at[i, k - 1],
            device_id=at(above, tp), device_id_type=MESH)

    def down(i, k, p):
        return pltpu.make_async_remote_copy(
            src_ref=slab(p, i), dst_ref=slab(p, i), send_sem=down_send.at[k - 1], recv_sem=down_recv.at[i, k - 1],
            device_id=at(below, tp), device_id_type=MESH)

    def o_up(k, p):
        ref = strip(lax.rem(p + 2 * planes, planes), 0)
        return pltpu.make_async_remote_copy(
            src_ref=ref, dst_ref=ref, send_sem=ou_send.at[k - 1], recv_sem=ou_recv.at[k - 1],
            device_id=at(above, tp), device_id_type=MESH)

    def o_down(k, p):
        ref = strip(lax.rem(p + 2 * planes, planes), 0)
        return pltpu.make_async_remote_copy(
            src_ref=ref, dst_ref=ref, send_sem=od_send.at[k - 1], recv_sem=od_recv.at[k - 1],
            device_id=at(below, tp), device_id_type=MESH)

    def when(condition, action):
        @pl.when(condition)
        def _():
            action()

    first, last = plane == 0, plane == planes - 1

    def relay(k, i):
        when(~last & (plane - k + 1 >= 0), lambda: up(i, k, plane - k + 1).start())
        when(~first & (plane + k - 1 < planes), lambda: down(i, k, plane + k - 1).start())

    def relayed(k, i):
        when(plane - k >= 0, lambda: up(i, k, plane - k).wait_recv())
        when(plane + k < planes, lambda: down(i, k, plane + k).wait_recv())

    def relay_left(k):
        slabs_of_a_plane = w_all.at[pl.ds(0, group)]
        when(~last & (plane - k + 1 >= 0), lambda: all_of(slabs_of_a_plane, up_send.at[k - 1]).wait())
        when(~first & (plane + k - 1 < planes), lambda: all_of(slabs_of_a_plane, down_send.at[k - 1]).wait())

    def o_relay(k):
        when(~last & (plane - k + 1 >= 0), lambda: o_up(k, plane - k + 1).start())
        when(~first & (plane + k - 1 < planes), lambda: o_down(k, plane + k - 1).start())

    def o_relay_left(k):
        when(~last & (plane - k + 1 >= 0), lambda: o_up(k, plane - k + 1).wait_send())
        when(~first & (plane + k - 1 < planes), lambda: o_down(k, plane + k - 1).wait_send())

    def hops(body):
        def one(k, _):
            for i in range(group):
                body(k, i)
            return _

        return one

    def nearest(m):
        left, right = plane, planes - 1 - plane
        short = jnp.minimum(left, right)
        zigzag = plane + (m // 2 if m % 2 == 0 else -((m + 1) // 2))
        return jnp.where(m <= 2 * short, zigzag, jnp.where(left < right, m, planes - 1 - m))

    def side_out(m, i):
        ref = strip(nearest(m), 0)
        return pltpu.make_async_remote_copy(
            src_ref=ref, dst_ref=ref, send_sem=b_send.at[0], recv_sem=b_recv.at[m, i - 1],
            device_id=at(mate(i), tp), device_id_type=MESH)

    def side_in(m, i):
        ref = strip(nearest(m), i)
        return pltpu.make_async_remote_copy(
            src_ref=ref, dst_ref=ref, send_sem=b_send.at[0], recv_sem=b_recv.at[m, i - 1],
            device_id=at(mate(i), tp), device_id_type=MESH)

    up_hops = min(2, planes - 1) if group == 4 else 0
    down_hops = min(3, planes - 1) if group == 4 else 0
    z_hops = max(up_hops, down_hops)
    z_least = min(up_hops, down_hops)

    def edge_at(m):
        return max(m - z_least, 0)

    def edge_out(m, i):
        ref = strip(nearest(m), i, i - 1)
        return pltpu.make_async_remote_copy(
            src_ref=ref, dst_ref=ref, send_sem=c_send.at[edge_at(m)], recv_sem=c_recv.at[edge_at(m), i - 1],
            device_id=at(mate(3 - i), tp), device_id_type=MESH)

    def edge_in(m, i):
        ref = strip(nearest(m), 3, i - 1)
        return pltpu.make_async_remote_copy(
            src_ref=ref, dst_ref=ref, send_sem=c_send.at[edge_at(m)], recv_sem=c_recv.at[edge_at(m), i - 1],
            device_id=at(mate(3 - i), tp), device_id_type=MESH)

    def sides(m):
        for i in near:
            side_out(m, i).start()

    def beyond(m):
        return (plane - nearest(m) > up_hops) | (nearest(m) - plane > down_hops)

    def edge_goes(m, action):
        if group == 4:
            if m == 0:
                action()
            elif m > z_least:
                when(beyond(m), action)

    def edges_on(m):
        for i in near:
            side_in(m, i).wait_recv()
            if group == 4:
                edge_out(m, i).start()

    def sides_arrive(m):
        def wait():
            for i in near:
                side_in(m, i).wait_recv()

        if group == 4 and m > z_least:
            when(~beyond(m), wait)
        elif m > 0:
            wait()

    def edges_arrive(m):
        edge_goes(m, lambda: [edge_in(m, i).wait_recv() for i in near])

    def edges_left(m):
        edge_goes(m, lambda: all_of(strip(0, 0), c_send.at[edge_at(m)]).wait())

    def z_up(k, p):
        ref = strip(lax.rem(p + 2 * planes, planes), 3)
        return pltpu.make_async_remote_copy(
            src_ref=ref, dst_ref=ref, send_sem=zu_send.at[k - 1], recv_sem=zu_recv.at[k - 1],
            device_id=at(above, tp), device_id_type=MESH)

    def z_down(k, p):
        ref = strip(lax.rem(p + 2 * planes, planes), 3)
        return pltpu.make_async_remote_copy(
            src_ref=ref, dst_ref=ref, send_sem=zd_send.at[k - 1], recv_sem=zd_recv.at[k - 1],
            device_id=at(below, tp), device_id_type=MESH)

    def z_relay(k):
        if k <= up_hops:
            when(~last & (plane - k + 1 >= 0), lambda: z_up(k, plane - k + 1).start())
        if k <= down_hops:
            when(~first & (plane + k - 1 < planes), lambda: z_down(k, plane + k - 1).start())

    def z_forward(k):
        def up_on():
            z_up(k, plane - k).wait_recv()
            z_up(k + 1, plane - k).start()

        def down_on():
            z_down(k, plane + k).wait_recv()
            z_down(k + 1, plane + k).start()

        if k < up_hops:
            when(~last & (plane - k >= 0), up_on)
        if k < down_hops:
            when(~first & (plane + k < planes), down_on)

    def z_relayed(k):
        if k <= up_hops:
            ends = last if k < up_hops else True
            when(ends & (plane - k >= 0), lambda: z_up(k, plane - k).wait_recv())
        if k <= down_hops:
            ends = first if k < down_hops else True
            when(ends & (plane + k < planes), lambda: z_down(k, plane + k).wait_recv())

    def z_relay_left(k):
        if k <= up_hops:
            when(~last & (plane - k + 1 >= 0), lambda: z_up(k, plane - k + 1).wait_send())
        if k <= down_hops:
            when(~first & (plane + k - 1 < planes), lambda: z_down(k, plane + k - 1).wait_send())

    def o_relayed(k):
        def from_below():
            o_up(k, plane - k).wait_recv()

        def from_above():
            o_down(k, plane + k).wait_recv()

        when(plane - k >= 0, from_below)
        when(plane + k < planes, from_above)

    def bit(s, p, t):
        return pl.ds(pl.multiple_of(s * half + (p * n_tp + t) * bit_rows, bit_rows), bit_rows)

    def tokens_out(i, p, s):
        return pltpu.make_async_remote_copy(
            src_ref=tok_ref.at[bit(s, p, tp)], dst_ref=tok_all.at[g, bit(s, p, tp)],
            send_sem=t_send.at[0], recv_sem=t_recv.at[i - 1, p, s], device_id=at(mate(i), tp), device_id_type=MESH)

    def tokens_in(i, p, s):
        return pltpu.make_async_remote_copy(
            src_ref=tok_ref.at[bit(s, p, tp)], dst_ref=tok_all.at[g ^ i, bit(s, p, tp)],
            send_sem=t_send.at[0], recv_sem=t_recv.at[i - 1, p, s], device_id=at(mate(i), tp), device_id_type=MESH)

    def corner_out(i, s):
        ref = tok_all.at[g ^ i, bit(s, i - 1, tp)]
        return pltpu.make_async_remote_copy(
            src_ref=ref, dst_ref=ref, send_sem=d_send.at[0], recv_sem=d_recv.at[i - 1, s],
            device_id=at(mate(3 - i), tp), device_id_type=MESH)

    def corner_in(i, s):
        ref = tok_all.at[g ^ 3, bit(s, i - 1, tp)]
        return pltpu.make_async_remote_copy(
            src_ref=ref, dst_ref=ref, send_sem=d_send.at[0], recv_sem=d_recv.at[i - 1, s],
            device_id=at(mate(3 - i), tp), device_id_type=MESH)

    def across(i, p, s, j):
        ref = tok_all.at[g ^ i, bit(s, p, tp)]
        return pltpu.make_async_remote_copy(
            src_ref=ref, dst_ref=ref, send_sem=f_send.at[j - 1], recv_sem=f_recv.at[i - 1, s, j - 1],
            device_id=at(sp, lax.rem(tp + j, n_tp)), device_id_type=MESH)

    def to_other_cores(i, p, s):
        for j in range(1, n_tp):
            across(i, p, s, j).start()

    def piece(i, step):
        return step if i == 1 else 1 - step

    for i in range(1, group):
        packed(i)
        w_in_plane(i).start()
    packed(0)
    if planes > 1:
        relay(1, 0)
    for step in range(2):
        for s in range(2):
            for i in near:
                tokens_out(i, piece(i, step), s).start()
    for i in range(1, group):
        w_in_plane_arrives(i).wait_recv()
        if planes > 1:
            relay(1, i)

    def pass_on(k, i):
        relayed(k, i)
        relay(k + 1, i)

    row = lax.broadcasted_iota(jnp.int32, (KEYS_BEHIND, 2 * KEYS_BEHIND), 0)
    col = lax.broadcasted_iota(jnp.int32, (KEYS_BEHIND, 2 * KEYS_BEHIND), 1)
    dist = KEYS_BEHIND + row - col
    band = (dist >= 0) & (dist <= KEYS_BEHIND)
    bias[0] = jnp.where(band, 0.0, neg_big)
    for number, d in enumerate(dilation_rates):
        bias[1 + number] = jnp.where(band & (base // d - KEYS_BEHIND + col >= 0), 0.0, neg_big)
    to_row = lax.broadcasted_iota(jnp.int32, (half, half), 0)
    from_row = lax.broadcasted_iota(jnp.int32, (half, half), 1)
    turn[0] = (from_row == to_row % run * wide + to_row // run).astype(jnp.float32).astype(jnp.bfloat16)
    turn[1] = (from_row == to_row % wide * run + to_row // wide).astype(jnp.float32).astype(jnp.bfloat16)

    @pl.when(plane == 0)
    def _():
        ks[:behind] = jnp.zeros((behind, LANES), jnp.float32)
        vs[:behind] = jnp.zeros((behind, LANES), jnp.float32)

    for h in range(1, far + 1):
        @pl.when(plane - h < 0)
        def _():
            gone = slice((far - h) * own // wide, (far - h + 1) * own // wide)
            k_cls[:, gone] = jnp.zeros((wide, own // wide, LANES), jnp.bfloat16)
            v_cls[:, gone] = jnp.zeros((wide, own // wide, LANES), jnp.bfloat16)

    if planes > 1:
        lax.fori_loop(1, planes - 1, hops(pass_on), 0)
    own_o.wait()
    if planes > 1:
        o_relay(1)
    for s in range(2):
        for i in near:
            tokens_in(i, piece(i, 0), s).wait_recv()
            if group == 4:
                corner_out(i, s).start()
            to_other_cores(i, piece(i, 0), s)
    if planes > 1:
        for i in range(group):
            relayed(planes - 1, i)
    for s in range(2):
        for i in near:
            tokens_in(i, piece(i, 1), s).wait_recv()
            to_other_cores(i, piece(i, 1), s)
    if near:
        sides(0)
    own_t.wait()

    def halo_out(h, i, k):
        view = pl.ds(pl.multiple_of((g ^ i) * rows + k * half, half), half)
        return pltpu.make_async_remote_copy(
            src_ref=kv_ref.at[view], dst_ref=halo_ref.at[far - h, view],
            send_sem=h_send.at[h - 1], recv_sem=h_recv.at[h - 1, i, k],
            device_id=at(lax.rem(sp + h * group, n), tp), device_id_type=MESH)

    def by_classes(y):
        sorted_rows = jnp.dot(turn[0], y, preferred_element_type=jnp.float32).astype(jnp.bfloat16)
        return sorted_rows.reshape(wide, run, y.shape[1])

    def sort_unit(h):
        def unit(u, carry):
            i, k = u // 2, lax.rem(u, 2)
            halo_out(h, i, k).wait_recv()
            start = (g ^ i) * rows + k * half
            by_class = by_classes(halo_ref[far - h, pl.ds(pl.multiple_of(start, half), half), :])
            at_run = pl.ds(pl.multiple_of((far - h) * (own // wide) + start // wide, run), run)
            k_cls[:, at_run, :] = by_class[:, :, :LANES]
            v_cls[:, at_run, :] = by_class[:, :, LANES:]
            return carry

        return unit

    def tile(i, k):
        block = g ^ i
        x = tok_all[block, pl.ds(pl.multiple_of(k * half, half), half), :]
        w = w_all[...].reshape(-1, 3 * LANES)
        y = jnp.dot(x, w, preferred_element_type=jnp.float32).astype(jnp.bfloat16)
        start = block * rows + k * half
        to = pl.ds(pl.multiple_of(start, half), half)
        past = pl.ds(pl.multiple_of(behind + start, half), half)
        kv_ref[to, :] = y[:, LANES:]
        qs[to, :] = y[:, :LANES].astype(jnp.float32) * HEAD_SIZE ** (-0.5)
        ks[past, :] = y[:, LANES : 2 * LANES].astype(jnp.float32)
        vs[past, :] = y[:, 2 * LANES :].astype(jnp.float32)
        by_class = by_classes(y)
        at_run = pl.ds(pl.multiple_of(start // wide, run), run)
        q_cls[:, at_run, :] = by_class[:, :, :LANES] * HEAD_SIZE ** (-0.5)
        past_run = pl.ds(pl.multiple_of(old + start // wide, run), run)
        k_cls[:, past_run, :] = by_class[:, :, LANES : 2 * LANES]
        v_cls[:, past_run, :] = by_class[:, :, 2 * LANES :]
        for h in range(1, far + 1):
            @pl.when(plane + h < planes)
            def _():
                halo_out(h, i, k).start()

    def tiles(picks, ready):
        def one(s, _):
            i, k = picks(s)
            ready(i, k)
            tile(i, k)
            return _

        lax.fori_loop(0, 2, one, 0)

    def crossed(i, k):
        for j in range(1, n_tp):
            all_of(tok_all.at[0, pl.ds(0, 2 * bit_rows)], f_recv.at[i - 1, k, j - 1]).wait()

    def o_pass(k):
        if k < planes:
            o_relayed(k)
            if k + 1 < planes:
                o_relay(k + 1)

    def unroll_of(trips):
        return next(u for u in (3, 2, 5, 1) if trips % u == 0)

    def attention(number, trips, place, opening=False):
        d = dilation_rates[number]
        step = min(KEYS_BEHIND, own // d)
        span = step + KEYS_BEHIND
        mask_at = 1 + number if opening else 0

        def block(index, _):
            cls, b = place(index)
            start = b * (step * d) + cls
            q_at = pl.ds(start, step, stride=d) if d > 1 else pl.ds(pl.multiple_of(start, step), step)
            k_start = behind - KEYS_BEHIND * d + start
            k_at = pl.ds(k_start, span, stride=d) if d > 1 else pl.ds(pl.multiple_of(k_start, step), span)
            q = qs[q_at, :]
            k = ks[k_at, :].astype(jnp.bfloat16)
            v = vs[k_at, :].astype(jnp.bfloat16)
            v = jnp.concatenate([v, jnp.ones((span, LANES), jnp.bfloat16)], axis=1)
            low = lax.broadcasted_iota(jnp.int32, (step, LANES), 1) < HEAD_SIZE
            q2 = jnp.concatenate([jnp.where(low, q, 0.0), jnp.where(low, 0.0, q)], axis=0).astype(jnp.bfloat16)
            s = lax.dot_general(q2, k, (((1,), (1,)), ((), ())), preferred_element_type=jnp.float32)
            seen = bias[mask_at, :step, :span]
            s = s + jnp.concatenate([seen, seen], axis=0)
            top = jnp.max(s, axis=1, keepdims=True)
            p = jnp.exp(s - top)
            o = jnp.dot(p.astype(jnp.bfloat16), v, preferred_element_type=jnp.float32)
            top = jnp.where(low, top[:step], top[step:])
            den = jnp.where(low, o[:step, LANES:], o[step:, LANES:])
            o = jnp.where(low, o[:step, :LANES], o[step:, :LANES])
            if number == 0:
                top_s[q_at, :] = top
                den_s[q_at, :] = den
                acc_s[q_at, :] = o
            else:
                was = top_s[q_at, :]
                new = jnp.maximum(was, top)
                old_scale, scale = jnp.exp(was - new), jnp.exp(top - new)
                top_s[q_at, :] = new
                den_s[q_at, :] = den_s[q_at, :] * old_scale + den * scale
                acc_s[q_at, :] = acc_s[q_at, :] * old_scale + o * scale
            return _

        lax.fori_loop(0, trips, block, 0, unroll=unroll_of(trips))

    ahead = group == 4 and rows == KEYS_BEHIND * dilation_rates[1]
    per = rows // KEYS_BEHIND
    ready_row = 1 + 2 * (g // 2)

    def early_near(u):
        return 0, jnp.where(u < 9, (g ^ (u // 3)) * per + 1 + lax.rem(u, 3), per * ready_row)

    def late_near(u):
        rest = jnp.where(u == 3, 2, 4 - ready_row)
        return 0, jnp.where(u < 3, (g ^ 3) * per + 1 + u, per * rest)

    def early_middle(u):
        return u, ready_row

    def late_middle(u):
        return lax.rem(u, 4), jnp.where(u < 4, 2, 4 - ready_row)

    tiles(lambda s: (0, s), lambda i, k: None)
    if group > 1:
        o_pass(1)
    if group == 2:
        tiles(lambda s: (1, s), crossed)
    if group == 4:
        tiles(lambda s: (1 + s, 0), crossed)
        tiles(lambda s: (1 + s, 1), crossed)
        if ahead:
            attention(0, 10, early_near)
        for s in range(2):
            if s == 1:
                when(plane >= 1, lambda: lax.fori_loop(0, 2, sort_unit(1), 0))
            for i in near:
                corner_in(i, s).wait_recv()
                to_other_cores(3, i - 1, s)
            if s == 0:
                if ahead:
                    attention(1, 4, early_middle)
            crossed(3, s)
            tile(3, s)
            if s == 0 and 2 < planes:
                o_relayed(2)
        if 3 < planes:
            o_relay(3)

    by_plane = group > 1
    def wide_attention(cls, _):
        step = own // wide
        span = step + KEYS_BEHIND
        q = q_cls[cls].astype(jnp.float32)
        k = k_cls[cls, old - KEYS_BEHIND :, :]
        v = v_cls[cls, old - KEYS_BEHIND :, :]
        v = jnp.concatenate([v, jnp.ones((span, LANES), jnp.bfloat16)], axis=1)
        low = lax.broadcasted_iota(jnp.int32, (step, LANES), 1) < HEAD_SIZE
        q2 = jnp.concatenate([jnp.where(low, q, 0.0), jnp.where(low, 0.0, q)], axis=0).astype(jnp.bfloat16)
        s = lax.dot_general(q2, k, (((1,), (1,)), ((), ())), preferred_element_type=jnp.float32)
        seen = bias[len(dilation_rates), :step, :span]
        s = s + jnp.concatenate([seen, seen], axis=0)
        top = jnp.max(s, axis=1, keepdims=True)
        p = jnp.exp(s - top)
        o = jnp.dot(p.astype(jnp.bfloat16), v, preferred_element_type=jnp.float32)
        top = jnp.where(low, top[:step], top[step:])
        den = jnp.where(low, o[:step, LANES:], o[step:, LANES:])
        out_cls[cls] = jnp.where(low, o[:step, :LANES], o[step:, :LANES]) / den
        lse_cls[cls] = top + jnp.log(den)
        return _

    counts = [own // d // min(KEYS_BEHIND, own // d) for d in dilation_rates[:-1]]

    strips = list(range(planes)) if by_plane else []
    early, late = strips[1:3], strips[3:]

    def later(k, _):
        o_relayed(k)
        when(k + 1 < planes, lambda: o_relay(k + 1))
        return _

    def spread_first():
        if by_plane:
            edges_on(0)
            for m in early:
                sides(m)

    def spread_rest():
        started = {1: 1, 2: 2, 4: 3}[group]
        if started < planes:
            lax.fori_loop(started, planes, later, 0)
        for m in late:
            when(relayed_in_plane(m), lambda: sides(m))

    def relayed_in_plane(m):
        return beyond(m) if group == 4 else plane >= 0

    def sort(h):
        unit = sort_unit(h)
        lax.fori_loop(begin if h == 1 else 0, 2 * group, unit, 0)
        if h == 1:
            ks[:behind] = halo_ref[far - 1, own - behind :, :LANES].astype(jnp.float32)
            vs[:behind] = halo_ref[far - 1, own - behind :, LANES:].astype(jnp.float32)

    begin = 2 if group == 4 else 0
    if ahead:
        attention(0, 5, late_near)
    else:
        for number, d in enumerate(dilation_rates[:-1]):
            if counts[number] > 1:
                attention(number, (counts[number] - 1) * d, lambda u, d=d: (lax.rem(u, d), 1 + u // d))
    spread_first()
    if ahead:
        attention(1, 8, late_middle)
    def pass_corner():
        edges_arrive(0)
        z_relay(1)

    when(last, pass_corner)
    for h in range(1, far + 1):
        when(plane - h >= 0, functools.partial(sort, h))

    for number, d in enumerate(dilation_rates[:-1]):
        attention(number, d, lambda u: (u, 0), opening=True)
    when(~last, pass_corner)
    lax.fori_loop(0, wide, wide_attention, 0, unroll=4)
    spread_rest()
    def att_lanes(i):
        return att_all.at[:, pl.ds(pl.multiple_of((g ^ i) * LANES, LANES), LANES)]

    def att_out(i):
        mine = pl.ds(pl.multiple_of((g ^ i) * rows, rows), rows)
        return pltpu.make_async_remote_copy(
            src_ref=att.at[mine], dst_ref=att_lanes(0), send_sem=a_send.at[0], recv_sem=a_recv.at[i - 1],
            device_id=at(mate(i), tp), device_id_type=MESH)

    def att_in(i):
        return pltpu.make_async_remote_copy(
            src_ref=att.at[pl.ds(0, rows)], dst_ref=att_lanes(i), send_sem=a_send.at[0], recv_sem=a_recv.at[i - 1],
            device_id=at(mate(i), tp), device_id_type=MESH)

    def lse_out(i):
        return pltpu.make_async_remote_copy(
            src_ref=lse_ref.at[g ^ i], dst_ref=lse_all.at[g], send_sem=l_send.at[0], recv_sem=l_recv.at[i - 1],
            device_id=at(mate(i), tp), device_id_type=MESH)

    def lse_in(i):
        return pltpu.make_async_remote_copy(
            src_ref=lse_ref.at[g ^ i], dst_ref=lse_all.at[g ^ i], send_sem=l_send.at[0], recv_sem=l_recv.at[i - 1],
            device_id=at(mate(i), tp), device_id_type=MESH)

    def split(x):
        high = x.astype(jnp.bfloat16)
        return [high, (x - high.astype(jnp.float32)).astype(jnp.bfloat16)]

    def finish(index, carry):
        i = lax.rem(index + 1, group)
        block = g ^ i
        for k in range(2):
            start = block * rows + k * half
            at_run = pl.ds(pl.multiple_of(start // wide, run), run)
            here = pl.ds(pl.multiple_of(start, half), half)
            terms = split(out_cls[:, at_run, :].reshape(half, LANES)) + split(lse_cls[:, at_run, :].reshape(half, LANES))
            back_in_order = jnp.dot(turn[1], jnp.concatenate(terms, axis=1), preferred_element_type=jnp.float32)
            out = back_in_order[:, :LANES] + back_in_order[:, LANES : 2 * LANES]
            lse = back_in_order[:, 2 * LANES : 3 * LANES] + back_in_order[:, 3 * LANES :]
            was = top_s[here, :]
            new = jnp.maximum(was, lse)
            old_scale, scale = jnp.exp(was - new), jnp.exp(lse - new)
            den = den_s[here, :] * old_scale + scale
            att[here, :] = ((acc_s[here, :] * old_scale + out * scale) / den).astype(jnp.bfloat16)
            lse = new + jnp.log(den)
            for t in range(half // LANES):
                columns = lse[t * LANES : (t + 1) * LANES].T
                off = k * half + t * LANES
                for h in range(heads):
                    lse_ref[block, h : h + 1, off : off + LANES] = columns[h * HEAD_SIZE : h * HEAD_SIZE + 1, :]

        @pl.when(i > 0)
        def _():
            att_out(i).start()
            lse_out(i).start()

        return carry

    lax.fori_loop(0, group, finish, 0)
    own_a = pltpu.make_async_copy(att.at[pl.ds(pl.multiple_of(g * rows, rows), rows)], att_lanes(0), own_sem.at[1])
    own_a.start()
    own_l = pltpu.make_async_copy(lse_ref.at[g], lse_all.at[g], own_sem.at[2])
    own_l.start()
    for m in late:
        when(~relayed_in_plane(m), lambda: sides(m))
    z_forward(1)
    for m in late:
        edge_goes(m, lambda: edges_on(m))
    own_a.wait()
    for i in range(1, group):
        att_in(i).wait_recv()

    total_columns = sums.shape[1]
    if by_plane:
        strip_columns = group * cut
        pieces = [(m, 0, strip_columns) for m in strips]
        if group == 4 and 2 * cut % LANES == 0:
            pieces = pieces[:-1] + [(strips[-1], side, 2 * cut) for side in range(2)]
    else:
        pieces = [(c, 0, total_columns // sum_pieces) for c in range(sum_pieces)]

    def columns_of(c):
        m, side, size = pieces[c]
        if not by_plane:
            return pl.ds(m * size, size)
        start = nearest(m) * strip_columns
        if size < strip_columns:
            start = start + (side ^ (g // 2)) * size
        return pl.ds(pl.multiple_of(start, LANES), size)

    def rows_of(j):
        return pl.ds(pl.multiple_of(lax.rem(tp + j, n_tp) * part, part), part)

    def sum_out(c, j):
        return pltpu.make_async_remote_copy(
            src_ref=sums.at[rows_of(j), columns_of(c)], dst_ref=sums_in.at[j - 1, :, columns_of(c)],
            send_sem=s_send.at[j - 1], recv_sem=s_recv.at[j - 1, c],
            device_id=at(sp, lax.rem(tp + j, n_tp)), device_id_type=MESH)

    def multiply(c):
        w = o_all[columns_of(c), :]
        product = lax.dot_general(att_all[...], w, (((1,), (1,)), ((), ())), preferred_element_type=jnp.float32)
        sums[:, columns_of(c)] = product.astype(jnp.bfloat16)
        for j in range(1, n_tp):
            sum_out(c, j).start()

    def add_up(c):
        total = sums[rows_of(0), columns_of(c)].astype(jnp.float32)
        for j in range(1, n_tp):
            sum_out(c, j).wait_recv()
            total += sums_in[j - 1, :, columns_of(c)].astype(jnp.float32)
        mixed_ref[:, columns_of(c)] = total.astype(jnp.bfloat16)

    lag = 2
    for c, (m, side, size) in enumerate(pieces):
        if by_plane and side == 0:
            sides_arrive(m)
        if by_plane and (side == 1 or size == strip_columns):
            if m > 0:
                edges_arrive(m)
                z_relayed(m)
        multiply(c)
        if c == 0:
            for k in range(2, z_hops):
                z_forward(k)
        if c >= lag:
            add_up(c - lag)
    for c in range(max(len(pieces) - lag, 0), len(pieces)):
        add_up(c)

    own_l.wait()
    for i in range(1, group):
        lse_in(i).wait_recv()
    for b in range(group):
        lse_out_ref[b * heads : (b + 1) * heads, :] = lse_all[b]

    if group > 1:
        all_of(w_ref.at[pl.ds(1, group - 1)], w1_send.at[0]).wait()
        for j in range(1, n_tp):
            all_of(tok_all.at[pl.ds(1, group - 1), pl.ds(0, 4 * bit_rows)], f_send.at[j - 1]).wait()
        all_of(tok_all.at[pl.ds(0, len(near)), pl.ds(0, 4 * bit_rows)], t_send.at[0]).wait()
        if group == 4:
            all_of(tok_all.at[0, pl.ds(0, 4 * bit_rows)], d_send.at[0]).wait()
    if planes > 1:
        lax.fori_loop(1, planes, lambda k, _: (relay_left(k), _)[1], 0)
        lax.fori_loop(1, planes, lambda k, _: (o_relay_left(k), _)[1], 0)
    for h in range(1, far + 1):
        when(plane + h < planes, lambda: all_of(kv_ref, h_send.at[h - 1]).wait())
    for j in range(1, n_tp):
        all_of(mixed_ref, s_send.at[j - 1]).wait()
    if group > 1:
        all_of(att.at[pl.ds(0, (group - 1) * rows)], a_send.at[0]).wait()
        all_of(lse_ref.at[pl.ds(0, group - 1)], l_send.at[0]).wait()
        all_of(o_all.at[pl.ds(0, planes * len(near) * cut)], b_send.at[0]).wait()
        for m in range(planes):
            edges_left(m)
        for k in range(1, z_hops + 1):
            z_relay_left(k)


def shards(n, n_tp, tokens, w_query, w_key, w_value, w_out):
    rows, model = tokens.shape
    depth, width = w_query.shape
    slabs = width // LANES
    reach = KEYS_BEHIND * dilation_rates[-1]
    group = 1
    while group < 4 and group * rows < reach and slabs % (2 * group) == 0 and n % (2 * group) == 0:
        group *= 2
    assert slabs == group
    far = (reach + group * rows - 1) // (group * rows)
    planes = n // group
    own = group * rows
    part = rows // n_tp
    heads = LANES // HEAD_SIZE

    turned = w_out.T
    cut = w_out.shape[1]
    wide = dilation_rates[-1]
    behind = KEYS_BEHIND * dilation_rates[-2]
    sum_pieces = 5 if group == 4 else planes if group > 1 else (4 if n * cut % (4 * LANES) == 0 else 1)
    sum_pieces = max(sum_pieces, planes + 1) if group > 1 else sum_pieces
    corners = max(planes - min(2, planes - 1), 1) if group == 4 else 1
    mates, others, hops, near = max(group - 1, 1), max(n_tp - 1, 1), max(planes - 1, 1), max(group // 2, 1)

    f32, bf16 = jnp.float32, jnp.bfloat16
    dma = pltpu.SemaphoreType.DMA
    vmem = pl.BlockSpec(memory_space=VMEM)
    mixed, lse = pl.pallas_call(
        functools.partial(layer_kernel, n, n_tp, group, far, heads, sum_pieces),
        out_shape=(
            jax.ShapeDtypeStruct((part, n * cut), bf16),
            jax.ShapeDtypeStruct((group * heads, rows), f32),
        ),
        in_specs=[pl.BlockSpec(memory_space=pltpu.HBM)] * 5,
        out_specs=(vmem, vmem),
        scratch_shapes=[
            VMEM((group, rows, model), bf16),
            VMEM((n, depth, 3 * LANES), bf16),
            VMEM((group, depth, 3 * LANES), bf16),
            VMEM((own, 2 * LANES), bf16), VMEM((far, own, 2 * LANES), bf16),
            VMEM((n * cut, width), bf16),
            VMEM((own, LANES), f32), VMEM((behind + own, LANES), f32), VMEM((behind + own, LANES), f32),
            VMEM((wide, own // wide, LANES), bf16),
            VMEM((wide, (far + 1) * own // wide, LANES), bf16), VMEM((wide, (far + 1) * own // wide, LANES), bf16),
            VMEM((wide, own // wide, LANES), f32), VMEM((wide, own // wide, LANES), f32),
            VMEM((2, rows // 2, rows // 2), bf16),
            VMEM((1 + len(dilation_rates), KEYS_BEHIND, 2 * KEYS_BEHIND), f32),
            VMEM((own, LANES), f32), VMEM((own, LANES), f32), VMEM((own, LANES), f32),
            VMEM((own, LANES), bf16), VMEM((group, heads, rows), f32), VMEM((group, heads, rows), f32),
            VMEM((rows, group * LANES), bf16),
            VMEM((rows, n * cut), bf16), VMEM((others, part, n * cut), bf16),
            dma((group,)), dma((4,)),
            dma((1,)), dma((mates,)),
            dma((hops,)), dma((group, hops)),
            dma((hops,)), dma((group, hops)),
            dma((1,)), dma((near, 2, 2)),
            dma((1,)), dma((near, 2)),
            dma((others,)), dma((mates, 2, others)),
            dma((far,)), dma((far, group, 2)),
            dma((hops,)), dma((hops,)), dma((hops,)), dma((hops,)),
            dma((1,)), dma((planes if group > 1 else 1, near)),
            dma((corners,)), dma((corners, near)),
            dma((2,)), dma((2,)), dma((3,)), dma((3,)),
            dma((1,)), dma((mates,)), dma((1,)), dma((mates,)),
            dma((others,)), dma((others, sum_pieces)),
        ],
        compiler_params=pltpu.CompilerParams(collective_id=0, has_side_effects=True, vmem_limit_bytes=46 << 20),
        cost_estimate=pl.CostEstimate(
            flops=2 * own * model * 3 * LANES, bytes_accessed=1 << 24, transcendentals=1 << 22),
        name="layer",
    )(*[pltpu.with_memory_space_constraint(x, pltpu.HBM) for x in (w_query, w_key, w_value, tokens, turned)])
    return mixed, lse


def solution(mesh):
    placed = (P("sp", None), P("sp", "tp"), P("sp", "tp"), P("sp", "tp"), P("tp", "sp"))
    return jax.shard_map(
        functools.partial(shards, mesh.shape["sp"], mesh.shape["tp"]),
        mesh=mesh,
        in_specs=placed,
        out_specs=(P(("sp", "tp"), None), P("tp", "sp")),
        check_vma=False,
    )
```

```python
import functools

import jax
import jax.numpy as jnp
from jax import lax
from jax.experimental import pallas as pl
from jax.experimental.pallas import tpu as pltpu
from jax.sharding import PartitionSpec as P

HEAD_SIZE = 64
KEYS_BEHIND = 128
LANES = 128

dilation_rates = (1, 4, 16)
neg_big = -1e30

MESH = pl.DeviceIdType.MESH
VMEM = pltpu.VMEM


def at(sp, tp):
    return {"sp": sp, "tp": tp}


def layer_kernel(
    n, n_tp, group, far, heads, sum_pieces, wq_ref, wk_ref, wv_ref, tok_ref, o_ref, mixed_ref, lse_out_ref,
    tok_all, w_all, w_ref, kv_ref, halo_ref, o_all, qs, ks, vs, q_cls, k_cls, v_cls, out_cls, lse_cls, turn, bias,
    top_s, den_s, acc_s, att, lse_ref, lse_all, att_all, sums, sums_in,
    pack_sem, own_sem, w1_send, w1_recv, up_send, up_recv, down_send, down_recv, t_send, t_recv, d_send, d_recv,
    f_send, f_recv, h_send, h_recv, ou_send, ou_recv, od_send, od_recv, b_send, b_recv, c_send, c_recv,
    zu_send, zu_recv, zd_send, zd_recv, a_send, a_recv, l_send, l_recv, s_send, s_recv,
):
    sp, tp = lax.axis_index("sp"), lax.axis_index("tp")
    planes = n // group
    g, plane = lax.rem(sp, group), sp // group
    rows = tok_ref.shape[0]
    own = group * rows
    base = plane * own
    half = rows // 2
    bit_rows = half // (2 * n_tp)
    part = mixed_ref.shape[0]
    cut, width = o_ref.shape
    half_cut = cut // 2
    wide = dilation_rates[-1]
    behind = KEYS_BEHIND * dilation_rates[-2]
    run = half // wide
    old = far * own // wide

    above = lax.rem(sp + group, n)
    below = lax.rem(sp + n - group, n)

    def mate(i):
        return plane * group + (g ^ i)

    near = [i for i in (1, 2) if i < group]

    barrier = pltpu.get_barrier_semaphore()
    greeted = 0

    def greet(sp_to, tp_to):
        pl.semaphore_signal(barrier, inc=1, device_id=at(sp_to, tp_to), device_id_type=MESH)
        return 1

    for i in range(1, group):
        greeted += greet(mate(i), tp)
    if planes > 1:
        for h in range(1, max(far, 1) + 1):
            greeted += greet(lax.rem(sp + h * group, n), tp)
            greeted += greet(lax.rem(sp + n - h * group, n), tp)
    for j in range(1, n_tp):
        greeted += greet(sp, lax.rem(tp + j, n_tp))

    own_t = pltpu.make_async_copy(tok_ref, tok_all.at[g], own_sem.at[0])

    def strip(q, i, part_of=None):
        origin = q * group + (g ^ i)
        if part_of is None:
            return o_all.at[pl.ds(pl.multiple_of(origin * cut, cut), cut)]
        return o_all.at[pl.ds(pl.multiple_of(origin * cut + part_of * half_cut, half_cut), half_cut)]

    own_o = pltpu.make_async_copy(o_ref, strip(plane, 0), own_sem.at[3])

    def pack(t, i):
        source = (wq_ref, wk_ref, wv_ref)[t].at[:, pl.ds(pl.multiple_of((g ^ i) * LANES, LANES), LANES)]
        lanes = pl.ds(t * LANES, LANES)
        to = w_all.at[sp, :, lanes] if i == 0 else w_ref.at[i, :, lanes]
        return pltpu.make_async_copy(source, to, pack_sem.at[i])

    def all_of(view, sem):
        return pltpu.make_async_copy(view, view, sem)

    def packed(i):
        view = w_all.at[sp] if i == 0 else w_ref.at[i]
        all_of(view, pack_sem.at[i]).wait()

    for i in list(range(1, group)) + [0]:
        for t in range(3):
            pack(t, i).start()
    own_o.start()
    own_t.start()
    pl.semaphore_wait(barrier, greeted)

    def w_in_plane(i):
        return pltpu.make_async_remote_copy(
            src_ref=w_ref.at[i], dst_ref=w_all.at[sp], send_sem=w1_send.at[0], recv_sem=w1_recv.at[i - 1],
            device_id=at(mate(i), tp), device_id_type=MESH)

    def w_in_plane_arrives(i):
        return pltpu.make_async_remote_copy(
            src_ref=w_ref.at[i], dst_ref=w_all.at[mate(i)], send_sem=w1_send.at[0], recv_sem=w1_recv.at[i - 1],
            device_id=at(mate(i), tp), device_id_type=MESH)

    def slab(p, i):
        return w_all.at[lax.rem(p + 2 * planes, planes) * group + (g ^ i)]

    def up(i, k, p):
        return pltpu.make_async_remote_copy(
            src_ref=slab(p, i), dst_ref=slab(p, i), send_sem=up_send.at[k - 1], recv_sem=up_recv.at[i, k - 1],
            device_id=at(above, tp), device_id_type=MESH)

    def down(i, k, p):
        return pltpu.make_async_remote_copy(
            src_ref=slab(p, i), dst_ref=slab(p, i), send_sem=down_send.at[k - 1], recv_sem=down_recv.at[i, k - 1],
            device_id=at(below, tp), device_id_type=MESH)

    def o_up(k, p):
        ref = strip(lax.rem(p + 2 * planes, planes), 0)
        return pltpu.make_async_remote_copy(
            src_ref=ref, dst_ref=ref, send_sem=ou_send.at[k - 1], recv_sem=ou_recv.at[k - 1],
            device_id=at(above, tp), device_id_type=MESH)

    def o_down(k, p):
        ref = strip(lax.rem(p + 2 * planes, planes), 0)
        return pltpu.make_async_remote_copy(
            src_ref=ref, dst_ref=ref, send_sem=od_send.at[k - 1], recv_sem=od_recv.at[k - 1],
            device_id=at(below, tp), device_id_type=MESH)

    def when(condition, action):
        @pl.when(condition)
        def _():
            action()

    first, last = plane == 0, plane == planes - 1

    def relay(k, i):
        when(~last & (plane - k + 1 >= 0), lambda: up(i, k, plane - k + 1).start())
        when(~first & (plane + k - 1 < planes), lambda: down(i, k, plane + k - 1).start())

    def relayed(k, i):
        when(plane - k >= 0, lambda: up(i, k, plane - k).wait_recv())
        when(plane + k < planes, lambda: down(i, k, plane + k).wait_recv())

    def relay_left(k):
        slabs_of_a_plane = w_all.at[pl.ds(0, group)]
        when(~last & (plane - k + 1 >= 0), lambda: all_of(slabs_of_a_plane, up_send.at[k - 1]).wait())
        when(~first & (plane + k - 1 < planes), lambda: all_of(slabs_of_a_plane, down_send.at[k - 1]).wait())

    def o_relay(k):
        when(~last & (plane - k + 1 >= 0), lambda: o_up(k, plane - k + 1).start())
        when(~first & (plane + k - 1 < planes), lambda: o_down(k, plane + k - 1).start())

    def o_relay_left(k):
        when(~last & (plane - k + 1 >= 0), lambda: o_up(k, plane - k + 1).wait_send())
        when(~first & (plane + k - 1 < planes), lambda: o_down(k, plane + k - 1).wait_send())

    def hops(body):
        def one(k, _):
            for i in range(group):
                body(k, i)
            return _

        return one

    def nearest(m):
        left, right = plane, planes - 1 - plane
        short = jnp.minimum(left, right)
        zigzag = plane + (m // 2 if m % 2 == 0 else -((m + 1) // 2))
        return jnp.where(m <= 2 * short, zigzag, jnp.where(left < right, m, planes - 1 - m))

    def side_out(m, i):
        ref = strip(nearest(m), 0)
        return pltpu.make_async_remote_copy(
            src_ref=ref, dst_ref=ref, send_sem=b_send.at[0], recv_sem=b_recv.at[m, i - 1],
            device_id=at(mate(i), tp), device_id_type=MESH)

    def side_in(m, i):
        ref = strip(nearest(m), i)
        return pltpu.make_async_remote_copy(
            src_ref=ref, dst_ref=ref, send_sem=b_send.at[0], recv_sem=b_recv.at[m, i - 1],
            device_id=at(mate(i), tp), device_id_type=MESH)

    up_hops = min(2, planes - 1) if group == 4 else 0
    down_hops = up_hops
    straight = group == 4 and planes - 1 > up_hops
    z_hops = max(up_hops, down_hops)
    z_least = min(up_hops, down_hops)

    def edge_at(m):
        return max(m - z_least, 0)

    def edge_out(m, i):
        ref = strip(nearest(m), i, i - 1)
        return pltpu.make_async_remote_copy(
            src_ref=ref, dst_ref=ref, send_sem=c_send.at[edge_at(m)], recv_sem=c_recv.at[edge_at(m), i - 1],
            device_id=at(mate(3 - i), tp), device_id_type=MESH)

    def edge_in(m, i):
        ref = strip(nearest(m), 3, i - 1)
        return pltpu.make_async_remote_copy(
            src_ref=ref, dst_ref=ref, send_sem=c_send.at[edge_at(m)], recv_sem=c_recv.at[edge_at(m), i - 1],
            device_id=at(mate(3 - i), tp), device_id_type=MESH)

    def sides(m):
        for i in near:
            side_out(m, i).start()

    def straight_out():
        ref = strip(planes - 1, 3)
        return pltpu.make_async_remote_copy(
            src_ref=ref, dst_ref=ref, send_sem=zd_send.at[2], recv_sem=zd_recv.at[2],
            device_id=at(above, tp), device_id_type=MESH)

    def straight_in():
        ref = strip(planes - 1, 3)
        return pltpu.make_async_remote_copy(
            src_ref=ref, dst_ref=ref, send_sem=zd_send.at[2], recv_sem=zd_recv.at[2],
            device_id=at(below, tp), device_id_type=MESH)

    def beyond(m):
        there = nearest(m) - plane
        return (-there > up_hops) | ((there > down_hops) & (there < planes - 1))

    def edge_goes(m, action):
        if group == 4:
            if m == 0:
                action()
            elif m > z_least:
                when(beyond(m), action)

    def edges_on(m):
        for i in near:
            side_in(m, i).wait_recv()
            if group == 4:
                edge_out(m, i).start()

    def sides_arrive(m):
        def wait():
            for i in near:
                side_in(m, i).wait_recv()

        if group == 4 and m > z_least:
            when(~beyond(m), wait)
        elif m > 0:
            wait()

    def edges_arrive(m):
        edge_goes(m, lambda: [edge_in(m, i).wait_recv() for i in near])

    def edges_left(m):
        edge_goes(m, lambda: all_of(strip(0, 0), c_send.at[edge_at(m)]).wait())

    def z_up(k, p):
        ref = strip(lax.rem(p + 2 * planes, planes), 3)
        return pltpu.make_async_remote_copy(
            src_ref=ref, dst_ref=ref, send_sem=zu_send.at[k - 1], recv_sem=zu_recv.at[k - 1],
            device_id=at(above, tp), device_id_type=MESH)

    def z_down(k, p):
        ref = strip(lax.rem(p + 2 * planes, planes), 3)
        return pltpu.make_async_remote_copy(
            src_ref=ref, dst_ref=ref, send_sem=zd_send.at[k - 1], recv_sem=zd_recv.at[k - 1],
            device_id=at(below, tp), device_id_type=MESH)

    def z_relay(k):
        if k <= up_hops:
            when(~last & (plane - k + 1 >= 0), lambda: z_up(k, plane - k + 1).start())
        if k <= down_hops:
            when(~first & (plane + k - 1 < planes), lambda: z_down(k, plane + k - 1).start())

    def z_forward(k):
        def up_on():
            z_up(k, plane - k).wait_recv()
            z_up(k + 1, plane - k).start()

        def down_on():
            z_down(k, plane + k).wait_recv()
            z_down(k + 1, plane + k).start()

        if k < up_hops:
            when(~last & (plane - k >= 0), up_on)
        if k < down_hops:
            when(~first & (plane + k < planes), down_on)

    def z_relayed(k):
        if k <= up_hops:
            ends = last if k < up_hops else True
            when(ends & (plane - k >= 0), lambda: z_up(k, plane - k).wait_recv())
        if k <= down_hops:
            ends = first if k < down_hops else True
            when(ends & (plane + k < planes), lambda: z_down(k, plane + k).wait_recv())

    def z_relay_left(k):
        if k <= up_hops:
            when(~last & (plane - k + 1 >= 0), lambda: z_up(k, plane - k + 1).wait_send())
        if k <= down_hops:
            when(~first & (plane + k - 1 < planes), lambda: z_down(k, plane + k - 1).wait_send())

    def o_relayed(k):
        def from_below():
            o_up(k, plane - k).wait_recv()

        def from_above():
            o_down(k, plane + k).wait_recv()

        when(plane - k >= 0, from_below)
        when(plane + k < planes, from_above)

    def bit(s, p, t):
        return pl.ds(pl.multiple_of(s * half + (p * n_tp + t) * bit_rows, bit_rows), bit_rows)

    def tokens_out(i, p, s):
        return pltpu.make_async_remote_copy(
            src_ref=tok_ref.at[bit(s, p, tp)], dst_ref=tok_all.at[g, bit(s, p, tp)],
            send_sem=t_send.at[0], recv_sem=t_recv.at[i - 1, p, s], device_id=at(mate(i), tp), device_id_type=MESH)

    def tokens_in(i, p, s):
        return pltpu.make_async_remote_copy(
            src_ref=tok_ref.at[bit(s, p, tp)], dst_ref=tok_all.at[g ^ i, bit(s, p, tp)],
            send_sem=t_send.at[0], recv_sem=t_recv.at[i - 1, p, s], device_id=at(mate(i), tp), device_id_type=MESH)

    def corner_out(i, s):
        ref = tok_all.at[g ^ i, bit(s, i - 1, tp)]
        return pltpu.make_async_remote_copy(
            src_ref=ref, dst_ref=ref, send_sem=d_send.at[0], recv_sem=d_recv.at[i - 1, s],
            device_id=at(mate(3 - i), tp), device_id_type=MESH)

    def corner_in(i, s):
        ref = tok_all.at[g ^ 3, bit(s, i - 1, tp)]
        return pltpu.make_async_remote_copy(
            src_ref=ref, dst_ref=ref, send_sem=d_send.at[0], recv_sem=d_recv.at[i - 1, s],
            device_id=at(mate(3 - i), tp), device_id_type=MESH)

    def across(i, p, s, j):
        ref = tok_all.at[g ^ i, bit(s, p, tp)]
        return pltpu.make_async_remote_copy(
            src_ref=ref, dst_ref=ref, send_sem=f_send.at[j - 1], recv_sem=f_recv.at[i - 1, s, j - 1],
            device_id=at(sp, lax.rem(tp + j, n_tp)), device_id_type=MESH)

    def to_other_cores(i, p, s):
        for j in range(1, n_tp):
            across(i, p, s, j).start()

    def piece(i, step):
        return step if i == 1 else 1 - step

    for i in range(1, group):
        packed(i)
        w_in_plane(i).start()
    packed(0)
    if planes > 1:
        relay(1, 0)
    for step in range(2):
        for s in range(2):
            for i in near:
                tokens_out(i, piece(i, step), s).start()
    for i in range(1, group):
        w_in_plane_arrives(i).wait_recv()
        if planes > 1:
            relay(1, i)

    def pass_on(k, i):
        relayed(k, i)
        relay(k + 1, i)

    row = lax.broadcasted_iota(jnp.int32, (KEYS_BEHIND, 2 * KEYS_BEHIND), 0)
    col = lax.broadcasted_iota(jnp.int32, (KEYS_BEHIND, 2 * KEYS_BEHIND), 1)
    dist = KEYS_BEHIND + row - col
    band = (dist >= 0) & (dist <= KEYS_BEHIND)
    bias[0] = jnp.where(band, 0.0, neg_big)
    for number, d in enumerate(dilation_rates):
        bias[1 + number] = jnp.where(band & (base // d - KEYS_BEHIND + col >= 0), 0.0, neg_big)
    to_row = lax.broadcasted_iota(jnp.int32, (half, half), 0)
    from_row = lax.broadcasted_iota(jnp.int32, (half, half), 1)
    turn[0] = (from_row == to_row % run * wide + to_row // run).astype(jnp.float32).astype(jnp.bfloat16)
    turn[1] = (from_row == to_row % wide * run + to_row // wide).astype(jnp.float32).astype(jnp.bfloat16)

    @pl.when(plane == 0)
    def _():
        ks[:behind] = jnp.zeros((behind, LANES), jnp.float32)
        vs[:behind] = jnp.zeros((behind, LANES), jnp.float32)

    for h in range(1, far + 1):
        @pl.when(plane - h < 0)
        def _():
            gone = slice((far - h) * own // wide, (far - h + 1) * own // wide)
            k_cls[:, gone] = jnp.zeros((wide, own // wide, LANES), jnp.bfloat16)
            v_cls[:, gone] = jnp.zeros((wide, own // wide, LANES), jnp.bfloat16)

    if planes > 1:
        lax.fori_loop(1, planes - 1, hops(pass_on), 0)
    own_o.wait()
    if planes > 1:
        o_relay(1)
    for s in range(2):
        for i in near:
            tokens_in(i, piece(i, 0), s).wait_recv()
            if group == 4:
                corner_out(i, s).start()
            to_other_cores(i, piece(i, 0), s)
    if planes > 1:
        for i in range(group):
            relayed(planes - 1, i)
    for s in range(2):
        for i in near:
            tokens_in(i, piece(i, 1), s).wait_recv()
            to_other_cores(i, piece(i, 1), s)
    if near:
        sides(0)
    own_t.wait()

    def halo_out(h, i, k):
        view = pl.ds(pl.multiple_of((g ^ i) * rows + k * half, half), half)
        return pltpu.make_async_remote_copy(
            src_ref=kv_ref.at[view], dst_ref=halo_ref.at[far - h, view],
            send_sem=h_send.at[h - 1], recv_sem=h_recv.at[h - 1, i, k],
            device_id=at(lax.rem(sp + h * group, n), tp), device_id_type=MESH)

    def by_classes(y):
        sorted_rows = jnp.dot(turn[0], y, preferred_element_type=jnp.float32).astype(jnp.bfloat16)
        return sorted_rows.reshape(wide, run, y.shape[1])

    def sort_unit(h):
        def unit(u, carry):
            i, k = u // 2, lax.rem(u, 2)
            halo_out(h, i, k).wait_recv()
            start = (g ^ i) * rows + k * half
            by_class = by_classes(halo_ref[far - h, pl.ds(pl.multiple_of(start, half), half), :])
            at_run = pl.ds(pl.multiple_of((far - h) * (own // wide) + start // wide, run), run)
            k_cls[:, at_run, :] = by_class[:, :, :LANES]
            v_cls[:, at_run, :] = by_class[:, :, LANES:]
            return carry

        return unit

    def tile(i, k):
        block = g ^ i
        x = tok_all[block, pl.ds(pl.multiple_of(k * half, half), half), :]
        w = w_all[...].reshape(-1, 3 * LANES)
        y = jnp.dot(x, w, preferred_element_type=jnp.float32).astype(jnp.bfloat16)
        start = block * rows + k * half
        to = pl.ds(pl.multiple_of(start, half), half)
        past = pl.ds(pl.multiple_of(behind + start, half), half)
        kv_ref[to, :] = y[:, LANES:]
        qs[to, :] = y[:, :LANES].astype(jnp.float32) * HEAD_SIZE ** (-0.5)
        ks[past, :] = y[:, LANES : 2 * LANES].astype(jnp.float32)
        vs[past, :] = y[:, 2 * LANES :].astype(jnp.float32)
        by_class = by_classes(y)
        at_run = pl.ds(pl.multiple_of(start // wide, run), run)
        q_cls[:, at_run, :] = by_class[:, :, :LANES] * HEAD_SIZE ** (-0.5)
        past_run = pl.ds(pl.multiple_of(old + start // wide, run), run)
        k_cls[:, past_run, :] = by_class[:, :, LANES : 2 * LANES]
        v_cls[:, past_run, :] = by_class[:, :, 2 * LANES :]
        for h in range(1, far + 1):
            @pl.when(plane + h < planes)
            def _():
                halo_out(h, i, k).start()

    def tiles(picks, ready):
        def one(s, _):
            i, k = picks(s)
            ready(i, k)
            tile(i, k)
            return _

        lax.fori_loop(0, 2, one, 0)

    def crossed(i, k):
        for j in range(1, n_tp):
            all_of(tok_all.at[0, pl.ds(0, 2 * bit_rows)], f_recv.at[i - 1, k, j - 1]).wait()

    def o_pass(k):
        if k < planes:
            o_relayed(k)
            if k + 1 < planes:
                o_relay(k + 1)

    def unroll_of(trips):
        return next(u for u in (5, 4, 3, 2, 1) if trips % u == 0)

    def attention(number, trips, place, opening=False):
        d = dilation_rates[number]
        step = min(KEYS_BEHIND, own // d)
        span = step + KEYS_BEHIND
        mask_at = 1 + number if opening else 0

        def block(index, _):
            cls, b = place(index)
            start = b * (step * d) + cls
            q_at = pl.ds(start, step, stride=d) if d > 1 else pl.ds(pl.multiple_of(start, step), step)
            k_start = behind - KEYS_BEHIND * d + start
            k_at = pl.ds(k_start, span, stride=d) if d > 1 else pl.ds(pl.multiple_of(k_start, step), span)
            q = qs[q_at, :]
            k = ks[k_at, :].astype(jnp.bfloat16)
            v = vs[k_at, :].astype(jnp.bfloat16)
            v = jnp.concatenate([v, jnp.ones((span, LANES), jnp.bfloat16)], axis=1)
            low = lax.broadcasted_iota(jnp.int32, (step, LANES), 1) < HEAD_SIZE
            q2 = jnp.concatenate([jnp.where(low, q, 0.0), jnp.where(low, 0.0, q)], axis=0).astype(jnp.bfloat16)
            s = lax.dot_general(q2, k, (((1,), (1,)), ((), ())), preferred_element_type=jnp.float32)
            seen = bias[mask_at, :step, :span]
            s = s + jnp.concatenate([seen, seen], axis=0)
            top = jnp.max(s, axis=1, keepdims=True)
            p = jnp.exp(s - top)
            o = jnp.dot(p.astype(jnp.bfloat16), v, preferred_element_type=jnp.float32)
            top = jnp.where(low, top[:step], top[step:])
            den = jnp.where(low, o[:step, LANES:], o[step:, LANES:])
            o = jnp.where(low, o[:step, :LANES], o[step:, :LANES])
            if number == 0:
                top_s[q_at, :] = top
                den_s[q_at, :] = den
                acc_s[q_at, :] = o
            else:
                was = top_s[q_at, :]
                new = jnp.maximum(was, top)
                old_scale, scale = jnp.exp(was - new), jnp.exp(top - new)
                top_s[q_at, :] = new
                den_s[q_at, :] = den_s[q_at, :] * old_scale + den * scale
                acc_s[q_at, :] = acc_s[q_at, :] * old_scale + o * scale
            return _

        lax.fori_loop(0, trips, block, 0, unroll=unroll_of(trips))

    ahead = group == 4 and rows == KEYS_BEHIND * dilation_rates[1]
    per = rows // KEYS_BEHIND
    ready_row = 1 + 2 * (g // 2)

    def early_near(u):
        return 0, jnp.where(u < 9, (g ^ (u // 3)) * per + 1 + lax.rem(u, 3), per * ready_row)

    def late_near(u):
        rest = jnp.where(u == 3, 2, 4 - ready_row)
        return 0, jnp.where(u < 3, (g ^ 3) * per + 1 + u, per * rest)

    def early_middle(u):
        return u, ready_row

    def late_middle(u):
        return lax.rem(u, 4), jnp.where(u < 4, 2, 4 - ready_row)

    tiles(lambda s: (0, s), lambda i, k: None)
    if group > 1:
        o_pass(1)
    if group == 2:
        tiles(lambda s: (1, s), crossed)
    if group == 4:
        tiles(lambda s: (1 + s, 0), crossed)
        tiles(lambda s: (1 + s, 1), crossed)
        if ahead:
            attention(0, 10, early_near)
        for s in range(2):
            if s == 1:
                when(plane >= 1, lambda: lax.fori_loop(0, 2, sort_unit(1), 0))
            for i in near:
                corner_in(i, s).wait_recv()
                to_other_cores(3, i - 1, s)
            if s == 0:
                if ahead:
                    attention(1, 4, early_middle)
            crossed(3, s)
            tile(3, s)
            if s == 0 and 2 < planes:
                o_relayed(2)
        if 3 < planes:
            o_relay(3)

    by_plane = group > 1
    def wide_attention(cls, _):
        step = own // wide
        span = step + KEYS_BEHIND
        q = q_cls[cls].astype(jnp.float32)
        k = k_cls[cls, old - KEYS_BEHIND :, :]
        v = v_cls[cls, old - KEYS_BEHIND :, :]
        v = jnp.concatenate([v, jnp.ones((span, LANES), jnp.bfloat16)], axis=1)
        low = lax.broadcasted_iota(jnp.int32, (step, LANES), 1) < HEAD_SIZE
        q2 = jnp.concatenate([jnp.where(low, q, 0.0), jnp.where(low, 0.0, q)], axis=0).astype(jnp.bfloat16)
        s = lax.dot_general(q2, k, (((1,), (1,)), ((), ())), preferred_element_type=jnp.float32)
        seen = bias[len(dilation_rates), :step, :span]
        s = s + jnp.concatenate([seen, seen], axis=0)
        top = jnp.max(s, axis=1, keepdims=True)
        p = jnp.exp(s - top)
        o = jnp.dot(p.astype(jnp.bfloat16), v, preferred_element_type=jnp.float32)
        top = jnp.where(low, top[:step], top[step:])
        den = jnp.where(low, o[:step, LANES:], o[step:, LANES:])
        out_cls[cls] = jnp.where(low, o[:step, :LANES], o[step:, :LANES]) / den
        lse_cls[cls] = top + jnp.log(den)
        return _

    counts = [own // d // min(KEYS_BEHIND, own // d) for d in dilation_rates[:-1]]

    strips = list(range(planes)) if by_plane else []
    early, late = strips[1:3], strips[3:]

    def later(k, _):
        o_relayed(k)
        when(k + 1 < planes, lambda: o_relay(k + 1))
        return _

    def spread_first():
        if by_plane:
            edges_on(0)
            for m in early:
                sides(m)

    def spread_rest():
        started = {1: 1, 2: 2, 4: 3}[group]
        if started < planes:
            lax.fori_loop(started, planes, later, 0)
        for m in late:
            when(relayed_in_plane(m), lambda: sides(m))

    def relayed_in_plane(m):
        return beyond(m) if group == 4 else plane >= 0

    def sort(h):
        unit = sort_unit(h)
        lax.fori_loop(begin if h == 1 else 0, 2 * group, unit, 0)
        if h == 1:
            ks[:behind] = halo_ref[far - 1, own - behind :, :LANES].astype(jnp.float32)
            vs[:behind] = halo_ref[far - 1, own - behind :, LANES:].astype(jnp.float32)

    begin = 2 if group == 4 else 0
    if ahead:
        attention(0, 5, late_near)
    else:
        for number, d in enumerate(dilation_rates[:-1]):
            if counts[number] > 1:
                attention(number, (counts[number] - 1) * d, lambda u, d=d: (lax.rem(u, d), 1 + u // d))
    spread_first()
    if ahead:
        attention(1, 8, late_middle)
    def pass_corner():
        edges_arrive(0)
        if straight:
            when(last, lambda: straight_out().start())
        z_relay(1)

    when(last, pass_corner)
    for h in range(1, far + 1):
        when(plane - h >= 0, functools.partial(sort, h))

    for number, d in enumerate(dilation_rates[:-1]):
        attention(number, d, lambda u: (u, 0), opening=True)
    when(~last, pass_corner)
    lax.fori_loop(0, wide, wide_attention, 0, unroll=4)
    spread_rest()
    def att_lanes(i):
        return att_all.at[:, pl.ds(pl.multiple_of((g ^ i) * LANES, LANES), LANES)]

    def att_out(i):
        mine = pl.ds(pl.multiple_of((g ^ i) * rows, rows), rows)
        return pltpu.make_async_remote_copy(
            src_ref=att.at[mine], dst_ref=att_lanes(0), send_sem=a_send.at[0], recv_sem=a_recv.at[i - 1],
            device_id=at(mate(i), tp), device_id_type=MESH)

    def att_in(i):
        return pltpu.make_async_remote_copy(
            src_ref=att.at[pl.ds(0, rows)], dst_ref=att_lanes(i), send_sem=a_send.at[0], recv_sem=a_recv.at[i - 1],
            device_id=at(mate(i), tp), device_id_type=MESH)

    def lse_out(i):
        return pltpu.make_async_remote_copy(
            src_ref=lse_ref.at[g ^ i], dst_ref=lse_all.at[g], send_sem=l_send.at[0], recv_sem=l_recv.at[i - 1],
            device_id=at(mate(i), tp), device_id_type=MESH)

    def lse_in(i):
        return pltpu.make_async_remote_copy(
            src_ref=lse_ref.at[g ^ i], dst_ref=lse_all.at[g ^ i], send_sem=l_send.at[0], recv_sem=l_recv.at[i - 1],
            device_id=at(mate(i), tp), device_id_type=MESH)

    def split(x):
        high = x.astype(jnp.bfloat16)
        return [high, (x - high.astype(jnp.float32)).astype(jnp.bfloat16)]

    def finish(index, carry):
        i = lax.rem(index + 1, group)
        block = g ^ i
        for k in range(2):
            start = block * rows + k * half
            at_run = pl.ds(pl.multiple_of(start // wide, run), run)
            here = pl.ds(pl.multiple_of(start, half), half)
            terms = split(out_cls[:, at_run, :].reshape(half, LANES)) + split(lse_cls[:, at_run, :].reshape(half, LANES))
            back_in_order = jnp.dot(turn[1], jnp.concatenate(terms, axis=1), preferred_element_type=jnp.float32)
            out = back_in_order[:, :LANES] + back_in_order[:, LANES : 2 * LANES]
            lse = back_in_order[:, 2 * LANES : 3 * LANES] + back_in_order[:, 3 * LANES :]
            was = top_s[here, :]
            new = jnp.maximum(was, lse)
            old_scale, scale = jnp.exp(was - new), jnp.exp(lse - new)
            den = den_s[here, :] * old_scale + scale
            att[here, :] = ((acc_s[here, :] * old_scale + out * scale) / den).astype(jnp.bfloat16)
            lse = new + jnp.log(den)
            for t in range(half // LANES):
                columns = lse[t * LANES : (t + 1) * LANES].T
                off = k * half + t * LANES
                for h in range(heads):
                    lse_ref[block, h : h + 1, off : off + LANES] = columns[h * HEAD_SIZE : h * HEAD_SIZE + 1, :]

        @pl.when(i > 0)
        def _():
            att_out(i).start()
            lse_out(i).start()

        return carry

    lax.fori_loop(0, group, finish, 0)
    own_a = pltpu.make_async_copy(att.at[pl.ds(pl.multiple_of(g * rows, rows), rows)], att_lanes(0), own_sem.at[1])
    own_a.start()
    own_l = pltpu.make_async_copy(lse_ref.at[g], lse_all.at[g], own_sem.at[2])
    own_l.start()
    for m in late:
        when(~relayed_in_plane(m), lambda: sides(m))
    z_forward(1)
    for m in late:
        edge_goes(m, lambda: edges_on(m))
    own_a.wait()
    for i in range(1, group):
        att_in(i).wait_recv()

    total_columns = sums.shape[1]
    if by_plane:
        strip_columns = group * cut
        pieces = [(m, 0, strip_columns) for m in strips]
        if group == 4 and 2 * cut % LANES == 0:
            pieces = pieces[:-1] + [(strips[-1], side, 2 * cut) for side in range(2)]
    else:
        pieces = [(c, 0, total_columns // sum_pieces) for c in range(sum_pieces)]

    def columns_of(c):
        m, side, size = pieces[c]
        if not by_plane:
            return pl.ds(m * size, size)
        start = nearest(m) * strip_columns
        if size < strip_columns:
            start = start + (side ^ (g // 2)) * size
        return pl.ds(pl.multiple_of(start, LANES), size)

    def rows_of(j):
        return pl.ds(pl.multiple_of(lax.rem(tp + j, n_tp) * part, part), part)

    def sum_out(c, j):
        return pltpu.make_async_remote_copy(
            src_ref=sums.at[rows_of(j), columns_of(c)], dst_ref=sums_in.at[j - 1, :, columns_of(c)],
            send_sem=s_send.at[j - 1], recv_sem=s_recv.at[j - 1, c],
            device_id=at(sp, lax.rem(tp + j, n_tp)), device_id_type=MESH)

    def multiply(c):
        w = o_all[columns_of(c), :]
        product = lax.dot_general(att_all[...], w, (((1,), (1,)), ((), ())), preferred_element_type=jnp.float32)
        sums[:, columns_of(c)] = product.astype(jnp.bfloat16)
        for j in range(1, n_tp):
            sum_out(c, j).start()

    def add_up(c):
        total = sums[rows_of(0), columns_of(c)].astype(jnp.float32)
        for j in range(1, n_tp):
            sum_out(c, j).wait_recv()
            total += sums_in[j - 1, :, columns_of(c)].astype(jnp.float32)
        mixed_ref[:, columns_of(c)] = total.astype(jnp.bfloat16)

    lag = 2
    for c, (m, side, size) in enumerate(pieces):
        if by_plane and side == 0:
            sides_arrive(m)
        if by_plane and (side == 1 or size == strip_columns):
            if m > 0:
                edges_arrive(m)
                z_relayed(m)
                if straight and m == planes - 1:
                    when(first, lambda: straight_in().wait_recv())
        multiply(c)
        if c == 0:
            for k in range(2, z_hops):
                z_forward(k)
        if c >= lag:
            add_up(c - lag)
    for c in range(max(len(pieces) - lag, 0), len(pieces)):
        add_up(c)

    own_l.wait()
    for i in range(1, group):
        lse_in(i).wait_recv()
    for b in range(group):
        lse_out_ref[b * heads : (b + 1) * heads, :] = lse_all[b]

    if group > 1:
        all_of(w_ref.at[pl.ds(1, group - 1)], w1_send.at[0]).wait()
        for j in range(1, n_tp):
            all_of(tok_all.at[pl.ds(1, group - 1), pl.ds(0, 4 * bit_rows)], f_send.at[j - 1]).wait()
        all_of(tok_all.at[pl.ds(0, len(near)), pl.ds(0, 4 * bit_rows)], t_send.at[0]).wait()
        if group == 4:
            all_of(tok_all.at[0, pl.ds(0, 4 * bit_rows)], d_send.at[0]).wait()
    if planes > 1:
        lax.fori_loop(1, planes, lambda k, _: (relay_left(k), _)[1], 0)
        lax.fori_loop(1, planes, lambda k, _: (o_relay_left(k), _)[1], 0)
    for h in range(1, far + 1):
        when(plane + h < planes, lambda: all_of(kv_ref, h_send.at[h - 1]).wait())
    for j in range(1, n_tp):
        all_of(mixed_ref, s_send.at[j - 1]).wait()
    if group > 1:
        all_of(att.at[pl.ds(0, (group - 1) * rows)], a_send.at[0]).wait()
        all_of(lse_ref.at[pl.ds(0, group - 1)], l_send.at[0]).wait()
        all_of(o_all.at[pl.ds(0, planes * len(near) * cut)], b_send.at[0]).wait()
        for m in range(planes):
            edges_left(m)
        for k in range(1, z_hops + 1):
            z_relay_left(k)
        if straight:
            when(last, lambda: straight_out().wait_send())


def shards(n, n_tp, tokens, w_query, w_key, w_value, w_out):
    rows, model = tokens.shape
    depth, width = w_query.shape
    slabs = width // LANES
    reach = KEYS_BEHIND * dilation_rates[-1]
    group = 1
    while group < 4 and group * rows < reach and slabs % (2 * group) == 0 and n % (2 * group) == 0:
        group *= 2
    assert slabs == group
    far = (reach + group * rows - 1) // (group * rows)
    planes = n // group
    own = group * rows
    part = rows // n_tp
    heads = LANES // HEAD_SIZE

    turned = w_out.T
    cut = w_out.shape[1]
    wide = dilation_rates[-1]
    behind = KEYS_BEHIND * dilation_rates[-2]
    sum_pieces = 5 if group == 4 else planes if group > 1 else (4 if n * cut % (4 * LANES) == 0 else 1)
    sum_pieces = max(sum_pieces, planes + 1) if group > 1 else sum_pieces
    corners = max(planes - min(2, planes - 1), 1) if group == 4 else 1
    mates, others, hops, near = max(group - 1, 1), max(n_tp - 1, 1), max(planes - 1, 1), max(group // 2, 1)

    f32, bf16 = jnp.float32, jnp.bfloat16
    dma = pltpu.SemaphoreType.DMA
    vmem = pl.BlockSpec(memory_space=VMEM)
    mixed, lse = pl.pallas_call(
        functools.partial(layer_kernel, n, n_tp, group, far, heads, sum_pieces),
        out_shape=(
            jax.ShapeDtypeStruct((part, n * cut), bf16),
            jax.ShapeDtypeStruct((group * heads, rows), f32),
        ),
        in_specs=[pl.BlockSpec(memory_space=pltpu.HBM)] * 5,
        out_specs=(vmem, vmem),
        scratch_shapes=[
            VMEM((group, rows, model), bf16),
            VMEM((n, depth, 3 * LANES), bf16),
            VMEM((group, depth, 3 * LANES), bf16),
            VMEM((own, 2 * LANES), bf16), VMEM((far, own, 2 * LANES), bf16),
            VMEM((n * cut, width), bf16),
            VMEM((own, LANES), f32), VMEM((behind + own, LANES), f32), VMEM((behind + own, LANES), f32),
            VMEM((wide, own // wide, LANES), bf16),
            VMEM((wide, (far + 1) * own // wide, LANES), bf16), VMEM((wide, (far + 1) * own // wide, LANES), bf16),
            VMEM((wide, own // wide, LANES), f32), VMEM((wide, own // wide, LANES), f32),
            VMEM((2, rows // 2, rows // 2), bf16),
            VMEM((1 + len(dilation_rates), KEYS_BEHIND, 2 * KEYS_BEHIND), f32),
            VMEM((own, LANES), f32), VMEM((own, LANES), f32), VMEM((own, LANES), f32),
            VMEM((own, LANES), bf16), VMEM((group, heads, rows), f32), VMEM((group, heads, rows), f32),
            VMEM((rows, group * LANES), bf16),
            VMEM((rows, n * cut), bf16), VMEM((others, part, n * cut), bf16),
            dma((group,)), dma((4,)),
            dma((1,)), dma((mates,)),
            dma((hops,)), dma((group, hops)),
            dma((hops,)), dma((group, hops)),
            dma((1,)), dma((near, 2, 2)),
            dma((1,)), dma((near, 2)),
            dma((others,)), dma((mates, 2, others)),
            dma((far,)), dma((far, group, 2)),
            dma((hops,)), dma((hops,)), dma((hops,)), dma((hops,)),
            dma((1,)), dma((planes if group > 1 else 1, near)),
            dma((corners,)), dma((corners, near)),
            dma((2,)), dma((2,)), dma((3,)), dma((3,)),
            dma((1,)), dma((mates,)), dma((1,)), dma((mates,)),
            dma((others,)), dma((others, sum_pieces)),
        ],
        compiler_params=pltpu.CompilerParams(collective_id=0, has_side_effects=True, vmem_limit_bytes=46 << 20),
        cost_estimate=pl.CostEstimate(
            flops=2 * own * model * 3 * LANES, bytes_accessed=1 << 24, transcendentals=1 << 22),
        name="layer",
    )(*[pltpu.with_memory_space_constraint(x, pltpu.HBM) for x in (w_query, w_key, w_value, tokens, turned)])
    return mixed, lse


def solution(mesh):
    placed = (P("sp", None), P("sp", "tp"), P("sp", "tp"), P("sp", "tp"), P("tp", "sp"))
    return jax.shard_map(
        functools.partial(shards, mesh.shape["sp"], mesh.shape["tp"]),
        mesh=mesh,
        in_specs=placed,
        out_specs=(P(("sp", "tp"), None), P("tp", "sp")),
        check_vma=False,
    )
```
